32 devices in a mesh: grp: 2 (over y), sp: 4 (over z), tp: 4 (over x, core).
Axes of the slice: x: 2, y: 2, z: 4, core: 2. Of those that a mesh axis runs over, the one named last changes fastest.
Arguments:
- queries: bfloat16 [4096, 1024], P(('grp', 'sp'), 'tp'), parts along dimension 0, may hold values from -6 to 6
- memory_keys: bfloat16 [4096, 1024], P(('grp', 'sp'), 'tp'), parts along dimension 0, may hold values from -6 to 6
- memory_values: bfloat16 [4096, 1024], P(('grp', 'sp'), 'tp'), parts along dimension 0, may hold values from -6 to 6
- output_preactivation: bfloat16 [4096, 1024], P(('grp', 'sp'), 'tp'), parts along dimension 0, may hold values from -12 to 12
- input_preactivation: float32 [8, 4096], P('tp', ('grp', 'sp')), parts along dimension 1, may hold values from -6 to 140
- forget_preactivation: float32 [8, 4096], P('tp', ('grp', 'sp')), parts along dimension 1, as said below
- extra_forget_terms: float32 [8, 4096], P('tp', ('grp', 'sp')), parts along dimension 1, may hold values from -1 to 0, as said below
- head_norm_gain: float32 [128], replicated, may hold values from 0.1 to 1.9
- output_projection_matrix: bfloat16 [1024, 2048], P('tp'), may hold values from -0.1875 to 0.1875
- residual: bfloat16 [4096, 2048], P(('grp', 'sp', 'tp')), parts along dimension 0, may hold values from -6 to 6
- feedforward_norm_gain: float32 [2048], replicated, may hold values from 0.1 to 1.9
- feedforward_up_matrix: bfloat16 [2048, 8192], P('sp', 'tp'), may hold values from -0.125 to 0.125
- feedforward_down_matrix: bfloat16 [8192, 2048], P('tp', 'sp'), may hold values from -0.0625 to 0.0625
Outputs:
- layer_out: bfloat16 [4096, 2048], P(('grp', 'sp', 'tp')), parts along dimension 0
The draws below stay inside these ranges and needn't reach their ends.
There are 2 independent parts, one for each index of `grp`. The reference program is written for one: setup_inputs(seed, part) draws one part's arguments, and reference() takes and returns one part's arrays. A program takes and returns all parts, laid end to end along the dimension named above; an argument that names none is the same for every part. Nothing has to cross between parts.
Inputs may be any that keep to these rules, and one draw needn't show every extreme that they name: `forget_preactivation`: forget gate pre-activations. `extra_forget_terms`: extra log forget terms, zero at most positions.
All inputs are finite; a program needn't handle non-finite values.
Results may differ from the reference program's by a relative error of at most 0.018.
Values may be sent and summed in bfloat16 or wider, within the bound.
A program may use at most 64 MiB of HBM per device.

```python
import math
import jax
import jax.numpy as jnp
from jax import lax

D = 2048
FF = 8192
H = 8
DH = 128
BLOCK = 128
TOK_DEV = 512
M_WIDTH = 1024
SEQ = 2048
N_TP = 4


def draw_input_preactivation(key, part):
    draws = jax.random.split(jax.random.fold_in(key, 11), 1)
    values = jnp.clip(jax.random.normal(draws[0], (H, SEQ), jnp.float32), -6.0, 6.0)
    return values


def draw_forget_preactivation(key, part):
    draws = jax.random.split(jax.random.fold_in(key, 23), 3)
    order = jax.random.permutation(draws[0], H)
    slowly = order < H // 2
    center = jnp.where(slowly, math.log(2.5 * SEQ), 4.0).astype(jnp.float32)
    shifts = jax.random.uniform(draws[1], (H, SEQ // TOK_DEV, 1), jnp.float32, -0.7, 0.7)
    shifts = jnp.broadcast_to(shifts, (H, SEQ // TOK_DEV, TOK_DEV)).reshape(H, SEQ)
    jitter = jax.random.uniform(draws[2], (H, SEQ), jnp.float32, -1.0, 1.0)
    return center[:, None] + shifts + jitter


def draw_extra_forget_terms(key, part):
    draws = jax.random.split(jax.random.fold_in(key, 37), 2)
    quarter = SEQ // 4
    spots = jnp.arange(4)[None, :] * quarter + jax.random.randint(draws[0], (H, 4), 0, quarter)
    depths = jnp.log(jax.random.uniform(draws[1], (H, 4), jnp.float32, 0.5, 0.8))
    hits = jnp.arange(SEQ)[None, None, :] == spots[:, :, None]
    return jnp.sum(jnp.where(hits, depths[:, :, None], 0.0), axis=1)


def steps_of(stream_key, extent, cuts, low, top_value):
    gain, own = 1.0, jax.random.fold_in(stream_key, 6)
    for position, shards_of in cuts:
        steps = jnp.exp(jax.random.uniform(jax.random.fold_in(own, position), (shards_of,), jnp.float32, low / len(cuts), top_value / len(cuts)))
        gain = gain * jnp.repeat(steps, extent[position] // shards_of).reshape([-1 if axis == position else 1 for axis in range(len(extent))])
    return gain


def scatter_about(rng, shape, scale, reach, cuts=(), held_as=jnp.bfloat16):
    result = jax.random.normal(rng, shape, jnp.float32) * scale
    if len(cuts) > 0:
        result = steps_of(rng, shape, cuts, -0.22, 0.18) * result
    return jnp.clip(result, min=-reach, max=reach).astype(held_as)


def setup_inputs(seed: int = 0, part: int = 0) -> dict:
    key_of = jax.random.split(jax.random.key(seed), 14)
    part_splits = jax.random.split(jax.random.fold_in(key_of[13], part), 14)
    return {
        "queries": scatter_about(part_splits[0], (SEQ, M_WIDTH), 1.0, 6.0, ((0, 4), (1, 4))),
        "memory_keys": scatter_about(part_splits[1], (SEQ, M_WIDTH), 1.0, 6.0, ((0, 4), (1, 4))),
        "memory_values": scatter_about(part_splits[2], (SEQ, M_WIDTH), 1.0, 6.0, ((0, 4), (1, 4))),
        "output_preactivation": scatter_about(part_splits[3], (SEQ, M_WIDTH), 2.0, 12.0, ((0, 4), (1, 4))),
        "input_preactivation": draw_input_preactivation(jax.random.fold_in(jax.random.fold_in(key_of[13], part), 71), part),
        "forget_preactivation": draw_forget_preactivation(jax.random.fold_in(jax.random.fold_in(key_of[13], part), 71), part),
        "extra_forget_terms": draw_extra_forget_terms(jax.random.fold_in(jax.random.fold_in(key_of[13], part), 71), part),
        "head_norm_gain": jnp.clip(1.0 + 0.18 * jax.random.normal(key_of[7], (DH,), jnp.float32), 0.1, 1.9),
        "output_projection_matrix": scatter_about(key_of[8], (M_WIDTH, D), M_WIDTH ** -0.5, 0.1875, ((0, 4),)),
        "residual": scatter_about(part_splits[9], (SEQ, D), 1.0, 6.0, ((0, 16),)),
        "feedforward_norm_gain": jnp.clip(1.0 + 0.18 * jax.random.normal(key_of[10], (D,), jnp.float32), 0.1, 1.9),
        "feedforward_up_matrix": scatter_about(key_of[11], (D, FF), D ** -0.5, 0.125, ((0, 4), (1, 4))),
        "feedforward_down_matrix": scatter_about(key_of[12], (FF, D), FF ** -0.5, 0.0625, ((0, 4), (1, 4))),
    }


neg_big = -1e+30
norm_eps = 1e-06
highest = lax.Precision.HIGHEST

def rms_norm(tensor, gain_vec):
    mean_sq = lax.optimization_barrier(jnp.mean(tensor * tensor, axis=-1, keepdims=True))
    return tensor * lax.rsqrt(mean_sq + norm_eps) * gain_vec

def memory_cell(queries, memory_keys, memory_values, input_preactivation, forget_logarithm):
    blocks = SEQ // BLOCK

    def to_blocks(tensor):
        return jnp.moveaxis(tensor.reshape((H, blocks, BLOCK) + tensor.shape[2:]), 1, 0)
    causal = jnp.arange(BLOCK)[:, None] >= jnp.arange(BLOCK)[None, :]

    def advance(state_now, pieces):
        memory, stab_max = state_now
        query_blk, key_blk, val_blk, gate_blk, fgt_blk = pieces
        decay_logarithm = jnp.cumsum(fgt_blk, axis=-1)
        log_weight = decay_logarithm[:, :, None] - decay_logarithm[:, None, :] + gate_blk[:, None, :]
        log_weight = jnp.where(causal, log_weight, neg_big)
        carry_log = decay_logarithm + stab_max[:, None]
        row_max = jnp.maximum(lax.optimization_barrier(jnp.max(log_weight, axis=-1)), carry_log)
        scores = jnp.einsum('htd,hsd->hts', query_blk, key_blk, precision=highest) * jnp.exp(log_weight - row_max[..., None])
        carry_scale = jnp.exp(carry_log - row_max)
        hidden = jnp.einsum('hts,hsv->htv', scores, val_blk, precision=highest)
        hidden = hidden + carry_scale[..., None] * jnp.einsum('hvk,htk->htv', memory, query_blk, precision=highest)
        block_total = decay_logarithm[:, -1]
        tail_log = block_total[:, None] - decay_logarithm + gate_blk
        new_max = jnp.maximum(block_total + stab_max, lax.optimization_barrier(jnp.max(tail_log, axis=-1)))
        weights = jnp.exp(tail_log - new_max[:, None])
        carry_decay = jnp.exp(block_total + stab_max - new_max)
        memory = carry_decay[:, None, None] * memory + jnp.einsum('hs,hsv,hsk->hvk', weights, val_blk, key_blk, precision=highest)
        return ((memory, new_max), hidden)
    start_state = (jnp.zeros((H, DH, DH), jnp.float32), jnp.zeros((H,), jnp.float32))
    pieces = (to_blocks(queries), to_blocks(memory_keys), to_blocks(memory_values), to_blocks(input_preactivation), to_blocks(forget_logarithm))
    _, results = lax.scan(advance, start_state, pieces)
    return jnp.moveaxis(results, 0, 1).reshape(H, SEQ, DH)

def to_heads(tensor):
    return tensor.astype(jnp.float32).reshape(SEQ, H, DH).transpose(1, 0, 2)

def reference(queries, memory_keys, memory_values, output_preactivation, input_preactivation, forget_preactivation, extra_forget_terms, head_norm_gain, output_projection_matrix, residual, feedforward_norm_gain, feedforward_up_matrix, feedforward_down_matrix):
    forget_logarithm = jax.nn.log_sigmoid(forget_preactivation) + extra_forget_terms
    hidden = memory_cell(to_heads(queries), to_heads(memory_keys) * DH ** (-0.5), to_heads(memory_values), input_preactivation, forget_logarithm)
    hidden = hidden.transpose(1, 0, 2)
    gated = rms_norm(hidden, head_norm_gain) * jax.nn.sigmoid(output_preactivation.astype(jnp.float32).reshape(SEQ, H, DH))
    mixed = gated.reshape(SEQ, H * DH).astype(jnp.bfloat16)
    width_tp = H * DH // N_TP
    branch = jnp.zeros((SEQ, D), jnp.float32)
    for group_idx in range(N_TP):
        lower_col = group_idx * width_tp
        partial_value = jnp.dot(mixed[:, lower_col:lower_col + width_tp], output_projection_matrix[lower_col:lower_col + width_tp], preferred_element_type=jnp.float32)
        branch = branch + lax.optimization_barrier(partial_value.astype(jnp.bfloat16)).astype(jnp.float32)
    mid_state = (residual.astype(jnp.float32) + branch).astype(jnp.bfloat16)
    normed = rms_norm(mid_state.astype(jnp.float32), feedforward_norm_gain).astype(jnp.bfloat16)
    ff_tp = FF // N_TP
    mlp_sum = jnp.zeros((SEQ, D), jnp.float32)
    for group_idx in range(N_TP):
        lower_col = group_idx * ff_tp
        upward = jnp.dot(normed, feedforward_up_matrix[:, lower_col:lower_col + ff_tp], preferred_element_type=jnp.float32)
        active = jnp.square(jax.nn.relu(upward)).astype(jnp.bfloat16)
        partial_value = jnp.dot(active, feedforward_down_matrix[lower_col:lower_col + ff_tp], preferred_element_type=jnp.float32)
        mlp_sum = mlp_sum + lax.optimization_barrier(partial_value.astype(jnp.bfloat16)).astype(jnp.float32)
    return (mid_state.astype(jnp.float32) + mlp_sum).astype(jnp.bfloat16)
```

```python
import functools

import jax
import jax.numpy as jnp
from jax import lax
from jax.experimental import pallas as pl
from jax.experimental.pallas import tpu as pltpu
from jax.sharding import PartitionSpec as P

BLOCK = 128
EPS = 1e-06
NEG = -1e30
MESH = pl.DeviceIdType.MESH
F32 = jnp.float32
BF16 = jnp.bfloat16


def split_dot(exact, wide, swap=False):
    high = wide.astype(BF16)
    low = (wide - high.astype(F32)).astype(BF16)
    if swap:
        return jnp.dot(high, exact, preferred_element_type=F32) + jnp.dot(
            low, exact, preferred_element_type=F32
        )
    return jnp.dot(exact, high, preferred_element_type=F32) + jnp.dot(
        exact, low, preferred_element_type=F32
    )


def aligned(start, multiple):
    return start if isinstance(start, int) else pl.multiple_of(start, multiple)


def kernel(
    dims,
    q_hbm, k_hbm, v_hbm, o_hbm, igate_ref, fgate_ref, extra_ref, hgain_ref, wout_hbm, res_hbm,
    fgain_ref, up_hbm, down_hbm,
    out_ref,
    qb, kb, vb, ob, resb, upw, dnw, wo, mixed, mixin, mid, ntok, act, psend, precv, msend, xrecv, zsend, zrecv,
    own_acc, mlp, keyt, memp, hloc, gates, cols_ref, st_out, st_in,
    in_sem, loc_sem, wu_send, wu_recv, wuy_send, wd_send, wd_recv, wdy_send, wo_send, wo_recv, wop_send,
    st_send, st_recv, mx_send, mx_recv, t_recv, tz_send, tx_send, tr_send, f_send,
    p_send, p_recv, x_send, x_recv, z_send, z_recv,
):
    grp, sp, tp, heads, blocks, rows, group, usubs, dsubs, pieces = dims
    g, z, t = lax.axis_index("grp"), lax.axis_index("sp"), lax.axis_index("tp")
    half = tp // 2
    core, x = lax.rem(t, 2), t // 2
    partner = t + 1 - 2 * core
    zi = lax.rem(z, group)
    other = z + 1 - 2 * zi
    same = half * group
    place = x * group + zi
    mine = core * same + place
    width = ntok.shape[2]
    part = upw.shape[2]
    up_rows = upw.shape[1]
    out_cols = dnw.shape[2]
    n = out_cols // pieces
    urows = up_rows // grp // usubs
    drows = part // grp // dsubs

    def there(gg, zz, tt):
        return {"grp": gg, "sp": zz, "tp": tt}

    def remote(src, dst, send, recv, where):
        return pltpu.make_async_remote_copy(
            src_ref=src, dst_ref=dst, send_sem=send, recv_sem=recv, device_id=where, device_id_type=MESH
        )

    def nth(k):
        power = sp & (sp - 1) == 0
        if not power:
            return lax.rem(z + k, sp)
        gray_of = k
        total = 0
        bit = 1
        while bit < sp:
            mask = (gray_of // bit + gray_of // (2 * bit)) % 2
            zbit = lax.rem(z // bit, 2)
            total = total + (zbit + mask - 2 * zbit * mask) * bit
            bit *= 2
        return total

    def load(i, src, dst):
        return pltpu.make_async_copy(src, dst, in_sem.at[i])

    loads = [load(i, s, d) for i, (s, d) in enumerate(
        ((k_hbm, kb), (v_hbm, vb), (q_hbm, qb), (o_hbm, ob), (res_hbm, resb))
    )]
    for c in loads:
        c.start()

    barrier = pltpu.get_barrier_semaphore()
    for j in range(1, tp):
        pl.semaphore_signal(barrier, inc=1, device_id=there(g, z, lax.rem(t + j, tp)), device_id_type=MESH)
    for j in range(1, grp):
        pl.semaphore_signal(barrier, inc=1, device_id=there(lax.rem(g + j, grp), z, t), device_id_type=MESH)

    def greet(j, _):
        pl.semaphore_signal(barrier, inc=1, device_id=there(g, lax.rem(z + j, sp), t), device_id_type=MESH)
        return 0

    lax.fori_loop(1, sp, greet, 0)
    pl.semaphore_wait(barrier, tp + grp + sp - 3)

    def up_rows_of(c, s):
        return pl.ds(aligned(c * (urows * usubs) + s * urows, 16), urows)

    def down_rows_of(c, s):
        return pl.ds(aligned(c * (drows * dsubs) + s * drows, 16), drows)

    def up_copy(zz, s):
        return remote(
            up_hbm.at[up_rows_of(g, s), pl.ds(aligned(lax.rem(zz, group) * part, 128), part)],
            upw.at[z, up_rows_of(g, s), :],
            wu_send.at[zz, s], wu_recv.at[z, g, s], there(g, zz, t),
        )

    def down_copy(zz, s):
        first = lax.rem(zz, group) * part + g * (drows * dsubs) + s * drows
        return remote(
            down_hbm.at[pl.ds(aligned(first, 16), drows), :],
            dnw.at[z, down_rows_of(g, s), :],
            wd_send.at[zz, s], wd_recv.at[z, g, s], there(g, zz, t),
        )

    def up_pass(o, s, j):
        at = upw.at[o, up_rows_of(g, s), :]
        return remote(at, at, wuy_send.at[o, s, j], wu_recv.at[o, g, s], there(lax.rem(g + j, grp), z, t))

    def down_pass(o, s, j):
        at = dnw.at[o, down_rows_of(g, s), :]
        return remote(at, at, wdy_send.at[o, s, j], wd_recv.at[o, g, s], there(lax.rem(g + j, grp), z, t))

    def up_arrived(o, c, s):
        at = upw.at[o, up_rows_of(c, s), :]
        return remote(at, at, wuy_send.at[o, s, 0], wu_recv.at[o, c, s], there(g, z, t))

    def down_arrived(o, c, s):
        at = dnw.at[o, down_rows_of(c, s), :]
        return remote(at, at, wdy_send.at[o, s, 0], wd_recv.at[o, c, s], there(g, z, t))

    def relay_up(k):
        o = nth(k)
        for s in range(usubs):
            up_arrived(o, g, s).wait_recv()
            for j in range(1, grp):
                up_pass(o, s, j).start()

    def relay_down(k):
        o = nth(k)
        for s in range(dsubs):
            down_arrived(o, g, s).wait_recv()
            for j in range(1, grp):
                down_pass(o, s, j).start()

    def finish_up(k):
        o = nth(k)
        for s in range(usubs):
            for j in range(1, grp):
                up_arrived(o, lax.rem(g + j, grp), s).wait_recv()

    def finish_down(k):
        o = nth(k)
        for s in range(dsubs):
            for j in range(1, grp):
                down_arrived(o, lax.rem(g + j, grp), s).wait_recv()

    def right(copy, first, last, subs, when=True):
        def body(d, _):
            @pl.when((z + d < sp) & when)
            def _():
                for s in subs:
                    copy(z + d, s).start()

            return 0

        lax.fori_loop(first, last, body, 0)

    def left(copy, first, last, subs, when=True):
        def body(d, _):
            @pl.when((z - d >= 0) & when)
            def _():
                for s in subs:
                    copy(z - d, s).start()

            return 0

        lax.fori_loop(first, last, body, 0)

    us, ds = range(usubs), range(dsubs)
    held_right, held_left = zi == 0, zi == group - 1
    right(up_copy, 1, 2, us[:1])
    left(up_copy, 1, sp, us)
    left(down_copy, 1, sp, ds, zi != group - 1)
    left(down_copy, 1, 2, ds[: dsubs // 2], held_left)

    def wo_copy(tt):
        return remote(wout_hbm, wo.at[t], wo_send.at[tt], wo_recv.at[t], there(g, z, tt))

    def wo_pass(j):
        tt = lax.rem(x + j, half) * 2 + core
        return remote(wo.at[tt], wo.at[tt], wop_send.at[j], wo_recv.at[tt], there(g, z, partner))

    def wo_arrived(tt):
        return remote(wo.at[tt], wo.at[tt], wop_send.at[0], wo_recv.at[tt], there(g, z, partner))

    for j in range(1, half):
        wo_copy(lax.rem(x + j, half) * 2 + core).start()
    wo_copy(partner).start()
    own = [
        pltpu.make_async_copy(wout_hbm, wo.at[t], loc_sem.at[0]),
        pltpu.make_async_copy(up_hbm.at[:, pl.ds(aligned(zi * part, 128), part)], upw.at[z], loc_sem.at[1]),
        pltpu.make_async_copy(down_hbm.at[pl.ds(aligned(zi * part, 16), part), :], dnw.at[z], loc_sem.at[2]),
    ]
    for c in own:
        c.start()

    dh = qb.shape[1] // heads
    scale = dh ** (-0.5)
    count = heads * blocks
    pad = -count % 8

    def stacked(value):
        pieces_of = [
            value[h : h + 1, b * BLOCK : (b + 1) * BLOCK] for h in range(heads) for b in range(blocks)
        ]
        if pad:
            pieces_of.append(jnp.zeros((pad, BLOCK), F32))
        return jnp.concatenate(pieces_of, axis=0)

    pre = fgate_ref[...]
    log_forget = jnp.minimum(pre, 0.0) - jnp.log1p(jnp.exp(-jnp.abs(pre))) + extra_ref[...]
    cum_row = stacked(log_forget)
    lane = lax.broadcasted_iota(jnp.int32, cum_row.shape, 1)
    step = 1
    while step < BLOCK:
        cum_row = cum_row + jnp.where(lane >= step, pltpu.roll(cum_row, step, 1), 0.0)
        step *= 2
    rest_row = stacked(igate_ref[...]) - cum_row
    cum_col = cum_row.T
    rest_col = rest_row.T

    loads[0].wait()
    loads[1].wait()
    before, totals = {}, {}
    for h in range(heads):
        cols = pl.ds(h * dh, dh)
        run = None
        for b in range(blocks):
            i = h * blocks + b
            at = pl.ds(b * BLOCK, BLOCK)
            total = cum_row[i : i + 1, BLOCK - 1 : BLOCK]
            tail = total + rest_col[:, i : i + 1]
            tail_max = jnp.max(tail, axis=0, keepdims=True)
            weighted = vb[at, cols].astype(F32) * jnp.exp(tail - tail_max)
            key_t = kb[at, cols].astype(F32).T.astype(BF16)
            keyt[h, b] = key_t
            mem = split_dot(key_t, weighted) * scale
            if run is None:
                run = (total, tail_max, mem)
            else:
                before[h, b] = (run[0], run[1])
                memp[h, b] = run[2]
                new = jnp.maximum(total + run[1], tail_max)
                run = (
                    total + run[0],
                    new,
                    jnp.exp(total + run[1] - new) * run[2] + jnp.exp(tail_max - new) * mem,
                )
        st_out[h, :dh, :] = run[2]
        st_out[h, dh : dh + 8, :] = jnp.broadcast_to(run[1], (8, dh))
        st_out[h, dh + 8 : dh + 16, :] = jnp.broadcast_to(run[0], (8, dh))

    def state_copy():
        return remote(st_out, st_in, st_send, st_recv, there(g, z + 1, t))

    @pl.when(z == 0)
    def _():
        st_in[...] = jnp.zeros_like(st_in)

    def state_on():
        for h in range(heads):
            m_in = st_in[h, dh : dh + 1, :]
            m_loc = st_out[h, dh : dh + 1, :]
            total = st_out[h, dh + 8 : dh + 9, :]
            new = jnp.maximum(total + m_in, m_loc)
            st_out[h, :dh, :] = (
                jnp.exp(total + m_in - new) * st_in[h, :dh, :] + jnp.exp(m_loc - new) * st_out[h, :dh, :]
            )
            st_out[h, dh : dh + 8, :] = jnp.broadcast_to(new, (8, dh))
        state_copy().start()

    def rest_of_sends():
        right(up_copy, 1, 2, us[1:], z == 0)
        right(up_copy, 2, sp, us)
        right(down_copy, 1, sp, ds, zi != 0)

    right(up_copy, 1, 2, us[1:], z > 0)

    @pl.when((z == 0) & (sp > 1))
    def _():
        state_on()

    @pl.when(z == 0)
    def _():
        rest_of_sends()

    loads[2].wait()
    loads[3].wait()
    causal = lax.broadcasted_iota(jnp.int32, (BLOCK, BLOCK), 0) >= lax.broadcasted_iota(
        jnp.int32, (BLOCK, BLOCK), 1
    )
    gain = hgain_ref[...]

    def take_state(when):
        @pl.when(when)
        def _():
            state_copy().wait_recv()

            @pl.when(z < sp - 1)
            def _():
                state_on()

            rest_of_sends()

    for h in range(heads):
        cols = pl.ds(h * dh, dh)
        if h == heads - 1:
            take_state(z == 1)
        for b in range(blocks):
            i = h * blocks + b
            at = pl.ds(b * BLOCK, BLOCK)
            cum = cum_col[:, i : i + 1]
            query = qb[at, cols]
            log_weight = jnp.where(causal, cum + rest_row[i : i + 1, :], NEG)
            row_max = jnp.max(log_weight, axis=1, keepdims=True)
            base = cum
            if b > 0:
                past, stab = before[h, b]
                base = cum + past
                carry = cum + stab
                row_max = jnp.maximum(row_max, carry)
            scores = (
                jnp.dot(query, keyt[h, b], preferred_element_type=F32)
                * scale
                * jnp.exp(log_weight - row_max)
            )
            hidden = split_dot(vb[at, cols], scores, swap=True)
            if b > 0:
                hidden = hidden + jnp.exp(carry - row_max) * split_dot(query, memp[h, b])
            hloc[at, cols] = hidden
            cols_ref[at, 2 * h : 2 * h + 1] = row_max
            cols_ref[at, 2 * h + 1 : 2 * h + 2] = base
            gates[at, cols] = gain * (1.0 / (1.0 + jnp.exp(-ob[at, cols].astype(F32))))

    take_state(z > 1)
    if sp > 1:
        relay_up(1)
    for j in range(1, half):
        wo_arrived(lax.rem(x + j, half) * 2 + core).wait_recv()
        wo_pass(j).start()

    for h in range(heads):
        cols = pl.ds(h * dh, dh)
        memory = st_in[h, :dh, :]
        stab = st_in[h, dh : dh + 1, 0:1]
        for b in range(blocks):
            at = pl.ds(b * BLOCK, BLOCK)
            local_max = cols_ref[at, 2 * h : 2 * h + 1]
            carry = cols_ref[at, 2 * h + 1 : 2 * h + 2] + stab
            row_max = jnp.maximum(local_max, carry)
            hidden = jnp.exp(local_max - row_max) * hloc[at, cols] + jnp.exp(carry - row_max) * split_dot(
                qb[at, cols], memory
            )
            mean_sq = jnp.mean(hidden * hidden, axis=1, keepdims=True)
            mixed[at, cols] = (hidden * lax.rsqrt(mean_sq + EPS) * gates[at, cols]).astype(BF16)

    def mixed_copy(j):
        d = lax.rem(t + j, tp)
        return remote(
            mixed.at[pl.ds(aligned(d * rows, 16), rows), :],
            mixin.at[t], mx_send.at[j], mx_recv.at[t], there(g, z, d),
        )

    def mixed_arrived(tt):
        return remote(mixin.at[tt], mixin.at[tt], mx_send.at[0], mx_recv.at[tt], there(g, z, partner))

    for j in range(1, tp):
        mixed_copy(j).start()
    mixin[t] = mixed[pl.ds(aligned(t * rows, 16), rows), :]
    own[0].wait()
    loads[4].wait()
    for j in range(1, half):
        wo_arrived(lax.rem(x + j, half) * 2 + 1 - core).wait_recv()
    wo_arrived(partner).wait_recv()
    for j in range(1, tp):
        mixed_arrived(lax.rem(t + j, tp)).wait_recv()

    chunk = min(512, width)
    sum_sq = jnp.zeros((rows, 1), F32)
    for c in range(width // chunk):
        at = pl.ds(c * chunk, chunk)
        branch = jnp.zeros((rows, chunk), F32)
        for tt in range(tp):
            branch = branch + jnp.dot(mixin[tt], wo[tt, :, at], preferred_element_type=F32).astype(
                BF16
            ).astype(F32)
        value = (resb[:, at].astype(F32) + branch).astype(BF16)
        mid[:, at] = value
        wide = value.astype(F32)
        sum_sq = sum_sq + jnp.sum(wide * wide, axis=1, keepdims=True)
    factor = lax.rsqrt(sum_sq * (1.0 / width) + EPS)
    for c in range(width // chunk):
        at = pl.ds(c * chunk, chunk)
        ntok[mine, :, at] = (mid[:, at].astype(F32) * factor * fgain_ref[:, at]).astype(BF16)

    def slot_of(xx, zz):
        return core * same + xx * group + zz

    def token(slot, send, where):
        return remote(ntok.at[slot], ntok.at[slot], send, t_recv.at[slot], where)

    def to_pair():
        return token(mine, tz_send, there(g, other, t))

    def to_x(j):
        return token(mine, tx_send.at[j], there(g, z, lax.rem(x + j, half) * 2 + core))

    def pass_x(j):
        return token(slot_of(x, 1 - zi), tr_send.at[j], there(g, z, lax.rem(x + j, half) * 2 + core))

    def to_partner(xx, zz):
        slot = slot_of(xx, zz)
        return token(slot, f_send.at[xx * group + zz], there(g, z, partner))

    def arrived(slot):
        return token(slot, tz_send, there(g, z, partner))

    if group > 1:
        to_pair().start()
    for j in range(1, half):
        to_x(j).start()
    to_partner(x, zi).start()
    left(down_copy, 1, 2, ds[dsubs // 2 :], held_left)
    left(down_copy, 2, sp, ds, held_left)
    right(down_copy, 1, sp, ds, held_right)

    def relays_up(first, last):
        def body(k, _):
            relay_up(k)
            return 0

        lax.fori_loop(first, last, body, 0)

    middle = 2 + (sp - 2) // 2
    relays_up(2, middle)
    for j in range(1, half):
        xx = lax.rem(x + j, half)
        arrived(slot_of(xx, zi)).wait_recv()
        to_partner(xx, zi).start()
    if group > 1:
        arrived(slot_of(x, 1 - zi)).wait_recv()
        for j in range(1, half):
            pass_x(j).start()
        to_partner(x, 1 - zi).start()
    relays_up(middle, sp)
    own[1].wait()

    def all_up(k, _):
        finish_up(k)
        return 0

    lax.fori_loop(1, sp, all_up, 0)
    if group > 1:
        for j in range(1, half):
            xx = lax.rem(x + j, half)
            arrived(slot_of(xx, 1 - zi)).wait_recv()
            to_partner(xx, 1 - zi).start()

    def up_half(side):
        def up_step(i, _):
            at = pl.ds(side * same + i * 2, 2)
            value = ntok[at].reshape(2 * rows, width)
            y = jnp.dot(value, upw[...].reshape(width, part), preferred_element_type=F32)
            y = jnp.maximum(y, 0.0)
            act[at] = (y * y).astype(BF16).reshape(2, rows, part)
            return 0

        lax.fori_loop(0, same // 2, up_step, 0)

    up_half(core)
    for xx in range(half):
        for zz in range(group):
            arrived((1 - core) * same + xx * group + zz).wait_recv()
    up_half(1 - core)
    own[2].wait()

    def pre_copy(unit):
        return remote(
            psend.at[unit], precv.at[unit], p_send.at[unit], p_recv.at[unit], there(g, z, partner)
        )

    def x_copy(unit, j):
        xx = lax.rem(x + j, half)
        return remote(
            msend.at[unit, pl.ds(xx * group, group)], xrecv.at[unit, x],
            x_send.at[unit, j], x_recv.at[unit, x], there(g, z, xx * 2 + core),
        )

    def x_arrived(unit, xx):
        at = xrecv.at[unit, xx]
        return remote(at, at, x_send.at[unit, 0], x_recv.at[unit, xx], there(g, z, partner))

    def z_copy(unit):
        return remote(zsend.at[unit], zrecv.at[unit], z_send.at[unit], z_recv.at[unit], there(g, other, t))

    def multiply(m, c):
        k, parity = m // pieces, lax.rem(m, 2)
        o = nth(k)
        unit = o * pieces + c

        def product(side):
            value = act[pl.ds(side * same, same)].reshape(same * rows, part)
            return jnp.dot(value, dnw[o, :, c * n : (c + 1) * n], preferred_element_type=F32)

        psend[unit] = product(1 - core).astype(BF16).reshape(psend.shape[1:])
        pre_copy(unit).start()
        own_acc[parity] = product(core).reshape(psend.shape[1:])

    def unit_of(m):
        return nth(m // pieces) * pieces + lax.rem(m, pieces)

    def spread(m):
        unit = unit_of(m)
        pre_copy(unit).wait_recv()
        msend[unit] = (own_acc[lax.rem(m, 2)] + precv[unit].astype(F32)).astype(BF16)
        for j in range(1, half):
            x_copy(unit, j).start()
        xrecv[unit, x] = msend[unit, pl.ds(x * group, group)]

    def gathered(unit, zz):
        total = xrecv[unit, 0, zz].astype(F32)
        for xx in range(1, half):
            total = total + xrecv[unit, xx, zz].astype(F32)
        return total

    def hand_over(m):
        unit = unit_of(m)
        for j in range(1, half):
            x_arrived(unit, lax.rem(x + j, half)).wait_recv()
        if group > 1:
            zsend[unit] = gathered(unit, 1 - zi).astype(BF16)
            z_copy(unit).start()

    def stage(k, _):
        @pl.when(k > 0)
        def _():
            relay_down(k)
            finish_down(k)

        for c in range(pieces):
            m = k * pieces + c
            multiply(m, c)

            @pl.when(m >= 1)
            def _():
                spread(m - 1)

            @pl.when(m >= 2)
            def _():
                hand_over(m - 2)

        return 0

    lax.fori_loop(0, sp, stage, 0)
    units = sp * pieces
    spread(units - 1)
    if units > 1:
        hand_over(units - 2)
    hand_over(units - 1)

    direct = out_cols % 128 == 0 and n % 128 == 0

    def finish(m, _):
        unit = unit_of(m)
        total = gathered(unit, zi)
        if group > 1:
            z_copy(unit).wait_recv()
            total = total + zrecv[unit].astype(F32)
        if direct:
            at = pl.ds(aligned(unit * n, 128), n)
            out_ref[:, at] = (mid[:, at].astype(F32) + total).astype(BF16)
        else:
            mlp[unit] = total
        return 0

    lax.fori_loop(0, units, finish, 0)
    if not direct:
        for unit in range(units):
            at = pl.ds(unit * n, n)
            out_ref[:, at] = (mid[:, at].astype(F32) + mlp[unit]).astype(BF16)

    def drain(o, _):
        @pl.when(o != z)
        def _():
            for s in us:
                up_copy(o, s).wait_send()
                for j in range(1, grp):
                    up_pass(o, s, j).wait_send()
            for s in ds:
                down_copy(o, s).wait_send()
                for j in range(1, grp):
                    down_pass(o, s, j).wait_send()

        for c in range(pieces):
            unit = o * pieces + c
            pre_copy(unit).wait_send()
            for j in range(1, half):
                x_copy(unit, j).wait_send()
            if group > 1:
                z_copy(unit).wait_send()
        return 0

    lax.fori_loop(0, sp, drain, 0)
    for j in range(1, half):
        wo_copy(lax.rem(x + j, half) * 2 + core).wait_send()
        wo_pass(j).wait_send()
        to_x(j).wait_send()
        if group > 1:
            pass_x(j).wait_send()
    wo_copy(partner).wait_send()
    for j in range(1, tp):
        mixed_copy(j).wait_send()
    if group > 1:
        to_pair().wait_send()
    for xx in range(half):
        for zz in range(group):
            to_partner(xx, zz).wait_send()

    @pl.when(z < sp - 1)
    def _():
        state_copy().wait_send()


def shards(
    mesh_shape,
    queries, memory_keys, memory_values, output_preactivation, input_preactivation,
    forget_preactivation, extra_forget_terms, head_norm_gain, output_projection_matrix, residual,
    feedforward_norm_gain, feedforward_up_matrix, feedforward_down_matrix,
):
    grp, sp, tp = mesh_shape
    tokens, across = queries.shape
    heads = input_preactivation.shape[0]
    blocks = tokens // BLOCK
    dh = across // heads
    rows, width = residual.shape
    up_rows, hidden = feedforward_up_matrix.shape
    out_cols = feedforward_down_matrix.shape[1]
    group = 2 if sp % 2 == 0 else 1
    part = hidden // group
    usubs = 2 if up_rows % (32 * grp) == 0 else 1
    dsubs = 2
    pieces = 2 if out_cols % 256 == 0 else 1
    half = tp // 2
    same = half * group
    layer = tp * group
    units = sp * pieces
    n = out_cols // pieces

    vmem = pl.BlockSpec(memory_space=pltpu.VMEM)
    hbm = pl.BlockSpec(memory_space=pl.ANY)
    dma = pltpu.SemaphoreType.DMA
    return pl.pallas_call(
        functools.partial(
            kernel, (grp, sp, tp, heads, blocks, rows, group, usubs, dsubs, pieces)
        ),
        out_shape=jax.ShapeDtypeStruct((rows, width), BF16),
        in_specs=[hbm] * 4 + [vmem] * 4 + [hbm] * 2 + [vmem] + [hbm] * 2,
        out_specs=vmem,
        scratch_shapes=[
            pltpu.VMEM((tokens, across), BF16),
            pltpu.VMEM((tokens, across), BF16),
            pltpu.VMEM((tokens, across), BF16),
            pltpu.VMEM((tokens, across), BF16),
            pltpu.VMEM((rows, width), BF16),
            pltpu.VMEM((sp, up_rows, part), BF16),
            pltpu.VMEM((sp, part, out_cols), BF16),
            pltpu.VMEM((tp, across, width), BF16),
            pltpu.VMEM((tokens, across), BF16),
            pltpu.VMEM((tp, rows, across), BF16),
            pltpu.VMEM((rows, width), BF16),
            pltpu.VMEM((layer, rows, width), BF16),
            pltpu.VMEM((layer, rows, part), BF16),
            pltpu.VMEM((units, same, rows, n), BF16),
            pltpu.VMEM((units, same, rows, n), BF16),
            pltpu.VMEM((units, same, rows, n), BF16),
            pltpu.VMEM((units, half, group, rows, n), BF16),
            pltpu.VMEM((units, rows, n), BF16),
            pltpu.VMEM((units, rows, n), BF16),
            pltpu.VMEM((2, same, rows, n), F32),
            pltpu.VMEM((units, rows, n) if n % 128 else (1, 8, 128), F32),
            pltpu.VMEM((heads, blocks, dh, BLOCK), BF16),
            pltpu.VMEM((heads, blocks, dh, dh), F32),
            pltpu.VMEM((tokens, across), F32),
            pltpu.VMEM((tokens, across), F32),
            pltpu.VMEM((tokens, 128), F32),
            pltpu.VMEM((heads, dh + 16, dh), F32),
            pltpu.VMEM((heads, dh + 16, dh), F32),
            dma((5,)),
            dma((3,)),
            dma((sp, usubs)),
            dma((sp, grp, usubs)),
            dma((sp, usubs, grp)),
            dma((sp, dsubs)),
            dma((sp, grp, dsubs)),
            dma((sp, dsubs, grp)),
            dma((tp,)),
            dma((tp,)),
            dma((half,)),
            dma,
            dma,
            dma((tp,)),
            dma((tp,)),
            dma((layer,)),
            dma,
            dma((half,)),
            dma((half,)),
            dma((same,)),
            dma((units,)),
            dma((units,)),
            dma((units, half)),
            dma((units, half)),
            dma((units,)),
            dma((units,)),
        ],
        compiler_params=pltpu.CompilerParams(
            collective_id=0, has_side_effects=True, vmem_limit_bytes=60 * 1024 * 1024
        ),
    )(
        queries, memory_keys, memory_values, output_preactivation,
        input_preactivation, forget_preactivation, extra_forget_terms,
        head_norm_gain.reshape(1, dh), output_projection_matrix, residual,
        feedforward_norm_gain.reshape(1, width), feedforward_up_matrix, feedforward_down_matrix,
    )


def solution(mesh):
    in_specs = (
        P(("grp", "sp"), "tp"),
        P(("grp", "sp"), "tp"),
        P(("grp", "sp"), "tp"),
        P(("grp", "sp"), "tp"),
        P("tp", ("grp", "sp")),
        P("tp", ("grp", "sp")),
        P("tp", ("grp", "sp")),
        P(),
        P("tp", None),
        P(("grp", "sp", "tp"), None),
        P(),
        P("sp", "tp"),
        P("tp", "sp"),
    )
    out_specs = P(("grp", "sp", "tp"), None)
    shape = (mesh.shape["grp"], mesh.shape["sp"], mesh.shape["tp"])
    return jax.shard_map(
        functools.partial(shards, shape),
        mesh=mesh,
        in_specs=in_specs,
        out_specs=out_specs,
        check_vma=False,
    )
```

```python
import functools

import jax
import jax.numpy as jnp
from jax import lax
from jax.experimental import pallas as pl
from jax.experimental.pallas import tpu as pltpu
from jax.sharding import PartitionSpec as P

BLOCK = 128
EPS = 1e-06
NEG = -1e30
MESH = pl.DeviceIdType.MESH
F32 = jnp.float32
BF16 = jnp.bfloat16


def split_dot(exact, wide, swap=False):
    high = wide.astype(BF16)
    low = (wide - high.astype(F32)).astype(BF16)
    if swap:
        return jnp.dot(high, exact, preferred_element_type=F32) + jnp.dot(
            low, exact, preferred_element_type=F32
        )
    return jnp.dot(exact, high, preferred_element_type=F32) + jnp.dot(
        exact, low, preferred_element_type=F32
    )


def aligned(start, multiple):
    return start if isinstance(start, int) else pl.multiple_of(start, multiple)


def kernel(
    dims,
    q_hbm, k_hbm, v_hbm, o_hbm, igate_ref, fgate_ref, extra_ref, hgain_ref, wout_hbm, res_hbm,
    fgain_ref, up_hbm, down_hbm,
    out_ref,
    qb, kb, vb, ob, resb, upw, dnw, wo, mixed, mixin, mid, ntok, act, psend, precv, msend, xrecv, zsend, zrecv,
    own_acc, mlp, keyt, memp, hloc, gates, cols_ref, st_out, st_in,
    in_sem, loc_sem, wu_send, wu_recv, wuy_send, wd_send, wd_recv, wdy_send, wo_send, wo_recv, wop_send,
    st_send, st_recv, mx_send, mx_recv, t_recv, tz_send, tx_send, tr_send, f_send,
    p_send, p_recv, x_send, x_recv, z_send, z_recv,
):
    grp, sp, tp, heads, blocks, rows, group, usubs, rsubs, pieces, tsubs = dims
    g, z, t = lax.axis_index("grp"), lax.axis_index("sp"), lax.axis_index("tp")
    half = tp // 2
    core, x = lax.rem(t, 2), t // 2
    partner = t + 1 - 2 * core
    zi = lax.rem(z, group)
    other = z + 1 - 2 * zi
    same = half * group
    mine = core * same + zi * half + x
    edge = (z == 0) | (z == sp - 1)
    dsubs = rsubs * pieces
    width = ntok.shape[2]
    part = upw.shape[2]
    up_rows = upw.shape[1]
    out_cols = dnw.shape[2]
    n = out_cols // pieces
    urows = up_rows // grp // usubs
    drows = part // grp // rsubs
    trows = rows // tsubs

    def there(gg, zz, tt):
        return {"grp": gg, "sp": zz, "tp": tt}

    def remote(src, dst, send, recv, where):
        return pltpu.make_async_remote_copy(
            src_ref=src, dst_ref=dst, send_sem=send, recv_sem=recv, device_id=where, device_id_type=MESH
        )

    def nth(k):
        power = sp & (sp - 1) == 0
        if not power:
            return lax.rem(z + k, sp)
        gray_of = k
        total = 0
        bit = 1
        while bit < sp:
            mask = (gray_of // bit + gray_of // (2 * bit)) % 2
            zbit = lax.rem(z // bit, 2)
            total = total + (zbit + mask - 2 * zbit * mask) * bit
            bit *= 2
        return total

    def load(i, src, dst):
        return pltpu.make_async_copy(src, dst, in_sem.at[i])

    loads = [load(i, s, d) for i, (s, d) in enumerate(
        ((k_hbm, kb), (v_hbm, vb), (q_hbm, qb), (o_hbm, ob), (res_hbm, resb))
    )]
    for c in loads:
        c.start()

    barrier = pltpu.get_barrier_semaphore()
    for j in range(1, tp):
        pl.semaphore_signal(barrier, inc=1, device_id=there(g, z, lax.rem(t + j, tp)), device_id_type=MESH)
    for j in range(1, grp):
        pl.semaphore_signal(barrier, inc=1, device_id=there(lax.rem(g + j, grp), z, t), device_id_type=MESH)

    def greet(j, _):
        pl.semaphore_signal(barrier, inc=1, device_id=there(g, lax.rem(z + j, sp), t), device_id_type=MESH)
        return 0

    lax.fori_loop(1, sp, greet, 0)
    pl.semaphore_wait(barrier, tp + grp + sp - 3)

    def up_rows_of(c, s):
        return pl.ds(aligned(c * (urows * usubs) + s * urows, 16), urows)

    def down_at(c, s):
        rows_at = pl.ds(aligned(c * (drows * rsubs) + s % rsubs * drows, 16), drows)
        return rows_at, pl.ds(s // rsubs * n, n)

    def up_copy(zz, s):
        return remote(
            up_hbm.at[up_rows_of(g, s), pl.ds(aligned(lax.rem(zz, group) * part, 128), part)],
            upw.at[z, up_rows_of(g, s), :],
            wu_send.at[zz, s], wu_recv.at[z, g, s], there(g, zz, t),
        )

    def down_copy(zz, s):
        first = lax.rem(zz, group) * part + g * (drows * rsubs) + s % rsubs * drows
        return remote(
            down_hbm.at[pl.ds(aligned(first, 16), drows), pl.ds(s // rsubs * n, n)],
            dnw.at[(z, *down_at(g, s))],
            wd_send.at[zz, s], wd_recv.at[z, g, s], there(g, zz, t),
        )

    def up_pass(o, s, j):
        at = upw.at[o, up_rows_of(g, s), :]
        return remote(at, at, wuy_send.at[o, s, j], wu_recv.at[o, g, s], there(lax.rem(g + j, grp), z, t))

    def down_pass(o, s, j):
        at = dnw.at[(o, *down_at(g, s))]
        return remote(at, at, wdy_send.at[o, s, j], wd_recv.at[o, g, s], there(lax.rem(g + j, grp), z, t))

    def up_arrived(o, c, s):
        at = upw.at[o, up_rows_of(c, s), :]
        return remote(at, at, wuy_send.at[o, s, 0], wu_recv.at[o, c, s], there(g, z, t))

    def down_arrived(o, c, s):
        at = dnw.at[(o, *down_at(c, s))]
        return remote(at, at, wdy_send.at[o, s, 0], wd_recv.at[o, c, s], there(g, z, t))

    def relay_up(k):
        o = nth(k)
        for s in range(usubs):
            up_arrived(o, g, s).wait_recv()
            for j in range(1, grp):
                up_pass(o, s, j).start()

    def of_piece(c):
        return range(c * rsubs, (c + 1) * rsubs)

    def relay_down(k, c):
        o = nth(k)
        for s in of_piece(c):
            down_arrived(o, g, s).wait_recv()
            for j in range(1, grp):
                down_pass(o, s, j).start()

    def finish_up(k):
        o = nth(k)
        for s in range(usubs):
            for j in range(1, grp):
                up_arrived(o, lax.rem(g + j, grp), s).wait_recv()

    def finish_down(k, c):
        o = nth(k)
        for s in of_piece(c):
            for j in range(1, grp):
                down_arrived(o, lax.rem(g + j, grp), s).wait_recv()

    def right(copy, first, last, subs, when=True, flip=False):
        def body(i, _):
            d = first + last - 1 - i if flip else i

            @pl.when((z + d < sp) & when)
            def _():
                for s in subs:
                    copy(z + d, s).start()

            return 0

        lax.fori_loop(first, last, body, 0)

    def left(copy, first, last, subs, when=True, flip=False):
        def body(i, _):
            d = first + last - 1 - i if flip else i

            @pl.when((z - d >= 0) & when)
            def _():
                for s in subs:
                    copy(z - d, s).start()

            return 0

        lax.fori_loop(first, last, body, 0)

    us, ds = range(usubs), range(dsubs)
    far_right, far_left = z + 2 < sp, z - 2 >= 0
    held_right = (zi == 0) & far_right
    held_left = (zi == group - 1) & far_left
    free_right = (zi != 0) | (z + 2 >= sp)
    free_left = (zi != group - 1) | (z - 2 < 0)
    right(up_copy, 1, 2, us[:1], z > 0)
    away_left, away_right = zi != group - 1, zi != 0
    left(up_copy, 1, 2, us)
    left(up_copy, 2, sp, us, zi == group - 1)
    left(down_copy, 1, sp, ds, free_left & jnp.logical_not(away_left))

    def wo_copy(tt):
        return remote(wout_hbm, wo.at[t], wo_send.at[tt], wo_recv.at[t], there(g, z, tt))

    def wo_pass(j):
        tt = lax.rem(x + j, half) * 2 + core
        return remote(wo.at[tt], wo.at[tt], wop_send.at[j], wo_recv.at[tt], there(g, z, partner))

    def wo_arrived(tt):
        return remote(wo.at[tt], wo.at[tt], wop_send.at[0], wo_recv.at[tt], there(g, z, partner))

    for j in range(1, half):
        wo_copy(lax.rem(x + j, half) * 2 + core).start()
    wo_copy(partner).start()
    own = [
        pltpu.make_async_copy(wout_hbm, wo.at[t], loc_sem.at[0]),
        pltpu.make_async_copy(up_hbm.at[:, pl.ds(aligned(zi * part, 128), part)], upw.at[z], loc_sem.at[1]),
        pltpu.make_async_copy(down_hbm.at[pl.ds(aligned(zi * part, 16), part), :], dnw.at[z], loc_sem.at[2]),
    ]
    for c in own:
        c.start()

    dh = qb.shape[1] // heads
    scale = dh ** (-0.5)
    count = heads * blocks
    pad = -count % 8

    def stacked(value):
        pieces_of = [
            value[h : h + 1, b * BLOCK : (b + 1) * BLOCK] for h in range(heads) for b in range(blocks)
        ]
        if pad:
            pieces_of.append(jnp.zeros((pad, BLOCK), F32))
        return jnp.concatenate(pieces_of, axis=0)

    pre = fgate_ref[...]
    log_forget = jnp.minimum(pre, 0.0) - jnp.log1p(jnp.exp(-jnp.abs(pre))) + extra_ref[...]
    cum_row = stacked(log_forget)
    lane = lax.broadcasted_iota(jnp.int32, cum_row.shape, 1)
    step = 1
    while step < BLOCK:
        cum_row = cum_row + jnp.where(lane >= step, pltpu.roll(cum_row, step, 1), 0.0)
        step *= 2
    rest_row = stacked(igate_ref[...]) - cum_row
    cum_col = cum_row.T
    rest_col = rest_row.T

    loads[0].wait()
    loads[1].wait()
    before, totals = {}, {}
    for h in range(heads):
        cols = pl.ds(h * dh, dh)
        run = None
        for b in range(blocks):
            i = h * blocks + b
            at = pl.ds(b * BLOCK, BLOCK)
            total = cum_row[i : i + 1, BLOCK - 1 : BLOCK]
            tail = total + rest_col[:, i : i + 1]
            tail_max = jnp.max(tail, axis=0, keepdims=True)
            weighted = vb[at, cols].astype(F32) * jnp.exp(tail - tail_max)
            key_t = kb[at, cols].astype(F32).T.astype(BF16)
            keyt[h, b] = key_t
            mem = split_dot(key_t, weighted) * scale
            if run is None:
                run = (total, tail_max, mem)
            else:
                before[h, b] = (run[0], run[1])
                memp[h, b] = run[2]
                new = jnp.maximum(total + run[1], tail_max)
                run = (
                    total + run[0],
                    new,
                    jnp.exp(total + run[1] - new) * run[2] + jnp.exp(tail_max - new) * mem,
                )
        st_out[h, :dh, :] = run[2]
        st_out[h, dh : dh + 8, :] = jnp.broadcast_to(run[1], (8, dh))
        st_out[h, dh + 8 : dh + 16, :] = jnp.broadcast_to(run[0], (8, dh))

    def state_copy():
        return remote(st_out, st_in, st_send, st_recv, there(g, z + 1, t))

    @pl.when(z == 0)
    def _():
        st_in[...] = jnp.zeros_like(st_in)

    def state_on():
        for h in range(heads):
            m_in = st_in[h, dh : dh + 1, :]
            m_loc = st_out[h, dh : dh + 1, :]
            total = st_out[h, dh + 8 : dh + 9, :]
            new = jnp.maximum(total + m_in, m_loc)
            st_out[h, :dh, :] = (
                jnp.exp(total + m_in - new) * st_in[h, :dh, :] + jnp.exp(m_loc - new) * st_out[h, :dh, :]
            )
            st_out[h, dh : dh + 8, :] = jnp.broadcast_to(new, (8, dh))
        state_copy().start()

    def rest_of_sends():
        right(up_copy, 1, 2, us, z == 0)
        right(up_copy, 2, sp, us)
        right(down_copy, 1, 2, ds[:rsubs], free_right & (z == 0))
        right(down_copy, 1, 2, ds[rsubs:], free_right & (zi == 0))

    right(up_copy, 1, 2, us[1:], z > 0)
    right(down_copy, 1, 2, ds[:rsubs], free_right & (zi == 0) & (z > 0))

    @pl.when((z == 0) & (sp > 1))
    def _():
        state_on()

    @pl.when(z == 0)
    def _():
        rest_of_sends()

    loads[2].wait()
    loads[3].wait()
    causal = lax.broadcasted_iota(jnp.int32, (BLOCK, BLOCK), 0) >= lax.broadcasted_iota(
        jnp.int32, (BLOCK, BLOCK), 1
    )
    gain = hgain_ref[...]

    def take_state(when):
        @pl.when(when)
        def _():
            state_copy().wait_recv()

            @pl.when(z < sp - 1)
            def _():
                state_on()

            rest_of_sends()

    for h in range(heads):
        cols = pl.ds(h * dh, dh)
        if h == heads - 1:
            take_state(z == 1)
        for b in range(blocks):
            i = h * blocks + b
            at = pl.ds(b * BLOCK, BLOCK)
            cum = cum_col[:, i : i + 1]
            query = qb[at, cols]
            log_weight = jnp.where(causal, cum + rest_row[i : i + 1, :], NEG)
            row_max = jnp.max(log_weight, axis=1, keepdims=True)
            base = cum
            if b > 0:
                past, stab = before[h, b]
                base = cum + past
                carry = cum + stab
                row_max = jnp.maximum(row_max, carry)
            scores = (
                jnp.dot(query, keyt[h, b], preferred_element_type=F32)
                * scale
                * jnp.exp(log_weight - row_max)
            )
            hidden = split_dot(vb[at, cols], scores, swap=True)
            if b > 0:
                hidden = hidden + jnp.exp(carry - row_max) * split_dot(query, memp[h, b])
            hloc[at, cols] = hidden
            cols_ref[at, 2 * h : 2 * h + 1] = row_max
            cols_ref[at, 2 * h + 1 : 2 * h + 2] = base
            gates[at, cols] = gain * (1.0 / (1.0 + jnp.exp(-ob[at, cols].astype(F32))))

    take_state(z > 1)
    for h in range(heads):
        cols = pl.ds(h * dh, dh)
        memory = st_in[h, :dh, :]
        stab = st_in[h, dh : dh + 1, 0:1]
        for b in range(blocks):
            at = pl.ds(b * BLOCK, BLOCK)
            local_max = cols_ref[at, 2 * h : 2 * h + 1]
            carry = cols_ref[at, 2 * h + 1 : 2 * h + 2] + stab
            row_max = jnp.maximum(local_max, carry)
            hidden = jnp.exp(local_max - row_max) * hloc[at, cols] + jnp.exp(carry - row_max) * split_dot(
                qb[at, cols], memory
            )
            mean_sq = jnp.mean(hidden * hidden, axis=1, keepdims=True)
            mixed[at, cols] = (hidden * lax.rsqrt(mean_sq + EPS) * gates[at, cols]).astype(BF16)

    def mixed_copy(j):
        d = lax.rem(t + j, tp)
        return remote(
            mixed.at[pl.ds(aligned(d * rows, 16), rows), :],
            mixin.at[t], mx_send.at[j], mx_recv.at[t], there(g, z, d),
        )

    def mixed_arrived(tt):
        return remote(mixin.at[tt], mixin.at[tt], mx_send.at[0], mx_recv.at[tt], there(g, z, partner))

    for j in range(1, tp):
        mixed_copy(j).start()
    mixin[t] = mixed[pl.ds(aligned(t * rows, 16), rows), :]
    left(up_copy, 2, sp, us, away_left)
    def relays_up(first, last):
        def body(k, _):
            relay_up(k)
            return 0

        lax.fori_loop(first, last, body, 0)

    def relays_down(k):
        for c in range(pieces):
            relay_down(k, c)

    middle = min(sp, 2 + (sp - 2) // 2)
    relays_up(1, min(2, sp))

    for j in range(1, half):
        wo_arrived(lax.rem(x + j, half) * 2 + core).wait_recv()
        wo_pass(j).start()

    own[0].wait()
    loads[4].wait()
    for j in range(1, half):
        wo_arrived(lax.rem(x + j, half) * 2 + 1 - core).wait_recv()
    wo_arrived(partner).wait_recv()
    for j in range(1, tp):
        mixed_arrived(lax.rem(t + j, tp)).wait_recv()

    chunk = min(512, width)
    sum_sq = jnp.zeros((rows, 1), F32)
    for c in range(width // chunk):
        at = pl.ds(c * chunk, chunk)
        branch = jnp.zeros((rows, chunk), F32)
        for tt in range(tp):
            branch = branch + jnp.dot(mixin[tt], wo[tt, :, at], preferred_element_type=F32).astype(
                BF16
            ).astype(F32)
        value = (resb[:, at].astype(F32) + branch).astype(BF16)
        mid[:, at] = value
        wide = value.astype(F32)
        sum_sq = sum_sq + jnp.sum(wide * wide, axis=1, keepdims=True)
    factor = lax.rsqrt(sum_sq * (1.0 / width) + EPS)
    for c in range(width // chunk):
        at = pl.ds(c * chunk, chunk)
        ntok[mine, :, at] = (mid[:, at].astype(F32) * factor * fgain_ref[:, at]).astype(BF16)

    def slot_of(xx, zz):
        return core * same + zz * half + xx

    def token(slot, s, send, where):
        at = ntok.at[slot, pl.ds(s * trows, trows), :]
        return remote(at, at, send, t_recv.at[slot, s], where)

    def to_pair(s):
        return token(mine, s, tz_send.at[s], there(g, other, t))

    def to_x(j, s):
        return token(mine, s, tx_send.at[j, s], there(g, z, lax.rem(x + j, half) * 2 + core))

    def pass_x(j, s):
        where = there(g, z, lax.rem(x + j, half) * 2 + core)
        return token(slot_of(x, 1 - zi), s, tr_send.at[j, s], where)

    def to_partner(xx, zz, s):
        return token(slot_of(xx, zz), s, f_send.at[zz * half + xx, s], there(g, z, partner))

    def arrived(slot, s):
        return token(slot, s, tz_send.at[s], there(g, z, partner))

    ts = range(tsubs)

    def give(xx, zz):
        for s in ts:
            to_partner(xx, zz, s).start()

    def take(slot):
        for s in ts:
            arrived(slot, s).wait_recv()

    for s in ts:
        if group > 1:
            to_pair(s).start()
    for j in range(1, half):
        for s in ts:
            to_x(j, s).start()
    give(x, zi)
    left(down_copy, 1, sp, ds, away_left)
    right(down_copy, 1, sp, ds, away_right)
    left(down_copy, 1, 2, ds, held_left)
    right(down_copy, 1, 2, ds, held_right)
    left(down_copy, 2, sp, ds, held_left, flip=True)
    right(down_copy, 2, sp, ds, held_right, flip=True)

    def relays_up(first, last):
        def body(k, _):
            relay_up(k)
            return 0

        lax.fori_loop(first, last, body, 0)

    @pl.when(edge)
    def _():
        relays_up(2, middle)

    @pl.when(jnp.logical_not(edge))
    def _():
        relays_up(2, sp)

    for j in range(1, half):
        xx = lax.rem(x + j, half)
        take(slot_of(xx, zi))
        give(xx, zi)

    @pl.when(edge)
    def _():
        relays_up(middle, sp)
        if sp > 1:
            relays_down(1)

    if group > 1:
        for s in ts:
            arrived(slot_of(x, 1 - zi), s).wait_recv()
            for j in range(1, half):
                pass_x(j, s).start()
        give(x, 1 - zi)
    own[1].wait()

    def all_up(k, _):
        finish_up(k)
        return 0

    lax.fori_loop(1, sp, all_up, 0)

    def up_quarter(side, zz):
        at = pl.ds(side * same + zz * half, half)
        value = ntok[at].reshape(half * rows, width)
        y = jnp.dot(value, upw[...].reshape(width, part), preferred_element_type=F32)
        y = jnp.maximum(y, 0.0)
        act[at] = (y * y).astype(BF16).reshape(half, rows, part)

    def up_step(i, _):
        side = core + (1 - 2 * core) * lax.rem(i, 2)
        zz = zi + (1 - 2 * zi) * (i // 2)

        @pl.when(i == 1)
        def _():
            for xx in range(half):
                take((1 - core) * same + zi * half + xx)

        if group > 1:
            @pl.when(i == 2)
            def _():
                for j in range(1, half):
                    xx = lax.rem(x + j, half)
                    take(slot_of(xx, 1 - zi))
                    give(xx, 1 - zi)

            @pl.when(i == 3)
            def _():
                for xx in range(half):
                    take((1 - core) * same + (1 - zi) * half + xx)

        up_quarter(side, zz)
        return 0

    lax.fori_loop(0, 2 * group, up_step, 0)
    early = min(3, sp)

    @pl.when(jnp.logical_not(edge))
    def _():
        for k in range(1, early):
            relays_down(k)

    own[2].wait()

    def pre_copy(unit):
        return remote(
            psend.at[unit], precv.at[unit], p_send.at[unit], p_recv.at[unit], there(g, z, partner)
        )

    def x_copy(unit, j):
        xx = lax.rem(x + j, half)
        return remote(
            msend.at[unit, :, xx], xrecv.at[unit, x],
            x_send.at[unit, j], x_recv.at[unit, x], there(g, z, xx * 2 + core),
        )

    def x_arrived(unit, xx):
        at = xrecv.at[unit, xx]
        return remote(at, at, x_send.at[unit, 0], x_recv.at[unit, xx], there(g, z, partner))

    def z_copy(unit):
        return remote(zsend.at[unit], zrecv.at[unit], z_send.at[unit], z_recv.at[unit], there(g, other, t))

    def multiply(unit, o, c):
        def product(side):
            value = act[pl.ds(side * same, same)].reshape(same * rows, part)
            return jnp.dot(value, dnw[o, :, c * n : (c + 1) * n], preferred_element_type=F32)

        psend[unit] = product(1 - core).astype(BF16).reshape(psend.shape[1:])
        pre_copy(unit).start()
        own_acc[...] = product(core).reshape(own_acc.shape)

    def unit_of(m):
        return nth(m // pieces) * pieces + lax.rem(m, pieces)

    def spread(unit):
        pre_copy(unit).wait_recv()
        msend[unit] = (own_acc[...] + precv[unit].astype(F32)).astype(BF16).reshape(msend.shape[1:])
        for j in range(1, half):
            x_copy(unit, j).start()
        for zz in range(group):
            xrecv[unit, x, zz] = msend[unit, zz, x]

    def gathered(unit, zz):
        total = xrecv[unit, 0, zz].astype(F32)
        for xx in range(1, half):
            total = total + xrecv[unit, xx, zz].astype(F32)
        return total

    def hand_over(m):
        unit = unit_of(m)
        for j in range(1, half):
            x_arrived(unit, lax.rem(x + j, half)).wait_recv()
        if group > 1:
            zsend[unit] = gathered(unit, 1 - zi).astype(BF16)
            z_copy(unit).start()

    def stage(k, _):
        o = nth(k)
        for c in range(pieces):
            m = k * pieces + c

            ahead, piece = (k, c + 1) if c + 1 < pieces else (k + 1, 0)

            @pl.when((ahead >= jnp.where(edge, 2, early)) & (ahead < sp))
            def _():
                relay_down(ahead, piece)

            @pl.when(k > 0)
            def _():
                finish_down(k, c)

            multiply(o * pieces + c, o, c)
            spread(o * pieces + c)

            @pl.when(m >= 2)
            def _():
                hand_over(m - 2)

        return 0

    lax.fori_loop(0, sp, stage, 0)
    units = sp * pieces
    if units > 1:
        hand_over(units - 2)
    hand_over(units - 1)

    direct = out_cols % 128 == 0 and n % 128 == 0

    def finish(m, _):
        unit = unit_of(m)
        total = gathered(unit, zi)
        if group > 1:
            z_copy(unit).wait_recv()
            total = total + zrecv[unit].astype(F32)
        if direct:
            at = pl.ds(aligned(unit * n, 128), n)
            out_ref[:, at] = (mid[:, at].astype(F32) + total).astype(BF16)
        else:
            mlp[unit] = total
        return 0

    lax.fori_loop(0, units, finish, 0)
    if not direct:
        for unit in range(units):
            at = pl.ds(unit * n, n)
            out_ref[:, at] = (mid[:, at].astype(F32) + mlp[unit]).astype(BF16)

    def drain(o, _):
        @pl.when(o != z)
        def _():
            for s in us:
                up_copy(o, s).wait_send()
                for j in range(1, grp):
                    up_pass(o, s, j).wait_send()
            for s in ds:
                down_copy(o, s).wait_send()
                for j in range(1, grp):
                    down_pass(o, s, j).wait_send()

        for c in range(pieces):
            unit = o * pieces + c
            pre_copy(unit).wait_send()
            for j in range(1, half):
                x_copy(unit, j).wait_send()
            if group > 1:
                z_copy(unit).wait_send()
        return 0

    lax.fori_loop(0, sp, drain, 0)
    for j in range(1, half):
        wo_copy(lax.rem(x + j, half) * 2 + core).wait_send()
        wo_pass(j).wait_send()
        for s in ts:
            to_x(j, s).wait_send()
            if group > 1:
                pass_x(j, s).wait_send()
    wo_copy(partner).wait_send()
    for j in range(1, tp):
        mixed_copy(j).wait_send()
    for s in ts:
        if group > 1:
            to_pair(s).wait_send()
        for xx in range(half):
            for zz in range(group):
                to_partner(xx, zz, s).wait_send()

    @pl.when(z < sp - 1)
    def _():
        state_copy().wait_send()


def shards(
    mesh_shape,
    queries, memory_keys, memory_values, output_preactivation, input_preactivation,
    forget_preactivation, extra_forget_terms, head_norm_gain, output_projection_matrix, residual,
    feedforward_norm_gain, feedforward_up_matrix, feedforward_down_matrix,
):
    grp, sp, tp = mesh_shape
    tokens, across = queries.shape
    heads = input_preactivation.shape[0]
    blocks = tokens // BLOCK
    dh = across // heads
    rows, width = residual.shape
    up_rows, hidden = feedforward_up_matrix.shape
    out_cols = feedforward_down_matrix.shape[1]
    group = 2 if sp % 2 == 0 else 1
    part = hidden // group
    usubs = 2 if up_rows % (32 * grp) == 0 else 1
    pieces = 2 if out_cols % 256 == 0 else 1
    rsubs = 2
    dsubs = rsubs * pieces
    tsubs = 4 if rows % 64 == 0 else 1
    half = tp // 2
    same = half * group
    layer = tp * group
    units = sp * pieces
    n = out_cols // pieces

    vmem = pl.BlockSpec(memory_space=pltpu.VMEM)
    hbm = pl.BlockSpec(memory_space=pl.ANY)
    dma = pltpu.SemaphoreType.DMA
    return pl.pallas_call(
        functools.partial(
            kernel, (grp, sp, tp, heads, blocks, rows, group, usubs, rsubs, pieces, tsubs)
        ),
        out_shape=jax.ShapeDtypeStruct((rows, width), BF16),
        in_specs=[hbm] * 4 + [vmem] * 4 + [hbm] * 2 + [vmem] + [hbm] * 2,
        out_specs=vmem,
        scratch_shapes=[
            pltpu.VMEM((tokens, across), BF16),
            pltpu.VMEM((tokens, across), BF16),
            pltpu.VMEM((tokens, across), BF16),
            pltpu.VMEM((tokens, across), BF16),
            pltpu.VMEM((rows, width), BF16),
            pltpu.VMEM((sp, up_rows, part), BF16),
            pltpu.VMEM((sp, part, out_cols), BF16),
            pltpu.VMEM((tp, across, width), BF16),
            pltpu.VMEM((tokens, across), BF16),
            pltpu.VMEM((tp, rows, across), BF16),
            pltpu.VMEM((rows, width), BF16),
            pltpu.VMEM((layer, rows, width), BF16),
            pltpu.VMEM((layer, rows, part), BF16),
            pltpu.VMEM((units, same, rows, n), BF16),
            pltpu.VMEM((units, same, rows, n), BF16),
            pltpu.VMEM((units, group, half, rows, n), BF16),
            pltpu.VMEM((units, half, group, rows, n), BF16),
            pltpu.VMEM((units, rows, n), BF16),
            pltpu.VMEM((units, rows, n), BF16),
            pltpu.VMEM((same, rows, n), F32),
            pltpu.VMEM((units, rows, n) if n % 128 else (1, 8, 128), F32),
            pltpu.VMEM((heads, blocks, dh, BLOCK), BF16),
            pltpu.VMEM((heads, blocks, dh, dh), F32),
            pltpu.VMEM((tokens, across), F32),
            pltpu.VMEM((tokens, across), F32),
            pltpu.VMEM((tokens, 128), F32),
            pltpu.VMEM((heads, dh + 16, dh), F32),
            pltpu.VMEM((heads, dh + 16, dh), F32),
            dma((5,)),
            dma((3,)),
            dma((sp, usubs)),
            dma((sp, grp, usubs)),
            dma((sp, usubs, grp)),
            dma((sp, dsubs)),
            dma((sp, grp, dsubs)),
            dma((sp, dsubs, grp)),
            dma((tp,)),
            dma((tp,)),
            dma((half,)),
            dma,
            dma,
            dma((tp,)),
            dma((tp,)),
            dma((layer, tsubs)),
            dma((tsubs,)),
            dma((half, tsubs)),
            dma((half, tsubs)),
            dma((same, tsubs)),
            dma((units,)),
            dma((units,)),
            dma((units, half)),
            dma((units, half)),
            dma((units,)),
            dma((units,)),
        ],
        compiler_params=pltpu.CompilerParams(
            collective_id=0, has_side_effects=True, vmem_limit_bytes=60 * 1024 * 1024
        ),
    )(
        queries, memory_keys, memory_values, output_preactivation,
        input_preactivation, forget_preactivation, extra_forget_terms,
        head_norm_gain.reshape(1, dh), output_projection_matrix, residual,
        feedforward_norm_gain.reshape(1, width), feedforward_up_matrix, feedforward_down_matrix,
    )


def solution(mesh):
    in_specs = (
        P(("grp", "sp"), "tp"),
        P(("grp", "sp"), "tp"),
        P(("grp", "sp"), "tp"),
        P(("grp", "sp"), "tp"),
        P("tp", ("grp", "sp")),
        P("tp", ("grp", "sp")),
        P("tp", ("grp", "sp")),
        P(),
        P("tp", None),
        P(("grp", "sp", "tp"), None),
        P(),
        P("sp", "tp"),
        P("tp", "sp"),
    )
    out_specs = P(("grp", "sp", "tp"), None)
    shape = (mesh.shape["grp"], mesh.shape["sp"], mesh.shape["tp"])
    return jax.shard_map(
        functools.partial(shards, shape),
        mesh=mesh,
        in_specs=in_specs,
        out_specs=out_specs,
        check_vma=False,
    )
```

```python
import functools

import jax
import jax.numpy as jnp
from jax import lax
from jax.experimental import pallas as pl
from jax.experimental.pallas import tpu as pltpu
from jax.sharding import PartitionSpec as P

BLOCK = 128
EPS = 1e-06
NEG = -1e30
MESH = pl.DeviceIdType.MESH
F32 = jnp.float32
BF16 = jnp.bfloat16


def split_dot(exact, wide, swap=False):
    high = wide.astype(BF16)
    low = (wide - high.astype(F32)).astype(BF16)
    if swap:
        return jnp.dot(high, exact, preferred_element_type=F32) + jnp.dot(
            low, exact, preferred_element_type=F32
        )
    return jnp.dot(exact, high, preferred_element_type=F32) + jnp.dot(
        exact, low, preferred_element_type=F32
    )


def aligned(start, multiple):
    return start if isinstance(start, int) else pl.multiple_of(start, multiple)


def kernel(
    dims,
    q_hbm, k_hbm, v_hbm, o_hbm, igate_hbm, fgate_hbm, extra_hbm, hgain_hbm, wout_hbm, res_hbm,
    fgain_hbm, up_hbm, down_hbm,
    out_ref,
    igate_ref, fgate_ref, extra_ref, hgain_ref, fgain_ref,
    qb, kb, vb, ob, resb, upw, dnw, wo, mixed, mixin, mid, ntok, act, psend, precv, msend, xrecv, zsend, zrecv,
    acc, mlp, keyt, memp, hloc, gates, cols_ref, st_loc, st_out, st_in, top_out, top_in,
    in_sem, loc_sem, wu_send, wu_recv, wuy_send, wd_send, wd_recv, wdy_send, wo_send, wo_recv, wop_send,
    st_send, st_recv, mx_send, mx_recv, t_recv, tz_send, tx_send, tr_send, f_send,
    p_send, p_recv, x_send, x_recv, z_send, z_recv,
):
    grp, sp, tp, heads, blocks, rows, group, usubs, rsubs, pieces, tsubs, parts = dims
    g, z, t = lax.axis_index("grp"), lax.axis_index("sp"), lax.axis_index("tp")
    half = tp // 2
    core, x = lax.rem(t, 2), t // 2
    partner = t + 1 - 2 * core
    zi = lax.rem(z, group)
    other = z + 1 - 2 * zi
    same = half * group
    mine = core * same + zi * half + x
    edge = (z == 0) | (z == sp - 1)
    dsubs = rsubs * pieces
    width = ntok.shape[2]
    part = upw.shape[2]
    up_rows = upw.shape[1]
    out_cols = dnw.shape[2]
    n = out_cols // pieces
    w = n // parts
    urows = up_rows // grp // usubs
    drows = part // grp // rsubs
    trows = rows // tsubs

    def there(gg, zz, tt):
        return {"grp": gg, "sp": zz, "tp": tt}

    def remote(src, dst, send, recv, where):
        return pltpu.make_async_remote_copy(
            src_ref=src, dst_ref=dst, send_sem=send, recv_sem=recv, device_id=where, device_id_type=MESH
        )

    def nth(k):
        power = sp & (sp - 1) == 0
        if not power:
            return lax.rem(z + k, sp)
        gray_of = k
        total = 0
        bit = 1
        while bit < sp:
            mask = (gray_of // bit + gray_of // (2 * bit)) % 2
            zbit = lax.rem(z // bit, 2)
            total = total + (zbit + mask - 2 * zbit * mask) * bit
            bit *= 2
        return total

    def load(i, src, dst):
        return pltpu.make_async_copy(src, dst, in_sem.at[i])

    loads = [load(i, s, d) for i, (s, d) in enumerate(
        (
            (k_hbm, kb), (v_hbm, vb), (q_hbm, qb), (o_hbm, ob), (res_hbm, resb), (fgate_hbm, fgate_ref),
            (extra_hbm, extra_ref), (igate_hbm, igate_ref), (hgain_hbm, hgain_ref), (fgain_hbm, fgain_ref),
        )
    )]
    for c in loads:
        c.start()

    barrier = pltpu.get_barrier_semaphore()
    for j in range(1, tp):
        pl.semaphore_signal(barrier, inc=1, device_id=there(g, z, lax.rem(t + j, tp)), device_id_type=MESH)
    for j in range(1, grp):
        pl.semaphore_signal(barrier, inc=1, device_id=there(lax.rem(g + j, grp), z, t), device_id_type=MESH)

    def greet(j, _):
        pl.semaphore_signal(barrier, inc=1, device_id=there(g, lax.rem(z + j, sp), t), device_id_type=MESH)
        return 0

    lax.fori_loop(1, sp, greet, 0)
    pl.semaphore_wait(barrier, tp + grp + sp - 3)

    def up_rows_of(c, s):
        return pl.ds(aligned(c * (urows * usubs) + s * urows, 16), urows)

    def down_at(c, s):
        rows_at = pl.ds(aligned(c * (drows * rsubs) + s % rsubs * drows, 16), drows)
        return rows_at, pl.ds(s // rsubs * n, n)

    def up_copy(zz, s):
        return remote(
            up_hbm.at[up_rows_of(g, s), pl.ds(aligned(lax.rem(zz, group) * part, 128), part)],
            upw.at[z, up_rows_of(g, s), :],
            wu_send.at[zz, s], wu_recv.at[z, g, s], there(g, zz, t),
        )

    def down_copy(zz, s):
        first = lax.rem(zz, group) * part + g * (drows * rsubs) + s % rsubs * drows
        return remote(
            down_hbm.at[pl.ds(aligned(first, 16), drows), pl.ds(s // rsubs * n, n)],
            dnw.at[(z, *down_at(g, s))],
            wd_send.at[zz, s], wd_recv.at[z, g, s], there(g, zz, t),
        )

    def up_pass(o, s, j):
        at = upw.at[o, up_rows_of(g, s), :]
        return remote(at, at, wuy_send.at[o, s, j], wu_recv.at[o, g, s], there(lax.rem(g + j, grp), z, t))

    def down_pass(o, s, j):
        at = dnw.at[(o, *down_at(g, s))]
        return remote(at, at, wdy_send.at[o, s, j], wd_recv.at[o, g, s], there(lax.rem(g + j, grp), z, t))

    def up_arrived(o, c, s):
        at = upw.at[o, up_rows_of(c, s), :]
        return remote(at, at, wuy_send.at[o, s, 0], wu_recv.at[o, c, s], there(g, z, t))

    def down_arrived(o, c, s):
        at = dnw.at[(o, *down_at(c, s))]
        return remote(at, at, wdy_send.at[o, s, 0], wd_recv.at[o, c, s], there(g, z, t))

    def relay_up(k):
        o = nth(k)
        for s in range(usubs):
            up_arrived(o, g, s).wait_recv()
            for j in range(1, grp):
                up_pass(o, s, j).start()

    def of_piece(c):
        return range(c * rsubs, (c + 1) * rsubs)

    def relay_down(k, c):
        o = nth(k)
        for s in of_piece(c):
            down_arrived(o, g, s).wait_recv()
            for j in range(1, grp):
                down_pass(o, s, j).start()

    def finish_up(k):
        o = nth(k)
        for s in range(usubs):
            for j in range(1, grp):
                up_arrived(o, lax.rem(g + j, grp), s).wait_recv()

    def finish_down(k, c):
        o = nth(k)
        for s in of_piece(c):
            for j in range(1, grp):
                down_arrived(o, lax.rem(g + j, grp), s).wait_recv()

    def right(copy, first, last, subs, when=True, flip=False):
        def body(i, _):
            d = first + last - 1 - i if flip else i

            @pl.when((z + d < sp) & when)
            def _():
                for s in subs:
                    copy(z + d, s).start()

            return 0

        lax.fori_loop(first, last, body, 0)

    def left(copy, first, last, subs, when=True, flip=False):
        def body(i, _):
            d = first + last - 1 - i if flip else i

            @pl.when((z - d >= 0) & when)
            def _():
                for s in subs:
                    copy(z - d, s).start()

            return 0

        lax.fori_loop(first, last, body, 0)

    us, ds = range(usubs), range(dsubs)
    far_right, far_left = z + 2 < sp, z - 2 >= 0
    held_right = (zi == 0) & far_right
    held_left = (zi == group - 1) & far_left
    free_right = (zi != 0) | (z + 2 >= sp)
    free_left = (zi != group - 1) | (z - 2 < 0)
    right(up_copy, 1, 2, us[:1], z > 0)
    away_left, away_right = zi != group - 1, zi != 0
    left(up_copy, 1, 2, us)
    left(up_copy, 2, sp, us, zi == group - 1)
    left(down_copy, 1, sp, ds, free_left & jnp.logical_not(away_left))

    def wo_copy(tt):
        return remote(wout_hbm, wo.at[t], wo_send.at[tt], wo_recv.at[t], there(g, z, tt))

    def wo_pass(j):
        tt = lax.rem(x + j, half) * 2 + core
        return remote(wo.at[tt], wo.at[tt], wop_send.at[j], wo_recv.at[tt], there(g, z, partner))

    def wo_arrived(tt):
        return remote(wo.at[tt], wo.at[tt], wop_send.at[0], wo_recv.at[tt], there(g, z, partner))

    for j in range(1, half):
        wo_copy(lax.rem(x + j, half) * 2 + core).start()
    wo_copy(partner).start()
    own = [
        pltpu.make_async_copy(wout_hbm, wo.at[t], loc_sem.at[0]),
        pltpu.make_async_copy(up_hbm.at[:, pl.ds(aligned(zi * part, 128), part)], upw.at[z], loc_sem.at[1]),
        pltpu.make_async_copy(down_hbm.at[pl.ds(aligned(zi * part, 16), part), :], dnw.at[z], loc_sem.at[2]),
    ]
    for c in own:
        c.start()

    dh = qb.shape[1] // heads
    scale = dh ** (-0.5)
    count = heads * blocks
    pad = -count % 8

    def stacked(value):
        pieces_of = [
            value[h : h + 1, b * BLOCK : (b + 1) * BLOCK] for h in range(heads) for b in range(blocks)
        ]
        if pad:
            pieces_of.append(jnp.zeros((pad, BLOCK), F32))
        return jnp.concatenate(pieces_of, axis=0)

    for i in (5, 6, 7):
        loads[i].wait()
    pre = fgate_ref[...]
    log_forget = jnp.minimum(pre, 0.0) - jnp.log1p(jnp.exp(-jnp.abs(pre))) + extra_ref[...]
    cum_row = stacked(log_forget)
    lane = lax.broadcasted_iota(jnp.int32, cum_row.shape, 1)
    step = 1
    while step < BLOCK:
        cum_row = cum_row + jnp.where(lane >= step, pltpu.roll(cum_row, step, 1), 0.0)
        step *= 2
    rest_row = stacked(igate_ref[...]) - cum_row
    cum_col = cum_row.T
    rest_col = rest_row.T

    loads[0].wait()
    loads[1].wait()
    before, totals = {}, {}
    for h in range(heads):
        cols = pl.ds(h * dh, dh)
        run = None
        for b in range(blocks):
            i = h * blocks + b
            at = pl.ds(b * BLOCK, BLOCK)
            total = cum_row[i : i + 1, BLOCK - 1 : BLOCK]
            tail = total + rest_col[:, i : i + 1]
            tail_max = jnp.max(tail, axis=0, keepdims=True)
            weighted = vb[at, cols].astype(F32) * jnp.exp(tail - tail_max)
            key_t = kb[at, cols].astype(F32).T.astype(BF16)
            keyt[h, b] = key_t
            mem = split_dot(key_t, weighted) * scale
            if run is None:
                run = (total, tail_max, mem)
            else:
                before[h, b] = (run[0], run[1])
                memp[h, b] = run[2]
                new = jnp.maximum(total + run[1], tail_max)
                run = (
                    total + run[0],
                    new,
                    jnp.exp(total + run[1] - new) * run[2] + jnp.exp(tail_max - new) * mem,
                )
        st_loc[h, :dh, :] = run[2]
        st_loc[h, dh : dh + 8, :] = jnp.broadcast_to(run[1], (8, dh))
        st_loc[h, dh + 8 : dh + 16, :] = jnp.broadcast_to(run[0], (8, dh))

    def state_copies():
        return (
            remote(top_out, top_in, st_send.at[0], st_recv.at[0], there(g, z + 1, t)),
            remote(st_out, st_in, st_send.at[1], st_recv.at[1], there(g, z + 1, t)),
        )

    @pl.when(z == 0)
    def _():
        st_in[...] = jnp.zeros_like(st_in)
        top_in[...] = jnp.zeros_like(top_in)

    def state_on():
        for h in range(heads):
            m_in = top_in[h, :1, :]
            m_loc = st_loc[h, dh : dh + 1, :]
            total = st_loc[h, dh + 8 : dh + 9, :]
            new = jnp.maximum(total + m_in, m_loc)
            st_out[h] = (
                jnp.exp(total + m_in - new) * st_in[h].astype(F32)
                + jnp.exp(m_loc - new) * st_loc[h, :dh, :]
            ).astype(BF16)
            top_out[h] = jnp.broadcast_to(new, (8, dh))
        for copy in state_copies():
            copy.start()

    def rest_of_sends():
        right(up_copy, 1, 2, us, z == 0)
        right(up_copy, 2, sp, us)
        right(down_copy, 1, 2, ds[:rsubs], free_right & (z == 0))
        right(down_copy, 1, 2, ds[rsubs:], free_right & (zi == 0))

    right(up_copy, 1, 2, us[1:], z > 0)
    right(down_copy, 1, 2, ds[:rsubs], free_right & (zi == 0) & (z > 0))

    @pl.when((z == 0) & (sp > 1))
    def _():
        state_on()

    @pl.when(z == 0)
    def _():
        rest_of_sends()

    loads[2].wait()
    loads[3].wait()
    causal = lax.broadcasted_iota(jnp.int32, (BLOCK, BLOCK), 0) >= lax.broadcasted_iota(
        jnp.int32, (BLOCK, BLOCK), 1
    )
    loads[8].wait()
    gain = hgain_ref[...]

    def take_state(when):
        @pl.when(when)
        def _():
            for copy in state_copies():
                copy.wait_recv()

            @pl.when(z < sp - 1)
            def _():
                state_on()

            rest_of_sends()

    for h in range(heads):
        cols = pl.ds(h * dh, dh)
        if h == heads - 1:
            take_state(z == 1)
        for b in range(blocks):
            i = h * blocks + b
            at = pl.ds(b * BLOCK, BLOCK)
            cum = cum_col[:, i : i + 1]
            query = qb[at, cols]
            log_weight = jnp.where(causal, cum + rest_row[i : i + 1, :], NEG)
            row_max = jnp.max(log_weight, axis=1, keepdims=True)
            base = cum
            if b > 0:
                past, stab = before[h, b]
                base = cum + past
                carry = cum + stab
                row_max = jnp.maximum(row_max, carry)
            scores = (
                jnp.dot(query, keyt[h, b], preferred_element_type=F32)
                * scale
                * jnp.exp(log_weight - row_max)
            )
            hidden = split_dot(vb[at, cols], scores, swap=True)
            if b > 0:
                hidden = hidden + jnp.exp(carry - row_max) * split_dot(query, memp[h, b])
            hloc[at, cols] = hidden
            cols_ref[at, 2 * h : 2 * h + 1] = row_max
            cols_ref[at, 2 * h + 1 : 2 * h + 2] = base
            gates[at, cols] = gain * (1.0 / (1.0 + jnp.exp(-ob[at, cols].astype(F32))))

    if sp > 1:
        @pl.when(z > 1)
        def _():
            relay_up(1)

    take_state(z > 1)
    for h in range(heads):
        cols = pl.ds(h * dh, dh)
        memory = st_in[h]
        stab = top_in[h, 0:1, 0:1]
        for b in range(blocks):
            at = pl.ds(b * BLOCK, BLOCK)
            local_max = cols_ref[at, 2 * h : 2 * h + 1]
            carry = cols_ref[at, 2 * h + 1 : 2 * h + 2] + stab
            row_max = jnp.maximum(local_max, carry)
            past = jnp.dot(qb[at, cols], memory, preferred_element_type=F32)
            hidden = jnp.exp(local_max - row_max) * hloc[at, cols] + jnp.exp(carry - row_max) * past
            mean_sq = jnp.mean(hidden * hidden, axis=1, keepdims=True)
            mixed[at, cols] = (hidden * lax.rsqrt(mean_sq + EPS) * gates[at, cols]).astype(BF16)

    def mixed_copy(j):
        d = lax.rem(t + j, tp)
        return remote(
            mixed.at[pl.ds(aligned(d * rows, 16), rows), :],
            mixin.at[t], mx_send.at[j], mx_recv.at[t], there(g, z, d),
        )

    def mixed_arrived(tt):
        return remote(mixin.at[tt], mixin.at[tt], mx_send.at[0], mx_recv.at[tt], there(g, z, partner))

    for j in range(1, tp):
        mixed_copy(j).start()
    mixin[t] = mixed[pl.ds(aligned(t * rows, 16), rows), :]
    left(up_copy, 2, sp, us, away_left)
    def relays_up(first, last):
        def body(k, _):
            relay_up(k)
            return 0

        lax.fori_loop(first, last, body, 0)

    def relays_down(k):
        for c in range(pieces):
            relay_down(k, c)

    middle = min(sp, 2 + (sp - 2) // 2)
    if sp > 1:
        @pl.when(z <= 1)
        def _():
            relay_up(1)

    for j in range(1, half):
        wo_arrived(lax.rem(x + j, half) * 2 + core).wait_recv()
        wo_pass(j).start()

    own[0].wait()
    loads[4].wait()
    loads[9].wait()
    for j in range(1, half):
        wo_arrived(lax.rem(x + j, half) * 2 + 1 - core).wait_recv()
    wo_arrived(partner).wait_recv()
    for j in range(1, tp):
        mixed_arrived(lax.rem(t + j, tp)).wait_recv()

    chunk = min(512, width)
    sum_sq = jnp.zeros((rows, 1), F32)
    for c in range(width // chunk):
        at = pl.ds(c * chunk, chunk)
        branch = jnp.zeros((rows, chunk), F32)
        for tt in range(tp):
            branch = branch + jnp.dot(mixin[tt], wo[tt, :, at], preferred_element_type=F32).astype(
                BF16
            ).astype(F32)
        value = (resb[:, at].astype(F32) + branch).astype(BF16)
        mid[:, at] = value
        wide = value.astype(F32)
        sum_sq = sum_sq + jnp.sum(wide * wide, axis=1, keepdims=True)
    factor = lax.rsqrt(sum_sq * (1.0 / width) + EPS)
    for c in range(width // chunk):
        at = pl.ds(c * chunk, chunk)
        ntok[mine, :, at] = (mid[:, at].astype(F32) * factor * fgain_ref[:, at]).astype(BF16)

    def slot_of(xx, zz):
        return core * same + zz * half + xx

    def token(slot, s, send, where):
        at = ntok.at[slot, pl.ds(s * trows, trows), :]
        return remote(at, at, send, t_recv.at[slot, s], where)

    def to_pair(s):
        return token(mine, s, tz_send.at[s], there(g, other, t))

    def to_x(j, s):
        return token(mine, s, tx_send.at[j, s], there(g, z, lax.rem(x + j, half) * 2 + core))

    def pass_x(j, s):
        where = there(g, z, lax.rem(x + j, half) * 2 + core)
        return token(slot_of(x, 1 - zi), s, tr_send.at[j, s], where)

    def to_partner(xx, zz, s):
        return token(slot_of(xx, zz), s, f_send.at[zz * half + xx, s], there(g, z, partner))

    def arrived(slot, s):
        return token(slot, s, tz_send.at[s], there(g, z, partner))

    ts = range(tsubs)

    def give(xx, zz):
        for s in ts:
            to_partner(xx, zz, s).start()

    def take(slot):
        for s in ts:
            arrived(slot, s).wait_recv()

    for s in ts:
        if group > 1:
            to_pair(s).start()
    for j in range(1, half):
        for s in ts:
            to_x(j, s).start()
    give(x, zi)
    left(down_copy, 1, sp, ds, away_left)
    right(down_copy, 1, sp, ds, away_right)
    left(down_copy, 1, 2, ds, held_left)
    right(down_copy, 1, 2, ds, held_right)
    left(down_copy, 2, sp, ds, held_left, flip=True)
    right(down_copy, 2, sp, ds, held_right, flip=True)

    def relays_up(first, last):
        def body(k, _):
            relay_up(k)
            return 0

        lax.fori_loop(first, last, body, 0)

    @pl.when(edge)
    def _():
        if sp > 1:
            relay_down(1, 0)
        relays_up(2, middle)

    @pl.when(jnp.logical_not(edge))
    def _():
        relays_up(2, sp)

    for j in range(1, half):
        xx = lax.rem(x + j, half)
        take(slot_of(xx, zi))
        give(xx, zi)

    @pl.when(edge)
    def _():
        relays_up(middle, sp)
        if sp > 1:
            for c in range(1, pieces):
                relay_down(1, c)

    if group > 1:
        for s in ts:
            arrived(slot_of(x, 1 - zi), s).wait_recv()
            for j in range(1, half):
                pass_x(j, s).start()
        give(x, 1 - zi)
    own[1].wait()

    def all_up(k, _):
        finish_up(k)
        return 0

    lax.fori_loop(1, sp, all_up, 0)

    def up_quarter(side, zz):
        at = pl.ds(side * same + zz * half, half)
        value = ntok[at].reshape(half * rows, width)
        y = jnp.dot(value, upw[...].reshape(width, part), preferred_element_type=F32)
        y = jnp.maximum(y, 0.0)
        act[at] = (y * y).astype(BF16).reshape(half, rows, part)

    def up_step(i, _):
        side = core + (1 - 2 * core) * lax.rem(i, 2)
        zz = zi + (1 - 2 * zi) * (i // 2)

        @pl.when(i == 1)
        def _():
            for xx in range(half):
                take((1 - core) * same + zi * half + xx)

        if group > 1:
            @pl.when(i == 2)
            def _():
                for j in range(1, half):
                    xx = lax.rem(x + j, half)
                    take(slot_of(xx, 1 - zi))
                    give(xx, 1 - zi)

            @pl.when(i == 3)
            def _():
                for xx in range(half):
                    take((1 - core) * same + (1 - zi) * half + xx)

        up_quarter(side, zz)
        return 0

    lax.fori_loop(0, 2 * group, up_step, 0)
    early = min(3, sp)

    @pl.when(jnp.logical_not(edge))
    def _():
        for k in range(1, early):
            relays_down(k)

    own[2].wait()

    def pre_copy(unit, h):
        return remote(
            psend.at[unit, h], precv.at[unit, h], p_send.at[unit, h], p_recv.at[unit, h], there(g, z, partner)
        )

    def x_copy(unit, h, j, zz):
        xx = lax.rem(x + j, half)
        return remote(
            msend.at[unit, h, zz, xx], xrecv.at[unit, h, x, zz],
            x_send.at[unit, h, j, zz], x_recv.at[unit, h, x, zz], there(g, z, xx * 2 + core),
        )

    def x_wait(unit, h, zz):
        for j in range(1, half):
            xx = lax.rem(x + j, half)
            at = xrecv.at[unit, h, xx, zz]
            remote(
                at, at, x_send.at[unit, h, 0, zz], x_recv.at[unit, h, xx, zz], there(g, z, partner)
            ).wait_recv()

    def z_copy(unit, h):
        return remote(
            zsend.at[unit, h], zrecv.at[unit, h], z_send.at[unit, h], z_recv.at[unit, h], there(g, other, t)
        )

    share = part // grp

    def product(side, o, c, which):
        at = pl.ds(aligned(which * share, 128), share)
        value = act[pl.ds(side * same, same), :, at].reshape(same * rows, share)
        return jnp.dot(value, dnw[o, at, c * n : (c + 1) * n], preferred_element_type=F32)

    def begin(o, c):
        for side in range(2):
            acc[side] = product(jnp.where(side == 0, 1 - core, core), o, c, g)

    def multiply(unit, o, c):
        def rest(side, place):
            total = acc[place]
            for j in range(1, grp):
                total = total + product(side, o, c, lax.rem(g + j, grp))
            return total

        total = rest(1 - core, 0).astype(BF16)
        for h in range(parts):
            psend[unit, h] = total[:, h * w : (h + 1) * w].reshape(psend.shape[2:])
            pre_copy(unit, h).start()
        acc[1] = rest(core, 1)

    def unit_of(m):
        return nth(m // pieces) * pieces + lax.rem(m, pieces)

    def spread(unit):
        for h in range(parts):
            pre_copy(unit, h).wait_recv()
            total = acc[1, :, h * w : (h + 1) * w].reshape(precv.shape[2:]) + precv[unit, h].astype(F32)
            msend[unit, h] = total.astype(BF16).reshape(msend.shape[2:])
            if group > 1:
                for j in range(1, half):
                    x_copy(unit, h, j, 1 - zi).start()
        for h in range(parts):
            for j in range(1, half):
                x_copy(unit, h, j, zi).start()
            for zz in range(group):
                xrecv[unit, h, x, zz] = msend[unit, h, zz, x]

    def gathered(unit, h, zz):
        total = xrecv[unit, h, 0, zz].astype(F32)
        for xx in range(1, half):
            total = total + xrecv[unit, h, xx, zz].astype(F32)
        return total

    def hand_over(m):
        unit = unit_of(m)
        if group > 1:
            for h in range(parts):
                x_wait(unit, h, 1 - zi)
                zsend[unit, h] = gathered(unit, h, 1 - zi).astype(BF16)
                z_copy(unit, h).start()

    def stage(k, _):
        o = nth(k)
        if early > 2:
            for c in range(pieces):
                @pl.when(edge & (k == c))
                def _():
                    relay_down(2, c)

        @pl.when((k >= early) & edge)
        def _():
            relays_down(k)

        for c in range(pieces):
            m = k * pieces + c

            begin(o, c)
            ahead, piece = (k, c + 1) if c + 1 < pieces else (k + 1, 0)

            @pl.when((ahead >= early) & (ahead < sp) & jnp.logical_not(edge))
            def _():
                relay_down(ahead, piece)

            @pl.when(k > 0)
            def _():
                finish_down(k, c)

            multiply(o * pieces + c, o, c)
            spread(o * pieces + c)

            @pl.when(m >= 2)
            def _():
                hand_over(m - 2)

        return 0

    lax.fori_loop(0, sp, stage, 0)
    units = sp * pieces
    if units > 1:
        hand_over(units - 2)
    hand_over(units - 1)

    direct = out_cols % 128 == 0 and n % 128 == 0

    def finish(m, _):
        unit = unit_of(m)
        for h in range(parts):
            x_wait(unit, h, zi)
            total = gathered(unit, h, zi)
            if group > 1:
                z_copy(unit, h).wait_recv()
                total = total + zrecv[unit, h].astype(F32)
            if direct:
                at = pl.ds(aligned(unit * n + h * w, 128), w)
                out_ref[:, at] = (mid[:, at].astype(F32) + total).astype(BF16)
            else:
                mlp[unit] = total
        return 0

    lax.fori_loop(0, units, finish, 0)
    if not direct:
        for unit in range(units):
            at = pl.ds(unit * n, n)
            out_ref[:, at] = (mid[:, at].astype(F32) + mlp[unit]).astype(BF16)

    def drain(o, _):
        @pl.when(o != z)
        def _():
            for s in us:
                up_copy(o, s).wait_send()
                for j in range(1, grp):
                    up_pass(o, s, j).wait_send()
            for s in ds:
                down_copy(o, s).wait_send()
                for j in range(1, grp):
                    down_pass(o, s, j).wait_send()

        for c in range(pieces):
            unit = o * pieces + c
            for h in range(parts):
                pre_copy(unit, h).wait_send()
                for j in range(1, half):
                    for zz in range(group):
                        x_copy(unit, h, j, zz).wait_send()
                if group > 1:
                    z_copy(unit, h).wait_send()
        return 0

    lax.fori_loop(0, sp, drain, 0)
    for j in range(1, half):
        wo_copy(lax.rem(x + j, half) * 2 + core).wait_send()
        wo_pass(j).wait_send()
        for s in ts:
            to_x(j, s).wait_send()
            if group > 1:
                pass_x(j, s).wait_send()
    wo_copy(partner).wait_send()
    for j in range(1, tp):
        mixed_copy(j).wait_send()
    for s in ts:
        if group > 1:
            to_pair(s).wait_send()
        for xx in range(half):
            for zz in range(group):
                to_partner(xx, zz, s).wait_send()

    @pl.when(z < sp - 1)
    def _():
        for copy in state_copies():
            copy.wait_send()


def shards(
    mesh_shape,
    queries, memory_keys, memory_values, output_preactivation, input_preactivation,
    forget_preactivation, extra_forget_terms, head_norm_gain, output_projection_matrix, residual,
    feedforward_norm_gain, feedforward_up_matrix, feedforward_down_matrix,
):
    grp, sp, tp = mesh_shape
    tokens, across = queries.shape
    heads = input_preactivation.shape[0]
    blocks = tokens // BLOCK
    dh = across // heads
    rows, width = residual.shape
    up_rows, hidden = feedforward_up_matrix.shape
    out_cols = feedforward_down_matrix.shape[1]
    group = 2 if sp % 2 == 0 else 1
    part = hidden // group
    usubs = 2 if up_rows % (32 * grp) == 0 else 1
    pieces = 2 if out_cols % 256 == 0 else 1
    rsubs = 4 if part % (64 * grp) == 0 else 1
    dsubs = rsubs * pieces
    tsubs = 4 if rows % 64 == 0 else 1
    half = tp // 2
    same = half * group
    layer = tp * group
    units = sp * pieces
    n = out_cols // pieces
    parts = 2 if n % 256 == 0 else 1
    w = n // parts

    vmem = pl.BlockSpec(memory_space=pltpu.VMEM)
    hbm = pl.BlockSpec(memory_space=pl.ANY)
    dma = pltpu.SemaphoreType.DMA
    return pl.pallas_call(
        functools.partial(
            kernel, (grp, sp, tp, heads, blocks, rows, group, usubs, rsubs, pieces, tsubs, parts)
        ),
        out_shape=jax.ShapeDtypeStruct((rows, width), BF16),
        in_specs=[hbm] * 13,
        out_specs=vmem,
        scratch_shapes=[
            pltpu.VMEM((heads, tokens), F32),
            pltpu.VMEM((heads, tokens), F32),
            pltpu.VMEM((heads, tokens), F32),
            pltpu.VMEM((1, dh), F32),
            pltpu.VMEM((1, width), F32),
            pltpu.VMEM((tokens, across), BF16),
            pltpu.VMEM((tokens, across), BF16),
            pltpu.VMEM((tokens, across), BF16),
            pltpu.VMEM((tokens, across), BF16),
            pltpu.VMEM((rows, width), BF16),
            pltpu.VMEM((sp, up_rows, part), BF16),
            pltpu.VMEM((sp, part, out_cols), BF16),
            pltpu.VMEM((tp, across, width), BF16),
            pltpu.VMEM((tokens, across), BF16),
            pltpu.VMEM((tp, rows, across), BF16),
            pltpu.VMEM((rows, width), BF16),
            pltpu.VMEM((layer, rows, width), BF16),
            pltpu.VMEM((layer, rows, part), BF16),
            pltpu.VMEM((units, parts, same, rows, w), BF16),
            pltpu.VMEM((units, parts, same, rows, w), BF16),
            pltpu.VMEM((units, parts, group, half, rows, w), BF16),
            pltpu.VMEM((units, parts, half, group, rows, w), BF16),
            pltpu.VMEM((units, parts, rows, w), BF16),
            pltpu.VMEM((units, parts, rows, w), BF16),
            pltpu.VMEM((2, same * rows, n), F32),
            pltpu.VMEM((units, rows, n) if n % 128 else (1, 8, 128), F32),
            pltpu.VMEM((heads, blocks, dh, BLOCK), BF16),
            pltpu.VMEM((heads, blocks, dh, dh), F32),
            pltpu.VMEM((tokens, across), F32),
            pltpu.VMEM((tokens, across), F32),
            pltpu.VMEM((tokens, 128), F32),
            pltpu.VMEM((heads, dh + 16, dh), F32),
            pltpu.VMEM((heads, dh, dh), BF16),
            pltpu.VMEM((heads, dh, dh), BF16),
            pltpu.VMEM((heads, 8, dh), F32),
            pltpu.VMEM((heads, 8, dh), F32),
            dma((10,)),
            dma((3,)),
            dma((sp, usubs)),
            dma((sp, grp, usubs)),
            dma((sp, usubs, grp)),
            dma((sp, dsubs)),
            dma((sp, grp, dsubs)),
            dma((sp, dsubs, grp)),
            dma((tp,)),
            dma((tp,)),
            dma((half,)),
            dma((2,)),
            dma((2,)),
            dma((tp,)),
            dma((tp,)),
            dma((layer, tsubs)),
            dma((tsubs,)),
            dma((half, tsubs)),
            dma((half, tsubs)),
            dma((same, tsubs)),
            dma((units, parts)),
            dma((units, parts)),
            dma((units, parts, half, group)),
            dma((units, parts, half, group)),
            dma((units, parts)),
            dma((units, parts)),
        ],
        compiler_params=pltpu.CompilerParams(
            collective_id=0, has_side_effects=True, vmem_limit_bytes=60 * 1024 * 1024
        ),
    )(
        queries, memory_keys, memory_values, output_preactivation,
        input_preactivation, forget_preactivation, extra_forget_terms,
        head_norm_gain.reshape(1, dh), output_projection_matrix, residual,
        feedforward_norm_gain.reshape(1, width), feedforward_up_matrix, feedforward_down_matrix,
    )


def solution(mesh):
    in_specs = (
        P(("grp", "sp"), "tp"),
        P(("grp", "sp"), "tp"),
        P(("grp", "sp"), "tp"),
        P(("grp", "sp"), "tp"),
        P("tp", ("grp", "sp")),
        P("tp", ("grp", "sp")),
        P("tp", ("grp", "sp")),
        P(),
        P("tp", None),
        P(("grp", "sp", "tp"), None),
        P(),
        P("sp", "tp"),
        P("tp", "sp"),
    )
    out_specs = P(("grp", "sp", "tp"), None)
    shape = (mesh.shape["grp"], mesh.shape["sp"], mesh.shape["tp"])
    return jax.shard_map(
        functools.partial(shards, shape),
        mesh=mesh,
        in_specs=in_specs,
        out_specs=out_specs,
        check_vma=False,
    )
```

```python
import functools

import jax
import jax.numpy as jnp
from jax import lax
from jax.experimental import pallas as pl
from jax.experimental.pallas import tpu as pltpu
from jax.sharding import PartitionSpec as P

BLOCK = 128
EPS = 1e-06
NEG = -1e30
MESH = pl.DeviceIdType.MESH
F32 = jnp.float32
BF16 = jnp.bfloat16


def split_dot(exact, wide, swap=False):
    high = wide.astype(BF16)
    low = (wide - high.astype(F32)).astype(BF16)
    if swap:
        return jnp.dot(high, exact, preferred_element_type=F32) + jnp.dot(
            low, exact, preferred_element_type=F32
        )
    return jnp.dot(exact, high, preferred_element_type=F32) + jnp.dot(
        exact, low, preferred_element_type=F32
    )


def aligned(start, multiple):
    return start if isinstance(start, int) else pl.multiple_of(start, multiple)


def kernel(
    dims,
    q_hbm, k_hbm, v_hbm, o_hbm, igate_hbm, fgate_hbm, extra_hbm, hgain_hbm, wout_hbm, res_hbm,
    fgain_hbm, up_hbm, down_hbm,
    out_ref,
    gates_in, hgain_ref, fgain_ref, qkvo, resb,
    upw, dnw, wo, mixed, mixin, mid, ntok, act, psend, precv, msend, xrecv, zsend, zrecv,
    acc, mlp, keyt, memp, hloc, gates, cols_ref, st_loc, st_out, st_in, top_out, top_in,
    in_sem, loc_sem, wu_send, wu_recv, uy_send, uy_recv, wd_send, wd_recv, dy_send, dy_recv,
    wo_send, wo_recv, st_send, st_recv, mx_send, mx_recv, t_send, t_recv, tz_recv,
    p_send, p_recv, x_send, x_recv, z_send, z_recv,
):
    grp, sp, tp, heads, blocks, rows, group, usubs, rsubs, pieces, tsubs, parts = dims
    g, z, t = lax.axis_index("grp"), lax.axis_index("sp"), lax.axis_index("tp")
    half = tp // 2
    core, x = lax.rem(t, 2), t // 2
    partner = t + 1 - 2 * core
    zi = lax.rem(z, group)
    other = z + 1 - 2 * zi
    same = half * group
    mine = core * same + zi * half + x
    edge = (z == 0) | (z == sp - 1)
    dsubs = rsubs * pieces
    width = ntok.shape[2]
    part = upw.shape[2]
    up_rows = upw.shape[1]
    out_cols = dnw.shape[2]
    n = out_cols // pieces
    w = n // parts
    urows = up_rows // grp // usubs
    drows = part // grp // rsubs
    trows = rows // tsubs

    def there(gg, zz, tt):
        return {"grp": gg, "sp": zz, "tp": tt}

    def remote(src, dst, send, recv, where):
        return pltpu.make_async_remote_copy(
            src_ref=src, dst_ref=dst, send_sem=send, recv_sem=recv, device_id=where, device_id_type=MESH
        )

    def nth(k):
        power = sp & (sp - 1) == 0
        if not power:
            return lax.rem(z + k, sp)
        gray_of = k
        total = 0
        bit = 1
        while bit < sp:
            mask = (gray_of // bit + gray_of // (2 * bit)) % 2
            zbit = lax.rem(z // bit, 2)
            total = total + (zbit + mask - 2 * zbit * mask) * bit
            bit *= 2
        return total

    kb, vb, qb, ob = (qkvo.at[i] for i in range(4))

    def await_recv(ref, sem):
        remote(ref, ref, mx_send, sem, there(g, z, partner)).wait_recv()

    def await_send(ref, sem):
        remote(ref, ref, sem, mx_recv, there(g, z, partner)).wait_send()

    loads = [
        pltpu.make_async_copy(src, dst, in_sem.at[i])
        for src, dst, i in (
            (fgate_hbm, gates_in.at[0], 0), (extra_hbm, gates_in.at[1], 0), (igate_hbm, gates_in.at[2], 0),
            (k_hbm, kb, 1), (v_hbm, vb, 1), (q_hbm, qb, 2), (o_hbm, ob, 2),
            (hgain_hbm, hgain_ref, 3), (fgain_hbm, fgain_ref, 4), (res_hbm, resb, 5),
        )
    ]
    for c in loads:
        c.start()

    def loaded(ref, i):
        pltpu.make_async_copy(ref, ref, in_sem.at[i]).wait()

    barrier = pltpu.get_barrier_semaphore()
    for j in range(1, tp):
        pl.semaphore_signal(barrier, inc=1, device_id=there(g, z, lax.rem(t + j, tp)), device_id_type=MESH)
    for j in range(1, grp):
        pl.semaphore_signal(barrier, inc=1, device_id=there(lax.rem(g + j, grp), z, t), device_id_type=MESH)

    def greet(j, _):
        pl.semaphore_signal(barrier, inc=1, device_id=there(g, lax.rem(z + j, sp), t), device_id_type=MESH)
        return 0

    lax.fori_loop(1, sp, greet, 0)
    pl.semaphore_wait(barrier, tp + grp + sp - 3)

    def up_rows_of(c, s):
        return pl.ds(aligned(c * (urows * usubs) + s * urows, 16), urows)

    def down_at(c, s):
        rows_at = pl.ds(aligned(c * (drows * rsubs) + s % rsubs * drows, 16), drows)
        return rows_at, pl.ds(s // rsubs * n, n)

    def up_copy(zz, s):
        return remote(
            up_hbm.at[up_rows_of(g, s), pl.ds(aligned(lax.rem(zz, group) * part, 128), part)],
            upw.at[z, up_rows_of(g, s), :],
            wu_send, wu_recv.at[z, s], there(g, zz, t),
        )

    def down_copy(zz, s):
        first = lax.rem(zz, group) * part + g * (drows * rsubs) + s % rsubs * drows
        return remote(
            down_hbm.at[pl.ds(aligned(first, 16), drows), pl.ds(s // rsubs * n, n)],
            dnw.at[(z, *down_at(g, s))],
            wd_send, wd_recv.at[z, s], there(g, zz, t),
        )

    def up_pass(o, s, j):
        at = upw.at[o, up_rows_of(g, s), :]
        return remote(at, at, uy_send, uy_recv, there(lax.rem(g + j, grp), z, t))

    def down_pass(o, s, j):
        at = dnw.at[(o, *down_at(g, s))]
        where = there(lax.rem(g + j, grp), z, t)
        return remote(at, at, dy_send, dy_recv.at[o, s // rsubs, grp - j - 1], where)

    def of_piece(c):
        return range(c * rsubs, (c + 1) * rsubs)

    def relay_up(k):
        o = nth(k)
        for s in range(usubs):
            await_recv(upw.at[o, up_rows_of(g, s), :], wu_recv.at[o, s])
            for j in range(1, grp):
                up_pass(o, s, j).start()

    def relay_down(k, c):
        o = nth(k)
        for s in of_piece(c):
            await_recv(dnw.at[(o, *down_at(g, s))], wd_recv.at[o, s])
            for j in range(1, grp):
                down_pass(o, s, j).start()

    def finish_down(k, c):
        o = nth(k)
        for j in range(1, grp):
            first = aligned(lax.rem(g + j, grp) * (drows * rsubs), 16)
            at = dnw.at[o, pl.ds(first, drows * rsubs), pl.ds(c * n, n)]
            await_recv(at, dy_recv.at[o, c, j - 1])

    def right(copy, first, last, subs, when=True, flip=False):
        def body(i, _):
            d = first + last - 1 - i if flip else i

            @pl.when((z + d < sp) & when)
            def _():
                for s in subs:
                    copy(z + d, s).start()

            return 0

        lax.fori_loop(first, last, body, 0)

    def left(copy, first, last, subs, when=True, flip=False):
        def body(i, _):
            d = first + last - 1 - i if flip else i

            @pl.when((z - d >= 0) & when)
            def _():
                for s in subs:
                    copy(z - d, s).start()

            return 0

        lax.fori_loop(first, last, body, 0)

    us, ds = range(usubs), range(dsubs)
    far_right, far_left = z + 2 < sp, z - 2 >= 0
    held_right = (zi == 0) & far_right
    held_left = (zi == group - 1) & far_left
    free_right = (zi != 0) | (z + 2 >= sp)
    free_left = (zi != group - 1) | (z - 2 < 0)
    right(up_copy, 1, 2, us[:1], z > 0)
    away_left, away_right = zi != group - 1, zi != 0
    left(up_copy, 1, 2, us)
    left(up_copy, 2, sp, us, zi == group - 1)
    left(down_copy, 1, sp, ds, free_left & jnp.logical_not(away_left))

    def wo_copy(tt):
        return remote(wout_hbm, wo.at[t], wo_send, wo_recv.at[t], there(g, z, tt))

    def wo_pass(j):
        tt = lax.rem(x + j, half) * 2 + core
        return remote(wo.at[tt], wo.at[tt], wo_send, wo_recv.at[tt], there(g, z, partner))

    def wo_arrived(tt):
        await_recv(wo.at[tt], wo_recv.at[tt])

    for j in range(1, half):
        wo_copy(lax.rem(x + j, half) * 2 + core).start()
    wo_copy(partner).start()
    own = [
        pltpu.make_async_copy(wout_hbm, wo.at[t], loc_sem.at[0]),
        pltpu.make_async_copy(up_hbm.at[:, pl.ds(aligned(zi * part, 128), part)], upw.at[z], loc_sem.at[1]),
        pltpu.make_async_copy(down_hbm.at[pl.ds(aligned(zi * part, 16), part), :], dnw.at[z], loc_sem.at[2]),
    ]
    for c in own:
        c.start()

    dh = qkvo.shape[2] // heads
    scale = dh ** (-0.5)
    count = heads * blocks
    pad = -count % 8

    def stacked(value):
        pieces_of = [
            value[h : h + 1, b * BLOCK : (b + 1) * BLOCK] for h in range(heads) for b in range(blocks)
        ]
        if pad:
            pieces_of.append(jnp.zeros((pad, BLOCK), F32))
        return jnp.concatenate(pieces_of, axis=0)

    loaded(gates_in, 0)
    pre = gates_in[0]
    log_forget = jnp.minimum(pre, 0.0) - jnp.log1p(jnp.exp(-jnp.abs(pre))) + gates_in[1]
    cum_row = stacked(log_forget)
    lane = lax.broadcasted_iota(jnp.int32, cum_row.shape, 1)
    step = 1
    while step < BLOCK:
        cum_row = cum_row + jnp.where(lane >= step, pltpu.roll(cum_row, step, 1), 0.0)
        step *= 2
    rest_row = stacked(gates_in[2]) - cum_row
    cum_col = cum_row.T
    rest_col = rest_row.T

    loaded(qkvo.at[pl.ds(0, 2)], 1)
    before, totals = {}, {}
    for h in range(heads):
        cols = pl.ds(h * dh, dh)
        run = None
        for b in range(blocks):
            i = h * blocks + b
            at = pl.ds(b * BLOCK, BLOCK)
            total = cum_row[i : i + 1, BLOCK - 1 : BLOCK]
            tail = total + rest_col[:, i : i + 1]
            tail_max = jnp.max(tail, axis=0, keepdims=True)
            weighted = vb[at, cols].astype(F32) * jnp.exp(tail - tail_max)
            key_t = kb[at, cols].astype(F32).T.astype(BF16)
            keyt[h, b] = key_t
            mem = split_dot(key_t, weighted) * scale
            if run is None:
                run = (total, tail_max, mem)
            else:
                before[h, b] = (run[0], run[1])
                memp[h, b] = run[2]
                new = jnp.maximum(total + run[1], tail_max)
                run = (
                    total + run[0],
                    new,
                    jnp.exp(total + run[1] - new) * run[2] + jnp.exp(tail_max - new) * mem,
                )
        st_loc[h, :dh, :] = run[2]
        st_loc[h, dh : dh + 8, :] = jnp.broadcast_to(run[1], (8, dh))
        st_loc[h, dh + 8 : dh + 16, :] = jnp.broadcast_to(run[0], (8, dh))

    def state_copies():
        return (
            remote(top_out, top_in, st_send.at[0], st_recv.at[0], there(g, z + 1, t)),
            remote(st_out, st_in, st_send.at[1], st_recv.at[1], there(g, z + 1, t)),
        )

    @pl.when(z == 0)
    def _():
        st_in[...] = jnp.zeros_like(st_in)
        top_in[...] = jnp.zeros_like(top_in)

    def state_on():
        for h in range(heads):
            m_in = top_in[h, :1, :]
            m_loc = st_loc[h, dh : dh + 1, :]
            total = st_loc[h, dh + 8 : dh + 9, :]
            new = jnp.maximum(total + m_in, m_loc)
            st_out[h] = (
                jnp.exp(total + m_in - new) * st_in[h].astype(F32)
                + jnp.exp(m_loc - new) * st_loc[h, :dh, :]
            ).astype(BF16)
            top_out[h] = jnp.broadcast_to(new, (8, dh))
        for copy in state_copies():
            copy.start()

    def rest_of_sends():
        right(up_copy, 1, 2, us, z == 0)
        right(up_copy, 2, sp, us)
        right(down_copy, 1, 2, ds[:rsubs], free_right & (z == 0))
        right(down_copy, 1, 2, ds[rsubs:], free_right & (zi == 0))

    right(up_copy, 1, 2, us[1:], z > 0)
    right(down_copy, 1, 2, ds[:rsubs], free_right & (zi == 0) & (z > 0))

    @pl.when((z == 0) & (sp > 1))
    def _():
        state_on()

    @pl.when(z == 0)
    def _():
        rest_of_sends()

    loaded(qkvo.at[pl.ds(2, 2)], 2)
    causal = lax.broadcasted_iota(jnp.int32, (BLOCK, BLOCK), 0) >= lax.broadcasted_iota(
        jnp.int32, (BLOCK, BLOCK), 1
    )
    loaded(hgain_ref, 3)
    gain = hgain_ref[...]

    def take_state(when):
        @pl.when(when)
        def _():
            for copy in state_copies():
                copy.wait_recv()

            @pl.when(z < sp - 1)
            def _():
                state_on()

            rest_of_sends()

    for h in range(heads):
        cols = pl.ds(h * dh, dh)
        if h == heads - 1:
            take_state(z == 1)
        for b in range(blocks):
            i = h * blocks + b
            at = pl.ds(b * BLOCK, BLOCK)
            cum = cum_col[:, i : i + 1]
            query = qb[at, cols]
            log_weight = jnp.where(causal, cum + rest_row[i : i + 1, :], NEG)
            row_max = jnp.max(log_weight, axis=1, keepdims=True)
            base = cum
            if b > 0:
                past, stab = before[h, b]
                base = cum + past
                carry = cum + stab
                row_max = jnp.maximum(row_max, carry)
            scores = (
                jnp.dot(query, keyt[h, b], preferred_element_type=F32)
                * scale
                * jnp.exp(log_weight - row_max)
            )
            hidden = split_dot(vb[at, cols], scores, swap=True)
            if b > 0:
                hidden = hidden + jnp.exp(carry - row_max) * split_dot(query, memp[h, b])
            hloc[at, cols] = hidden
            cols_ref[at, 2 * h : 2 * h + 1] = row_max
            cols_ref[at, 2 * h + 1 : 2 * h + 2] = base
            gates[at, cols] = gain * (1.0 / (1.0 + jnp.exp(-ob[at, cols].astype(F32))))

    if sp > 1:
        @pl.when(z > 1)
        def _():
            relay_up(1)

    take_state(z > 1)
    for h in range(heads):
        cols = pl.ds(h * dh, dh)
        memory = st_in[h]
        stab = top_in[h, 0:1, 0:1]
        for b in range(blocks):
            at = pl.ds(b * BLOCK, BLOCK)
            local_max = cols_ref[at, 2 * h : 2 * h + 1]
            carry = cols_ref[at, 2 * h + 1 : 2 * h + 2] + stab
            row_max = jnp.maximum(local_max, carry)
            past = jnp.dot(qb[at, cols], memory, preferred_element_type=F32)
            hidden = jnp.exp(local_max - row_max) * hloc[at, cols] + jnp.exp(carry - row_max) * past
            mean_sq = jnp.mean(hidden * hidden, axis=1, keepdims=True)
            mixed[at, cols] = (hidden * lax.rsqrt(mean_sq + EPS) * gates[at, cols]).astype(BF16)

    def mixed_copy(j):
        d = lax.rem(t + j, tp)
        return remote(
            mixed.at[pl.ds(aligned(d * rows, 16), rows), :],
            mixin.at[t], mx_send, mx_recv, there(g, z, d),
        )

    for j in range(1, tp):
        mixed_copy(j).start()
    mixin[t] = mixed[pl.ds(aligned(t * rows, 16), rows), :]
    left(up_copy, 2, sp, us, away_left)
    def relays_up(first, last):
        def body(k, _):
            relay_up(k)
            return 0

        lax.fori_loop(first, last, body, 0)

    def relays_down(k):
        for c in range(pieces):
            relay_down(k, c)

    middle = min(sp, 2 + (sp - 2) // 2)
    if sp > 1:
        @pl.when(z <= 1)
        def _():
            relay_up(1)

    for j in range(1, half):
        wo_arrived(lax.rem(x + j, half) * 2 + core)
        wo_pass(j).start()

    own[0].wait()
    loaded(fgain_ref, 4)
    loaded(resb, 5)
    for j in range(1, half):
        wo_arrived(lax.rem(x + j, half) * 2 + 1 - core)
    wo_arrived(partner)
    await_recv(mixin.at[pl.ds(0, tp - 1)], mx_recv)

    chunk = min(512, width)
    sum_sq = jnp.zeros((rows, 1), F32)
    for c in range(width // chunk):
        at = pl.ds(c * chunk, chunk)
        branch = jnp.zeros((rows, chunk), F32)
        for tt in range(tp):
            branch = branch + jnp.dot(mixin[tt], wo[tt, :, at], preferred_element_type=F32).astype(
                BF16
            ).astype(F32)
        value = (resb[:, at].astype(F32) + branch).astype(BF16)
        mid[:, at] = value
        wide = value.astype(F32)
        sum_sq = sum_sq + jnp.sum(wide * wide, axis=1, keepdims=True)
    factor = lax.rsqrt(sum_sq * (1.0 / width) + EPS)
    for c in range(width // chunk):
        at = pl.ds(c * chunk, chunk)
        ntok[mine, :, at] = (mid[:, at].astype(F32) * factor * fgain_ref[:, at]).astype(BF16)

    def slot_of(xx, zz):
        return core * same + zz * half + xx

    def row_part(slot, s):
        return ntok.at[slot, pl.ds(s * trows, trows), :]

    def to_pair(s):
        at = row_part(mine, s)
        return remote(at, at, t_send, tz_recv.at[s], there(g, other, t))

    def to_x(j):
        where = there(g, z, lax.rem(x + j, half) * 2 + core)
        return remote(ntok.at[mine], ntok.at[mine], t_send, t_recv.at[mine], where)

    def pass_x(j, s):
        slot = slot_of(x, 1 - zi)
        at = row_part(slot, s)
        return remote(at, at, t_send, t_recv.at[slot], there(g, z, lax.rem(x + j, half) * 2 + core))

    def give(xx, zz):
        slot = slot_of(xx, zz)
        remote(ntok.at[slot], ntok.at[slot], t_send, t_recv.at[slot], there(g, z, partner)).start()

    def take(slot):
        await_recv(ntok.at[slot], t_recv.at[slot])

    ts = range(tsubs)

    for s in ts:
        if group > 1:
            to_pair(s).start()
    for j in range(1, half):
        to_x(j).start()
    give(x, zi)
    left(down_copy, 1, sp, ds, away_left)
    right(down_copy, 1, sp, ds, away_right)
    left(down_copy, 1, 2, ds, held_left)
    right(down_copy, 1, 2, ds, held_right)
    left(down_copy, 2, sp, ds, held_left, flip=True)
    right(down_copy, 2, sp, ds, held_right, flip=True)

    def relays_up(first, last):
        def body(k, _):
            relay_up(k)
            return 0

        lax.fori_loop(first, last, body, 0)

    @pl.when(edge)
    def _():
        if sp > 1:
            relay_down(1, 0)
        relays_up(2, middle)

    @pl.when(jnp.logical_not(edge))
    def _():
        relays_up(2, sp)

    for j in range(1, half):
        xx = lax.rem(x + j, half)
        take(slot_of(xx, zi))
        give(xx, zi)

    @pl.when(edge)
    def _():
        relays_up(middle, sp)
        if sp > 1:
            for c in range(1, pieces):
                relay_down(1, c)

    if group > 1:
        for s in ts:
            await_recv(row_part(slot_of(x, 1 - zi), s), tz_recv.at[s])
            for j in range(1, half):
                pass_x(j, s).start()
        give(x, 1 - zi)
    own[1].wait()

    others = up_rows - up_rows // grp
    if sp > 1 and grp > 1:
        await_recv(upw.at[pl.ds(0, sp - 1), pl.ds(0, others), :], uy_recv)

    def up_quarter(side, zz):
        at = pl.ds(side * same + zz * half, half)
        value = ntok[at].reshape(half * rows, width)
        y = jnp.dot(value, upw[...].reshape(width, part), preferred_element_type=F32)
        y = jnp.maximum(y, 0.0)
        act[at] = (y * y).astype(BF16).reshape(half, rows, part)

    def up_step(i, _):
        side = core + (1 - 2 * core) * lax.rem(i, 2)
        zz = zi + (1 - 2 * zi) * (i // 2)

        @pl.when(i == 1)
        def _():
            for xx in range(half):
                take((1 - core) * same + zi * half + xx)

        if group > 1:
            @pl.when(i == 2)
            def _():
                for j in range(1, half):
                    xx = lax.rem(x + j, half)
                    take(slot_of(xx, 1 - zi))
                    give(xx, 1 - zi)

            @pl.when(i == 3)
            def _():
                for xx in range(half):
                    take((1 - core) * same + (1 - zi) * half + xx)

        up_quarter(side, zz)
        return 0

    lax.fori_loop(0, 2 * group, up_step, 0)
    early = min(3, sp)

    @pl.when(jnp.logical_not(edge))
    def _():
        for k in range(1, early):
            relays_down(k)

    own[2].wait()

    def pre_copy(unit, h):
        return remote(
            psend.at[unit, h], precv.at[unit, h], p_send, p_recv.at[unit, h], there(g, z, partner)
        )

    def x_copy(unit, h, j, zz):
        xx = lax.rem(x + j, half)
        return remote(
            msend.at[unit, h, zz, xx], xrecv.at[unit, h, x, zz],
            x_send, x_recv.at[unit, h, zz], there(g, z, xx * 2 + core),
        )

    def x_wait(unit, h, zz):
        await_recv(xrecv.at[unit, h, pl.ds(0, half - 1), zz], x_recv.at[unit, h, zz])

    def z_copy(unit, h):
        return remote(
            zsend.at[unit, h], zrecv.at[unit, h], z_send, z_recv.at[unit, h], there(g, other, t)
        )

    share = part // grp

    def product(side, o, c, which):
        at = pl.ds(aligned(which * share, 128), share)
        value = act[pl.ds(side * same, same), :, at].reshape(same * rows, share)
        return jnp.dot(value, dnw[o, at, c * n : (c + 1) * n], preferred_element_type=F32)

    def begin(o, c):
        for side in range(2):
            acc[side] = product(jnp.where(side == 0, 1 - core, core), o, c, g)

    def multiply(unit, o, c):
        def rest(side, place):
            total = acc[place]
            for j in range(1, grp):
                total = total + product(side, o, c, lax.rem(g + j, grp))
            return total

        total = rest(1 - core, 0).astype(BF16)
        for h in range(parts):
            psend[unit, h] = total[:, h * w : (h + 1) * w].reshape(psend.shape[2:])
            pre_copy(unit, h).start()
        acc[1] = rest(core, 1)

    def unit_of(m):
        return nth(m // pieces) * pieces + lax.rem(m, pieces)

    def spread(unit):
        for h in range(parts):
            pre_copy(unit, h).wait_recv()
            total = acc[1, :, h * w : (h + 1) * w].reshape(precv.shape[2:]) + precv[unit, h].astype(F32)
            msend[unit, h] = total.astype(BF16).reshape(msend.shape[2:])
            if group > 1:
                for j in range(1, half):
                    x_copy(unit, h, j, 1 - zi).start()
        for h in range(parts):
            for j in range(1, half):
                x_copy(unit, h, j, zi).start()
            for zz in range(group):
                xrecv[unit, h, x, zz] = msend[unit, h, zz, x]

    def gathered(unit, h, zz):
        total = xrecv[unit, h, 0, zz].astype(F32)
        for xx in range(1, half):
            total = total + xrecv[unit, h, xx, zz].astype(F32)
        return total

    def hand_over(m):
        unit = unit_of(m)
        if group > 1:
            for h in range(parts):
                x_wait(unit, h, 1 - zi)
                zsend[unit, h] = gathered(unit, h, 1 - zi).astype(BF16)
                z_copy(unit, h).start()

    def stage(k, _):
        o = nth(k)
        if early > 2:
            for c in range(pieces):
                @pl.when(edge & (k == c))
                def _():
                    relay_down(2, c)

        @pl.when((k >= early) & edge)
        def _():
            relays_down(k)

        for c in range(pieces):
            m = k * pieces + c

            begin(o, c)
            ahead, piece = (k, c + 1) if c + 1 < pieces else (k + 1, 0)

            @pl.when((ahead >= early) & (ahead < sp) & jnp.logical_not(edge))
            def _():
                relay_down(ahead, piece)

            @pl.when(k > 0)
            def _():
                finish_down(k, c)

            multiply(o * pieces + c, o, c)
            spread(o * pieces + c)

            @pl.when(m >= 2)
            def _():
                hand_over(m - 2)

        return 0

    lax.fori_loop(0, sp, stage, 0)
    units = sp * pieces
    if units > 1:
        hand_over(units - 2)
    hand_over(units - 1)

    direct = out_cols % 128 == 0 and n % 128 == 0

    def finish(m, _):
        unit = unit_of(m)
        for h in range(parts):
            x_wait(unit, h, zi)
            total = gathered(unit, h, zi)
            if group > 1:
                z_copy(unit, h).wait_recv()
                total = total + zrecv[unit, h].astype(F32)
            if direct:
                at = pl.ds(aligned(unit * n + h * w, 128), w)
                out_ref[:, at] = (mid[:, at].astype(F32) + total).astype(BF16)
            else:
                mlp[unit] = total
        return 0

    lax.fori_loop(0, units, finish, 0)
    if not direct:
        for unit in range(units):
            at = pl.ds(unit * n, n)
            out_ref[:, at] = (mid[:, at].astype(F32) + mlp[unit]).astype(BF16)

    if sp > 1:
        await_send(upw.at[pl.ds(0, sp - 1), pl.ds(0, up_rows // grp), :], wu_send)
        await_send(dnw.at[pl.ds(0, sp - 1), pl.ds(0, part // grp), :], wd_send)
        if grp > 1:
            await_send(upw.at[pl.ds(0, sp - 1), pl.ds(0, others), :], uy_send)
            await_send(dnw.at[pl.ds(0, sp - 1), pl.ds(0, part - share), :], dy_send)
    await_send(wo.at[pl.ds(0, 2 * half - 1)], wo_send)
    await_send(mixin.at[pl.ds(0, tp - 1)], mx_send)
    await_send(ntok.at[pl.ds(0, group * (half - 1) + same + group - 1)], t_send)
    await_send(psend, p_send)
    if half > 1:
        await_send(msend.at[:, :, :, pl.ds(0, half - 1)], x_send)
    if group > 1:
        await_send(zsend, z_send)

    @pl.when(z < sp - 1)
    def _():
        for copy in state_copies():
            copy.wait_send()


def shards(
    mesh_shape,
    queries, memory_keys, memory_values, output_preactivation, input_preactivation,
    forget_preactivation, extra_forget_terms, head_norm_gain, output_projection_matrix, residual,
    feedforward_norm_gain, feedforward_up_matrix, feedforward_down_matrix,
):
    grp, sp, tp = mesh_shape
    tokens, across = queries.shape
    heads = input_preactivation.shape[0]
    blocks = tokens // BLOCK
    dh = across // heads
    rows, width = residual.shape
    up_rows, hidden = feedforward_up_matrix.shape
    out_cols = feedforward_down_matrix.shape[1]
    group = 2 if sp % 2 == 0 else 1
    part = hidden // group
    usubs = 2 if up_rows % (32 * grp) == 0 else 1
    pieces = 2 if out_cols % 256 == 0 else 1
    rsubs = 4 if part % (64 * grp) == 0 else 1
    dsubs = rsubs * pieces
    tsubs = 4 if rows % 64 == 0 else 1
    half = tp // 2
    same = half * group
    layer = tp * group
    units = sp * pieces
    n = out_cols // pieces
    parts = 2 if n % 256 == 0 else 1
    w = n // parts

    vmem = pl.BlockSpec(memory_space=pltpu.VMEM)
    hbm = pl.BlockSpec(memory_space=pl.ANY)
    dma = pltpu.SemaphoreType.DMA
    return pl.pallas_call(
        functools.partial(
            kernel, (grp, sp, tp, heads, blocks, rows, group, usubs, rsubs, pieces, tsubs, parts)
        ),
        out_shape=jax.ShapeDtypeStruct((rows, width), BF16),
        in_specs=[hbm] * 13,
        out_specs=vmem,
        scratch_shapes=[
            pltpu.VMEM((3, heads, tokens), F32),
            pltpu.VMEM((1, dh), F32),
            pltpu.VMEM((1, width), F32),
            pltpu.VMEM((4, tokens, across), BF16),
            pltpu.VMEM((rows, width), BF16),
            pltpu.VMEM((sp, up_rows, part), BF16),
            pltpu.VMEM((sp, part, out_cols), BF16),
            pltpu.VMEM((tp, across, width), BF16),
            pltpu.VMEM((tokens, across), BF16),
            pltpu.VMEM((tp, rows, across), BF16),
            pltpu.VMEM((rows, width), BF16),
            pltpu.VMEM((layer, rows, width), BF16),
            pltpu.VMEM((layer, rows, part), BF16),
            pltpu.VMEM((units, parts, same, rows, w), BF16),
            pltpu.VMEM((units, parts, same, rows, w), BF16),
            pltpu.VMEM((units, parts, group, half, rows, w), BF16),
            pltpu.VMEM((units, parts, half, group, rows, w), BF16),
            pltpu.VMEM((units, parts, rows, w), BF16),
            pltpu.VMEM((units, parts, rows, w), BF16),
            pltpu.VMEM((2, same * rows, n), F32),
            pltpu.VMEM((units, rows, n) if n % 128 else (1, 8, 128), F32),
            pltpu.VMEM((heads, blocks, dh, BLOCK), BF16),
            pltpu.VMEM((heads, blocks, dh, dh), F32),
            pltpu.VMEM((tokens, across), F32),
            pltpu.VMEM((tokens, across), F32),
            pltpu.VMEM((tokens, 128), F32),
            pltpu.VMEM((heads, dh + 16, dh), F32),
            pltpu.VMEM((heads, dh, dh), BF16),
            pltpu.VMEM((heads, dh, dh), BF16),
            pltpu.VMEM((heads, 8, dh), F32),
            pltpu.VMEM((heads, 8, dh), F32),
            dma((6,)),
            dma((3,)),
            dma,
            dma((sp, usubs)),
            dma,
            dma,
            dma,
            dma((sp, dsubs)),
            dma,
            dma((sp, pieces, grp)),
            dma,
            dma((tp,)),
            dma((2,)),
            dma((2,)),
            dma,
            dma,
            dma,
            dma((layer,)),
            dma((tsubs,)),
            dma,
            dma((units, parts)),
            dma,
            dma((units, parts, group)),
            dma,
            dma((units, parts)),
        ],
        compiler_params=pltpu.CompilerParams(
            collective_id=0, has_side_effects=True, vmem_limit_bytes=60 * 1024 * 1024
        ),
    )(
        queries, memory_keys, memory_values, output_preactivation,
        input_preactivation, forget_preactivation, extra_forget_terms,
        head_norm_gain.reshape(1, dh), output_projection_matrix, residual,
        feedforward_norm_gain.reshape(1, width), feedforward_up_matrix, feedforward_down_matrix,
    )


def solution(mesh):
    in_specs = (
        P(("grp", "sp"), "tp"),
        P(("grp", "sp"), "tp"),
        P(("grp", "sp"), "tp"),
        P(("grp", "sp"), "tp"),
        P("tp", ("grp", "sp")),
        P("tp", ("grp", "sp")),
        P("tp", ("grp", "sp")),
        P(),
        P("tp", None),
        P(("grp", "sp", "tp"), None),
        P(),
        P("sp", "tp"),
        P("tp", "sp"),
    )
    out_specs = P(("grp", "sp", "tp"), None)
    shape = (mesh.shape["grp"], mesh.shape["sp"], mesh.shape["tp"])
    return jax.shard_map(
        functools.partial(shards, shape),
        mesh=mesh,
        in_specs=in_specs,
        out_specs=out_specs,
        check_vma=False,
    )
```

```python
import functools

import jax
import jax.numpy as jnp
from jax import lax
from jax.experimental import pallas as pl
from jax.experimental.pallas import tpu as pltpu
from jax.sharding import PartitionSpec as P

BLOCK = 128
EPS = 1e-06
NEG = -1e30
MESH = pl.DeviceIdType.MESH
F32 = jnp.float32
BF16 = jnp.bfloat16


def split_dot(exact, wide, swap=False):
    high = wide.astype(BF16)
    low = (wide - high.astype(F32)).astype(BF16)
    if swap:
        return jnp.dot(high, exact, preferred_element_type=F32) + jnp.dot(
            low, exact, preferred_element_type=F32
        )
    return jnp.dot(exact, high, preferred_element_type=F32) + jnp.dot(
        exact, low, preferred_element_type=F32
    )


def aligned(start, multiple):
    return start if isinstance(start, int) else pl.multiple_of(start, multiple)


def kernel(
    dims,
    q_hbm, k_hbm, v_hbm, o_hbm, igate_hbm, fgate_hbm, extra_hbm, hgain_hbm, wout_hbm, res_hbm,
    fgain_hbm, up_hbm, down_hbm,
    out_ref,
    gates_in, hgain_ref, fgain_ref, qkvo, resb,
    upw, dnw, wo, mixed, mixin, mid, ntok, act, psend, precv, msend, xrecv, zsend, zrecv,
    acc, mlp, keyt, memp, hloc, gates, cols_ref, st_loc, st_out, st_in, top_out, top_in,
    in_sem, loc_sem, wu_send, wu_recv, uy_send, uy_recv, wd_send, wd_recv, dy_send, dy_recv,
    wo_send, wo_recv, st_send, st_recv, mx_send, mx_recv, t_send, t_recv, tz_recv,
    p_send, p_recv, x_send, x_recv, x_home, z_send, z_recv,
):
    grp, sp, tp, heads, blocks, rows, group, usubs, rsubs, pieces, tsubs, parts = dims
    g, z, t = lax.axis_index("grp"), lax.axis_index("sp"), lax.axis_index("tp")
    half = tp // 2
    core, x = lax.rem(t, 2), t // 2
    partner = t + 1 - 2 * core
    zi = lax.rem(z, group)
    other = z + 1 - 2 * zi
    same = half * group
    mine = core * same + zi * half + x
    edge = (z == 0) | (z == sp - 1)
    dsubs = rsubs * pieces
    width = ntok.shape[2]
    part = upw.shape[2]
    up_rows = upw.shape[1]
    out_cols = dnw.shape[2]
    n = out_cols // pieces
    w = n // parts
    urows = up_rows // grp // usubs
    drows = part // grp // rsubs
    trows = rows // tsubs

    def there(gg, zz, tt):
        return {"grp": gg, "sp": zz, "tp": tt}

    def remote(src, dst, send, recv, where):
        return pltpu.make_async_remote_copy(
            src_ref=src, dst_ref=dst, send_sem=send, recv_sem=recv, device_id=where, device_id_type=MESH
        )

    def nth(k):
        power = sp & (sp - 1) == 0
        if not power:
            return lax.rem(z + k, sp)
        gray_of = k
        total = 0
        bit = 1
        while bit < sp:
            mask = (gray_of // bit + gray_of // (2 * bit)) % 2
            zbit = lax.rem(z // bit, 2)
            total = total + (zbit + mask - 2 * zbit * mask) * bit
            bit *= 2
        return total

    kb, vb, qb, ob = (qkvo.at[i] for i in range(4))

    def await_recv(ref, sem):
        remote(ref, ref, mx_send, sem, there(g, z, partner)).wait_recv()

    def await_send(ref, sem):
        remote(ref, ref, sem, mx_recv, there(g, z, partner)).wait_send()

    loads = [
        pltpu.make_async_copy(src, dst, in_sem.at[i])
        for src, dst, i in (
            (fgate_hbm, gates_in.at[0], 0), (extra_hbm, gates_in.at[1], 0), (igate_hbm, gates_in.at[2], 0),
            (k_hbm, kb, 1), (v_hbm, vb, 1), (q_hbm, qb, 2), (o_hbm, ob, 2),
            (hgain_hbm, hgain_ref, 3), (fgain_hbm, fgain_ref, 4), (res_hbm, resb, 5),
        )
    ]
    for c in loads:
        c.start()

    def loaded(ref, i):
        pltpu.make_async_copy(ref, ref, in_sem.at[i]).wait()

    barrier = pltpu.get_barrier_semaphore()
    for j in range(1, tp):
        pl.semaphore_signal(barrier, inc=1, device_id=there(g, z, lax.rem(t + j, tp)), device_id_type=MESH)
    for j in range(1, grp):
        pl.semaphore_signal(barrier, inc=1, device_id=there(lax.rem(g + j, grp), z, t), device_id_type=MESH)

    def greet(j, _):
        pl.semaphore_signal(barrier, inc=1, device_id=there(g, lax.rem(z + j, sp), t), device_id_type=MESH)
        return 0

    lax.fori_loop(1, sp, greet, 0)
    pl.semaphore_wait(barrier, tp + grp + sp - 3)

    def up_rows_of(c, s):
        return pl.ds(aligned(c * (urows * usubs) + s * urows, 16), urows)

    def down_at(c, s):
        rows_at = pl.ds(aligned(c * (drows * rsubs) + s % rsubs * drows, 16), drows)
        return rows_at, pl.ds(s // rsubs * n, n)

    def up_copy(zz, s):
        return remote(
            up_hbm.at[up_rows_of(g, s), pl.ds(aligned(lax.rem(zz, group) * part, 128), part)],
            upw.at[z, up_rows_of(g, s), :],
            wu_send, wu_recv.at[z, s], there(g, zz, t),
        )

    def down_copy(zz, s):
        first = lax.rem(zz, group) * part + g * (drows * rsubs) + s % rsubs * drows
        return remote(
            down_hbm.at[pl.ds(aligned(first, 16), drows), pl.ds(s // rsubs * n, n)],
            dnw.at[(z, *down_at(g, s))],
            wd_send, wd_recv.at[z, s], there(g, zz, t),
        )

    def up_pass(o, s, j):
        at = upw.at[o, up_rows_of(g, s), :]
        return remote(at, at, uy_send, uy_recv, there(lax.rem(g + j, grp), z, t))

    def down_pass(o, s, j):
        at = dnw.at[(o, *down_at(g, s))]
        where = there(lax.rem(g + j, grp), z, t)
        return remote(at, at, dy_send, dy_recv.at[o, s // rsubs, grp - j - 1], where)

    def of_piece(c):
        return range(c * rsubs, (c + 1) * rsubs)

    def relay_up(k):
        o = nth(k)
        for s in range(usubs):
            await_recv(upw.at[o, up_rows_of(g, s), :], wu_recv.at[o, s])
            for j in range(1, grp):
                up_pass(o, s, j).start()

    def relay_down(k, c):
        o = nth(k)
        for s in of_piece(c):
            await_recv(dnw.at[(o, *down_at(g, s))], wd_recv.at[o, s])
            for j in range(1, grp):
                down_pass(o, s, j).start()

    def finish_down(k, c):
        o = nth(k)
        for j in range(1, grp):
            first = aligned(lax.rem(g + j, grp) * (drows * rsubs), 16)
            at = dnw.at[o, pl.ds(first, drows * rsubs), pl.ds(c * n, n)]
            await_recv(at, dy_recv.at[o, c, j - 1])

    def right(copy, first, last, subs, when=True, flip=False):
        def body(i, _):
            d = first + last - 1 - i if flip else i

            @pl.when((z + d < sp) & when)
            def _():
                for s in subs:
                    copy(z + d, s).start()

            return 0

        lax.fori_loop(first, last, body, 0)

    def left(copy, first, last, subs, when=True, flip=False):
        def body(i, _):
            d = first + last - 1 - i if flip else i

            @pl.when((z - d >= 0) & when)
            def _():
                for s in subs:
                    copy(z - d, s).start()

            return 0

        lax.fori_loop(first, last, body, 0)

    us, ds = range(usubs), range(dsubs)
    far_right, far_left = z + 2 < sp, z - 2 >= 0
    held_right = (zi == 0) & far_right
    held_left = (zi == group - 1) & far_left
    free_right = (zi != 0) | (z + 2 >= sp)
    free_left = (zi != group - 1) | (z - 2 < 0)
    right(up_copy, 1, 2, us[:1], z > 0)
    away_left, away_right = zi != group - 1, zi != 0
    left(up_copy, 1, 2, us)
    left(up_copy, 2, sp, us, zi == group - 1)
    left(down_copy, 1, sp, ds, free_left & jnp.logical_not(away_left))

    def wo_copy(tt):
        return remote(wout_hbm, wo.at[t], wo_send, wo_recv.at[t], there(g, z, tt))

    def wo_pass(j):
        tt = lax.rem(x + j, half) * 2 + core
        return remote(wo.at[tt], wo.at[tt], wo_send, wo_recv.at[tt], there(g, z, partner))

    def wo_arrived(tt):
        await_recv(wo.at[tt], wo_recv.at[tt])

    for j in range(1, half):
        wo_copy(lax.rem(x + j, half) * 2 + core).start()
    wo_copy(partner).start()
    own = [
        pltpu.make_async_copy(wout_hbm, wo.at[t], loc_sem.at[0]),
        pltpu.make_async_copy(up_hbm.at[:, pl.ds(aligned(zi * part, 128), part)], upw.at[z], loc_sem.at[1]),
        pltpu.make_async_copy(down_hbm.at[pl.ds(aligned(zi * part, 16), part), :], dnw.at[z], loc_sem.at[2]),
    ]
    for c in own:
        c.start()

    dh = qkvo.shape[2] // heads
    scale = dh ** (-0.5)
    count = heads * blocks
    pad = -count % 8

    def stacked(value):
        pieces_of = [
            value[h : h + 1, b * BLOCK : (b + 1) * BLOCK] for h in range(heads) for b in range(blocks)
        ]
        if pad:
            pieces_of.append(jnp.zeros((pad, BLOCK), F32))
        return jnp.concatenate(pieces_of, axis=0)

    loaded(gates_in, 0)
    pre = gates_in[0]
    log_forget = jnp.minimum(pre, 0.0) - jnp.log1p(jnp.exp(-jnp.abs(pre))) + gates_in[1]
    cum_row = stacked(log_forget)
    lane = lax.broadcasted_iota(jnp.int32, cum_row.shape, 1)
    step = 1
    while step < BLOCK:
        cum_row = cum_row + jnp.where(lane >= step, pltpu.roll(cum_row, step, 1), 0.0)
        step *= 2
    rest_row = stacked(gates_in[2]) - cum_row
    cum_col = cum_row.T
    rest_col = rest_row.T

    loaded(qkvo.at[pl.ds(0, 2)], 1)
    before, totals = {}, {}
    for h in range(heads):
        cols = pl.ds(h * dh, dh)
        run = None
        for b in range(blocks):
            i = h * blocks + b
            at = pl.ds(b * BLOCK, BLOCK)
            total = cum_row[i : i + 1, BLOCK - 1 : BLOCK]
            tail = total + rest_col[:, i : i + 1]
            tail_max = jnp.max(tail, axis=0, keepdims=True)
            weighted = vb[at, cols].astype(F32) * jnp.exp(tail - tail_max)
            key_t = kb[at, cols].astype(F32).T.astype(BF16)
            keyt[h, b] = key_t
            mem = split_dot(key_t, weighted) * scale
            if run is None:
                run = (total, tail_max, mem)
            else:
                before[h, b] = (run[0], run[1])
                memp[h, b] = run[2]
                new = jnp.maximum(total + run[1], tail_max)
                run = (
                    total + run[0],
                    new,
                    jnp.exp(total + run[1] - new) * run[2] + jnp.exp(tail_max - new) * mem,
                )
        st_loc[h, :dh, :] = run[2]
        st_loc[h, dh : dh + 8, :] = jnp.broadcast_to(run[1], (8, dh))
        st_loc[h, dh + 8 : dh + 16, :] = jnp.broadcast_to(run[0], (8, dh))

    def state_copies():
        return (
            remote(top_out, top_in, st_send.at[0], st_recv.at[0], there(g, z + 1, t)),
            remote(st_out, st_in, st_send.at[1], st_recv.at[1], there(g, z + 1, t)),
        )

    @pl.when(z == 0)
    def _():
        st_in[...] = jnp.zeros_like(st_in)
        top_in[...] = jnp.zeros_like(top_in)

    def state_on():
        for h in range(heads):
            m_in = top_in[h, :1, :]
            m_loc = st_loc[h, dh : dh + 1, :]
            total = st_loc[h, dh + 8 : dh + 9, :]
            new = jnp.maximum(total + m_in, m_loc)
            st_out[h] = (
                jnp.exp(total + m_in - new) * st_in[h].astype(F32)
                + jnp.exp(m_loc - new) * st_loc[h, :dh, :]
            ).astype(BF16)
            top_out[h] = jnp.broadcast_to(new, (8, dh))
        for copy in state_copies():
            copy.start()

    def rest_of_sends():
        right(up_copy, 1, 2, us, z == 0)
        right(up_copy, 2, sp, us)
        right(down_copy, 1, 2, ds[:rsubs], free_right & (z == 0))
        right(down_copy, 1, 2, ds[rsubs:], free_right & (zi == 0))

    right(up_copy, 1, 2, us[1:], z > 0)
    right(down_copy, 1, 2, ds[:rsubs], free_right & (zi == 0) & (z > 0))

    @pl.when((z == 0) & (sp > 1))
    def _():
        state_on()

    @pl.when(z == 0)
    def _():
        rest_of_sends()

    loaded(qkvo.at[pl.ds(2, 2)], 2)
    causal = lax.broadcasted_iota(jnp.int32, (BLOCK, BLOCK), 0) >= lax.broadcasted_iota(
        jnp.int32, (BLOCK, BLOCK), 1
    )
    loaded(hgain_ref, 3)
    gain = hgain_ref[...]

    def take_state(when):
        @pl.when(when)
        def _():
            for copy in state_copies():
                copy.wait_recv()

            @pl.when(z < sp - 1)
            def _():
                state_on()

            rest_of_sends()

    for h in range(heads):
        cols = pl.ds(h * dh, dh)
        if h == heads - 1:
            take_state(z == 1)
        for b in range(blocks):
            i = h * blocks + b
            at = pl.ds(b * BLOCK, BLOCK)
            cum = cum_col[:, i : i + 1]
            query = qb[at, cols]
            log_weight = jnp.where(causal, cum + rest_row[i : i + 1, :], NEG)
            row_max = jnp.max(log_weight, axis=1, keepdims=True)
            base = cum
            if b > 0:
                past, stab = before[h, b]
                base = cum + past
                carry = cum + stab
                row_max = jnp.maximum(row_max, carry)
            scores = (
                jnp.dot(query, keyt[h, b], preferred_element_type=F32)
                * scale
                * jnp.exp(log_weight - row_max)
            )
            hidden = split_dot(vb[at, cols], scores, swap=True)
            if b > 0:
                hidden = hidden + jnp.exp(carry - row_max) * split_dot(query, memp[h, b])
            hloc[at, cols] = hidden
            cols_ref[at, 2 * h : 2 * h + 1] = row_max
            cols_ref[at, 2 * h + 1 : 2 * h + 2] = base
            gates[at, cols] = gain * (1.0 / (1.0 + jnp.exp(-ob[at, cols].astype(F32))))

    if sp > 1:
        @pl.when(z > 1)
        def _():
            relay_up(1)

    take_state(z > 1)
    for h in range(heads):
        cols = pl.ds(h * dh, dh)
        memory = st_in[h]
        stab = top_in[h, 0:1, 0:1]
        for b in range(blocks):
            at = pl.ds(b * BLOCK, BLOCK)
            local_max = cols_ref[at, 2 * h : 2 * h + 1]
            carry = cols_ref[at, 2 * h + 1 : 2 * h + 2] + stab
            row_max = jnp.maximum(local_max, carry)
            past = jnp.dot(qb[at, cols], memory, preferred_element_type=F32)
            hidden = jnp.exp(local_max - row_max) * hloc[at, cols] + jnp.exp(carry - row_max) * past
            mean_sq = jnp.mean(hidden * hidden, axis=1, keepdims=True)
            mixed[at, cols] = (hidden * lax.rsqrt(mean_sq + EPS) * gates[at, cols]).astype(BF16)

    def mixed_copy(j):
        d = lax.rem(t + j, tp)
        return remote(
            mixed.at[pl.ds(aligned(d * rows, 16), rows), :],
            mixin.at[t], mx_send, mx_recv, there(g, z, d),
        )

    for j in range(1, tp):
        mixed_copy(j).start()
    mixin[t] = mixed[pl.ds(aligned(t * rows, 16), rows), :]
    left(up_copy, 2, sp, us, away_left)
    def relays_up(first, last):
        def body(k, _):
            relay_up(k)
            return 0

        lax.fori_loop(first, last, body, 0)

    def relays_down(k):
        for c in range(pieces):
            relay_down(k, c)

    middle = min(sp, 2 + (sp - 2) // 2)
    if sp > 1:
        @pl.when(z <= 1)
        def _():
            relay_up(1)

    for j in range(1, half):
        wo_arrived(lax.rem(x + j, half) * 2 + core)
        wo_pass(j).start()

    own[0].wait()
    loaded(fgain_ref, 4)
    loaded(resb, 5)
    for j in range(1, half):
        wo_arrived(lax.rem(x + j, half) * 2 + 1 - core)
    wo_arrived(partner)
    await_recv(mixin.at[pl.ds(0, tp - 1)], mx_recv)

    chunk = min(512, width)
    sum_sq = jnp.zeros((rows, 1), F32)
    for c in range(width // chunk):
        at = pl.ds(c * chunk, chunk)
        branch = jnp.zeros((rows, chunk), F32)
        for tt in range(tp):
            branch = branch + jnp.dot(mixin[tt], wo[tt, :, at], preferred_element_type=F32).astype(
                BF16
            ).astype(F32)
        value = (resb[:, at].astype(F32) + branch).astype(BF16)
        mid[:, at] = value
        wide = value.astype(F32)
        sum_sq = sum_sq + jnp.sum(wide * wide, axis=1, keepdims=True)
    factor = lax.rsqrt(sum_sq * (1.0 / width) + EPS)
    for c in range(width // chunk):
        at = pl.ds(c * chunk, chunk)
        ntok[mine, :, at] = (mid[:, at].astype(F32) * factor * fgain_ref[:, at]).astype(BF16)

    def slot_of(xx, zz):
        return core * same + zz * half + xx

    def row_part(slot, s):
        return ntok.at[slot, pl.ds(s * trows, trows), :]

    def to_pair(s):
        at = row_part(mine, s)
        return remote(at, at, t_send, tz_recv.at[s], there(g, other, t))

    def to_x(j):
        where = there(g, z, lax.rem(x + j, half) * 2 + core)
        return remote(ntok.at[mine], ntok.at[mine], t_send, t_recv.at[mine], where)

    def pass_x(j, s):
        slot = slot_of(x, 1 - zi)
        at = row_part(slot, s)
        return remote(at, at, t_send, t_recv.at[slot], there(g, z, lax.rem(x + j, half) * 2 + core))

    def give(xx, zz):
        slot = slot_of(xx, zz)
        remote(ntok.at[slot], ntok.at[slot], t_send, t_recv.at[slot], there(g, z, partner)).start()

    def take(slot):
        await_recv(ntok.at[slot], t_recv.at[slot])

    ts = range(tsubs)

    for s in ts:
        if group > 1:
            to_pair(s).start()
    for j in range(1, half):
        to_x(j).start()
    give(x, zi)
    left(down_copy, 1, sp, ds, away_left)
    right(down_copy, 1, sp, ds, away_right)
    left(down_copy, 1, 2, ds, held_left)
    right(down_copy, 1, 2, ds, held_right)
    left(down_copy, 2, sp, ds, held_left, flip=True)
    right(down_copy, 2, sp, ds, held_right, flip=True)

    def relays_up(first, last):
        def body(k, _):
            relay_up(k)
            return 0

        lax.fori_loop(first, last, body, 0)

    @pl.when(edge)
    def _():
        if sp > 1:
            relay_down(1, 0)
        relays_up(2, middle)

    @pl.when(jnp.logical_not(edge))
    def _():
        relays_up(2, sp)

    for j in range(1, half):
        xx = lax.rem(x + j, half)
        take(slot_of(xx, zi))
        give(xx, zi)

    @pl.when(edge)
    def _():
        relays_up(middle, sp)
        if sp > 1:
            for c in range(1, pieces):
                relay_down(1, c)

    if group > 1:
        for s in ts:
            await_recv(row_part(slot_of(x, 1 - zi), s), tz_recv.at[s])
            for j in range(1, half):
                pass_x(j, s).start()
        give(x, 1 - zi)
    own[1].wait()

    others = up_rows - up_rows // grp
    if sp > 1 and grp > 1:
        await_recv(upw.at[pl.ds(0, sp - 1), pl.ds(0, others), :], uy_recv)

    def up_quarter(side, zz):
        at = pl.ds(side * same + zz * half, half)
        value = ntok[at].reshape(half * rows, width)
        y = jnp.dot(value, upw[...].reshape(width, part), preferred_element_type=F32)
        y = jnp.maximum(y, 0.0)
        act[at] = (y * y).astype(BF16).reshape(half, rows, part)

    def up_step(i, _):
        side = core + (1 - 2 * core) * lax.rem(i, 2)
        zz = zi + (1 - 2 * zi) * (i // 2)

        @pl.when(i == 1)
        def _():
            for xx in range(half):
                take((1 - core) * same + zi * half + xx)

        if group > 1:
            @pl.when(i == 2)
            def _():
                for j in range(1, half):
                    xx = lax.rem(x + j, half)
                    take(slot_of(xx, 1 - zi))
                    give(xx, 1 - zi)

            @pl.when(i == 3)
            def _():
                for xx in range(half):
                    take((1 - core) * same + (1 - zi) * half + xx)

        up_quarter(side, zz)
        return 0

    lax.fori_loop(0, 2 * group, up_step, 0)
    early = min(3, sp)

    @pl.when(jnp.logical_not(edge))
    def _():
        for k in range(1, early):
            relays_down(k)

    own[2].wait()

    def pre_copy(unit, h):
        return remote(
            psend.at[unit, h], precv.at[unit, h], p_send, p_recv.at[unit, h], there(g, z, partner)
        )

    def x_copy(unit, h, j, far):
        xx = lax.rem(x + j, half)
        zz = 1 - zi if far else zi
        return remote(
            msend.at[unit, h, zz, xx], xrecv.at[unit, h, x, zz],
            x_send, x_recv.at[unit, h] if far else x_home, there(g, z, xx * 2 + core),
        )

    def x_wait(unit, h):
        await_recv(xrecv.at[unit, h, pl.ds(0, half - 1), 0], x_recv.at[unit, h])

    def z_copy(unit, h):
        return remote(
            zsend.at[unit, h], zrecv.at[unit, h], z_send, z_recv.at[unit, h], there(g, other, t)
        )

    share = part // grp

    def product(side, o, c, which):
        at = pl.ds(aligned(which * share, 128), share)
        value = act[pl.ds(side * same, same), :, at].reshape(same * rows, share)
        return jnp.dot(value, dnw[o, at, c * n : (c + 1) * n], preferred_element_type=F32)

    def begin(o, c):
        for side in range(2):
            acc[side] = product(jnp.where(side == 0, 1 - core, core), o, c, g)

    def multiply(unit, o, c):
        def rest(side, place):
            total = acc[place]
            for j in range(1, grp):
                total = total + product(side, o, c, lax.rem(g + j, grp))
            return total

        total = rest(1 - core, 0).astype(BF16)
        for h in range(parts):
            psend[unit, h] = total[:, h * w : (h + 1) * w].reshape(psend.shape[2:])
            pre_copy(unit, h).start()
        acc[1] = rest(core, 1)

    def unit_of(m):
        return nth(m // pieces) * pieces + lax.rem(m, pieces)

    def spread(unit):
        for h in range(parts):
            pre_copy(unit, h).wait_recv()
            total = acc[1, :, h * w : (h + 1) * w].reshape(precv.shape[2:]) + precv[unit, h].astype(F32)
            msend[unit, h] = total.astype(BF16).reshape(msend.shape[2:])
            if group > 1:
                for j in range(1, half):
                    x_copy(unit, h, j, True).start()
        for h in range(parts):
            for j in range(1, half):
                x_copy(unit, h, j, False).start()
            for zz in range(group):
                xrecv[unit, h, x, zz] = msend[unit, h, zz, x]

    def gathered(unit, h, zz):
        total = xrecv[unit, h, 0, zz].astype(F32)
        for xx in range(1, half):
            total = total + xrecv[unit, h, xx, zz].astype(F32)
        return total

    def hand_over(m):
        unit = unit_of(m)
        if group > 1:
            for h in range(parts):
                x_wait(unit, h)
                zsend[unit, h] = gathered(unit, h, 1 - zi).astype(BF16)
                z_copy(unit, h).start()

    def stage(k, _):
        o = nth(k)
        if early > 2:
            for c in range(pieces):
                @pl.when(edge & (k == c))
                def _():
                    relay_down(2, c)

        @pl.when((k >= early) & edge)
        def _():
            relays_down(k)

        for c in range(pieces):
            m = k * pieces + c

            begin(o, c)
            ahead, piece = (k, c + 1) if c + 1 < pieces else (k + 1, 0)

            @pl.when((ahead >= early) & (ahead < sp) & jnp.logical_not(edge))
            def _():
                relay_down(ahead, piece)

            @pl.when(k > 0)
            def _():
                finish_down(k, c)

            multiply(o * pieces + c, o, c)
            spread(o * pieces + c)

            @pl.when(m >= 2)
            def _():
                hand_over(m - 2)

        return 0

    lax.fori_loop(0, sp, stage, 0)
    units = sp * pieces
    if units > 1:
        hand_over(units - 2)
    hand_over(units - 1)

    if half > 1:
        await_recv(xrecv.at[:, :, pl.ds(0, half - 1), 0], x_home)
    direct = out_cols % 128 == 0 and n % 128 == 0

    def finish(m, _):
        unit = unit_of(m)
        for h in range(parts):
            total = gathered(unit, h, zi)
            if group > 1:
                z_copy(unit, h).wait_recv()
                total = total + zrecv[unit, h].astype(F32)
            if direct:
                at = pl.ds(aligned(unit * n + h * w, 128), w)
                out_ref[:, at] = (mid[:, at].astype(F32) + total).astype(BF16)
            else:
                mlp[unit] = total
        return 0

    lax.fori_loop(0, units, finish, 0)
    if not direct:
        for unit in range(units):
            at = pl.ds(unit * n, n)
            out_ref[:, at] = (mid[:, at].astype(F32) + mlp[unit]).astype(BF16)

    if sp > 1:
        await_send(upw.at[pl.ds(0, sp - 1), pl.ds(0, up_rows // grp), :], wu_send)
        await_send(dnw.at[pl.ds(0, sp - 1), pl.ds(0, part // grp), :], wd_send)
        if grp > 1:
            await_send(upw.at[pl.ds(0, sp - 1), pl.ds(0, others), :], uy_send)
            await_send(dnw.at[pl.ds(0, sp - 1), pl.ds(0, part - share), :], dy_send)
    await_send(wo.at[pl.ds(0, 2 * half - 1)], wo_send)
    await_send(mixin.at[pl.ds(0, tp - 1)], mx_send)
    await_send(ntok.at[pl.ds(0, group * (half - 1) + same + group - 1)], t_send)
    await_send(psend, p_send)
    if half > 1:
        await_send(msend.at[:, :, :, pl.ds(0, half - 1)], x_send)
    if group > 1:
        await_send(zsend, z_send)

    @pl.when(z < sp - 1)
    def _():
        for copy in state_copies():
            copy.wait_send()


def shards(
    mesh_shape,
    queries, memory_keys, memory_values, output_preactivation, input_preactivation,
    forget_preactivation, extra_forget_terms, head_norm_gain, output_projection_matrix, residual,
    feedforward_norm_gain, feedforward_up_matrix, feedforward_down_matrix,
):
    grp, sp, tp = mesh_shape
    tokens, across = queries.shape
    heads = input_preactivation.shape[0]
    blocks = tokens // BLOCK
    dh = across // heads
    rows, width = residual.shape
    up_rows, hidden = feedforward_up_matrix.shape
    out_cols = feedforward_down_matrix.shape[1]
    group = 2 if sp % 2 == 0 else 1
    part = hidden // group
    usubs = 2 if up_rows % (32 * grp) == 0 else 1
    pieces = 2 if out_cols % 256 == 0 else 1
    rsubs = 4 if part % (64 * grp) == 0 else 1
    dsubs = rsubs * pieces
    tsubs = 4 if rows % 64 == 0 else 1
    half = tp // 2
    same = half * group
    layer = tp * group
    units = sp * pieces
    n = out_cols // pieces
    parts = 2 if n % 256 == 0 else 1
    w = n // parts

    vmem = pl.BlockSpec(memory_space=pltpu.VMEM)
    hbm = pl.BlockSpec(memory_space=pl.ANY)
    dma = pltpu.SemaphoreType.DMA
    arrays = (
        queries, memory_keys, memory_values, output_preactivation,
        input_preactivation, forget_preactivation, extra_forget_terms,
        head_norm_gain.reshape(1, dh), output_projection_matrix, residual,
        feedforward_norm_gain.reshape(1, width), feedforward_up_matrix, feedforward_down_matrix,
    )
    return pl.pallas_call(
        functools.partial(
            kernel, (grp, sp, tp, heads, blocks, rows, group, usubs, rsubs, pieces, tsubs, parts)
        ),
        out_shape=jax.ShapeDtypeStruct((rows, width), BF16),
        in_specs=[hbm] * 13,
        out_specs=vmem,
        scratch_shapes=[
            pltpu.VMEM((3, heads, tokens), F32),
            pltpu.VMEM((1, dh), F32),
            pltpu.VMEM((1, width), F32),
            pltpu.VMEM((4, tokens, across), BF16),
            pltpu.VMEM((rows, width), BF16),
            pltpu.VMEM((sp, up_rows, part), BF16),
            pltpu.VMEM((sp, part, out_cols), BF16),
            pltpu.VMEM((tp, across, width), BF16),
            pltpu.VMEM((tokens, across), BF16),
            pltpu.VMEM((tp, rows, across), BF16),
            pltpu.VMEM((rows, width), BF16),
            pltpu.VMEM((layer, rows, width), BF16),
            pltpu.VMEM((layer, rows, part), BF16),
            pltpu.VMEM((units, parts, same, rows, w), BF16),
            pltpu.VMEM((units, parts, same, rows, w), BF16),
            pltpu.VMEM((units, parts, group, half, rows, w), BF16),
            pltpu.VMEM((units, parts, half, group, rows, w), BF16),
            pltpu.VMEM((units, parts, rows, w), BF16),
            pltpu.VMEM((units, parts, rows, w), BF16),
            pltpu.VMEM((2, same * rows, n), F32),
            pltpu.VMEM((units, rows, n) if n % 128 else (1, 8, 128), F32),
            pltpu.VMEM((heads, blocks, dh, BLOCK), BF16),
            pltpu.VMEM((heads, blocks, dh, dh), F32),
            pltpu.VMEM((tokens, across), F32),
            pltpu.VMEM((tokens, across), F32),
            pltpu.VMEM((tokens, 128), F32),
            pltpu.VMEM((heads, dh + 16, dh), F32),
            pltpu.VMEM((heads, dh, dh), BF16),
            pltpu.VMEM((heads, dh, dh), BF16),
            pltpu.VMEM((heads, 8, dh), F32),
            pltpu.VMEM((heads, 8, dh), F32),
            dma((6,)),
            dma((3,)),
            dma,
            dma((sp, usubs)),
            dma,
            dma,
            dma,
            dma((sp, dsubs)),
            dma,
            dma((sp, pieces, max(grp - 1, 1))),
            dma,
            dma((tp,)),
            dma((2,)),
            dma((2,)),
            dma,
            dma,
            dma,
            dma((layer,)),
            dma((tsubs,)),
            dma,
            dma((units, parts)),
            dma,
            dma((units, parts)),
            dma,
            dma,
            dma((units, parts)),
        ],
        compiler_params=pltpu.CompilerParams(
            collective_id=0, has_side_effects=True, vmem_limit_bytes=44 * 1024 * 1024
        ),
    )(
        *(pltpu.with_memory_space_constraint(array, pltpu.HBM) for array in arrays)
    )


def solution(mesh):
    in_specs = (
        P(("grp", "sp"), "tp"),
        P(("grp", "sp"), "tp"),
        P(("grp", "sp"), "tp"),
        P(("grp", "sp"), "tp"),
        P("tp", ("grp", "sp")),
        P("tp", ("grp", "sp")),
        P("tp", ("grp", "sp")),
        P(),
        P("tp", None),
        P(("grp", "sp", "tp"), None),
        P(),
        P("sp", "tp"),
        P("tp", "sp"),
    )
    out_specs = P(("grp", "sp", "tp"), None)
    shape = (mesh.shape["grp"], mesh.shape["sp"], mesh.shape["tp"])
    return jax.shard_map(
        functools.partial(shards, shape),
        mesh=mesh,
        in_specs=in_specs,
        out_specs=out_specs,
        check_vma=False,
    )
```

```python
import functools

import jax
import jax.numpy as jnp
from jax import lax
from jax.experimental import pallas as pl
from jax.experimental.pallas import tpu as pltpu
from jax.sharding import PartitionSpec as P

BLOCK = 128
EPS = 1e-06
NEG = -1e30
MESH = pl.DeviceIdType.MESH
F32 = jnp.float32
BF16 = jnp.bfloat16


def split_dot(exact, wide, swap=False):
    high = wide.astype(BF16)
    low = (wide - high.astype(F32)).astype(BF16)
    if swap:
        return jnp.dot(high, exact, preferred_element_type=F32) + jnp.dot(
            low, exact, preferred_element_type=F32
        )
    return jnp.dot(exact, high, preferred_element_type=F32) + jnp.dot(
        exact, low, preferred_element_type=F32
    )


def aligned(start, multiple):
    return start if isinstance(start, int) else pl.multiple_of(start, multiple)


def kernel(
    dims,
    q_hbm, k_hbm, v_hbm, o_hbm, igate_hbm, fgate_hbm, extra_hbm, hgain_hbm, wout_hbm, res_hbm,
    fgain_hbm, up_hbm, down_hbm,
    out_ref,
    gates_in, hgain_ref, fgain_ref, qkvo, resb,
    upw, dnw, wo, mixed, mixin, mid, ntok, act, psend, precv, msend, xrecv, zsend, zrecv,
    acc, mlp, keyt, memp, hloc, gates, cols_ref, st_loc, st_out, st_in, top_out, top_in,
    in_sem, loc_sem, wu_send, wu_recv, uy_send, uy_recv, wd_send, wd_recv, dy_send, dy_recv,
    wo_send, wo_recv, st_send, st_recv, mx_send, mx_recv, t_send, t_recv, tz_recv,
    p_send, p_recv, x_send, x_recv, x_home, z_send, z_recv,
):
    grp, sp, tp, heads, blocks, rows, group, usubs, rsubs, pieces, tsubs, parts = dims
    g, z, t = lax.axis_index("grp"), lax.axis_index("sp"), lax.axis_index("tp")
    half = tp // 2
    core, x = lax.rem(t, 2), t // 2
    partner = t + 1 - 2 * core
    zi = lax.rem(z, group)
    other = z + 1 - 2 * zi
    same = half * group
    mine = core * same + zi * half + x
    edge = (z == 0) | (z == sp - 1)
    dsubs = rsubs * pieces
    width = ntok.shape[2]
    part = upw.shape[2]
    up_rows = upw.shape[1]
    out_cols = dnw.shape[2]
    n = out_cols // pieces
    w = n // parts
    urows = up_rows // grp // usubs
    drows = part // grp // rsubs
    trows = rows // tsubs

    def there(gg, zz, tt):
        return {"grp": gg, "sp": zz, "tp": tt}

    def remote(src, dst, send, recv, where):
        return pltpu.make_async_remote_copy(
            src_ref=src, dst_ref=dst, send_sem=send, recv_sem=recv, device_id=where, device_id_type=MESH
        )

    def nth(k, zz=None):
        zz = z if zz is None else zz
        power = sp & (sp - 1) == 0
        if not power:
            return lax.rem(zz + k, sp)
        gray_of = k
        total = 0
        bit = 1
        while bit < sp:
            mask = (gray_of // bit + gray_of // (2 * bit)) % 2
            zbit = lax.rem(zz // bit, 2)
            total = total + (zbit + mask - 2 * zbit * mask) * bit
            bit *= 2
        return total

    kb, vb, qb, ob = (qkvo.at[i] for i in range(4))

    def await_recv(ref, sem):
        remote(ref, ref, mx_send, sem, there(g, z, partner)).wait_recv()

    def await_send(ref, sem):
        remote(ref, ref, sem, mx_recv, there(g, z, partner)).wait_send()

    loads = [
        pltpu.make_async_copy(src, dst, in_sem.at[i])
        for src, dst, i in (
            (fgate_hbm, gates_in.at[0], 0), (extra_hbm, gates_in.at[1], 0), (igate_hbm, gates_in.at[2], 0),
            (k_hbm, kb, 1), (v_hbm, vb, 1), (q_hbm, qb, 2), (o_hbm, ob, 2),
            (hgain_hbm, hgain_ref, 3), (fgain_hbm, fgain_ref, 4), (res_hbm, resb, 5),
        )
    ]
    for c in loads:
        c.start()

    def loaded(ref, i):
        pltpu.make_async_copy(ref, ref, in_sem.at[i]).wait()

    barrier = pltpu.get_barrier_semaphore()
    for j in range(1, tp):
        pl.semaphore_signal(barrier, inc=1, device_id=there(g, z, lax.rem(t + j, tp)), device_id_type=MESH)
    for j in range(1, grp):
        pl.semaphore_signal(barrier, inc=1, device_id=there(lax.rem(g + j, grp), z, t), device_id_type=MESH)

    def greet(j, _):
        pl.semaphore_signal(barrier, inc=1, device_id=there(g, lax.rem(z + j, sp), t), device_id_type=MESH)
        return 0

    lax.fori_loop(1, sp, greet, 0)
    pl.semaphore_wait(barrier, tp + grp + sp - 3)

    def up_rows_of(c, s):
        return pl.ds(aligned(c * (urows * usubs) + s * urows, 16), urows)

    def down_at(c, s):
        rows_at = pl.ds(aligned(c * (drows * rsubs) + s % rsubs * drows, 16), drows)
        return rows_at, pl.ds(s // rsubs * n, n)

    def up_copy(zz, s):
        return remote(
            up_hbm.at[up_rows_of(g, s), pl.ds(aligned(lax.rem(zz, group) * part, 128), part)],
            upw.at[z, up_rows_of(g, s), :],
            wu_send, wu_recv.at[z, s], there(g, zz, t),
        )

    def down_copy(zz, s):
        final = (nth(sp - 1, zz) == z).astype(jnp.int32)
        slot = (z * pieces + s // rsubs) * (1 - final) + (sp * pieces + s) * final
        first = lax.rem(zz, group) * part + g * (drows * rsubs) + s % rsubs * drows
        return remote(
            down_hbm.at[pl.ds(aligned(first, 16), drows), pl.ds(s // rsubs * n, n)],
            dnw.at[(z, *down_at(g, s))],
            wd_send, wd_recv.at[slot], there(g, zz, t),
        )

    def up_pass(o, s, j):
        at = upw.at[o, up_rows_of(g, s), :]
        return remote(at, at, uy_send, uy_recv, there(lax.rem(g + j, grp), z, t))

    def down_pass(o, s, j):
        at = dnw.at[(o, *down_at(g, s))]
        where = there(lax.rem(g + j, grp), z, t)
        return remote(at, at, dy_send, dy_recv.at[o, s // rsubs, grp - j - 1], where)

    def of_piece(c):
        return range(c * rsubs, (c + 1) * rsubs)

    def relay_up(k):
        o = nth(k)
        for s in range(usubs):
            await_recv(upw.at[o, up_rows_of(g, s), :], wu_recv.at[o, s])
            for j in range(1, grp):
                up_pass(o, s, j).start()

    def relay_parts(o, c):
        for s in of_piece(c):
            await_recv(dnw.at[(o, *down_at(g, s))], wd_recv.at[sp * pieces + s])
            for j in range(1, grp):
                down_pass(o, s, j).start()

    def relay_whole(o, c):
        at = dnw.at[o, pl.ds(aligned(g * (drows * rsubs), 16), drows * rsubs), pl.ds(c * n, n)]
        await_recv(at, wd_recv.at[o * pieces + c])
        for j in range(1, grp):
            where = there(lax.rem(g + j, grp), z, t)
            remote(at, at, dy_send, dy_recv.at[o, c, grp - j - 1], where).start()

    def relay_down(k, c):
        o = nth(k)
        if isinstance(k, int):
            (relay_parts if k == sp - 1 else relay_whole)(o, c)
            return

        @pl.when(k == sp - 1)
        def _():
            relay_parts(o, c)

        @pl.when(k < sp - 1)
        def _():
            relay_whole(o, c)

    def finish_down(k, c):
        o = nth(k)
        for j in range(1, grp):
            first = aligned(lax.rem(g + j, grp) * (drows * rsubs), 16)
            at = dnw.at[o, pl.ds(first, drows * rsubs), pl.ds(c * n, n)]
            await_recv(at, dy_recv.at[o, c, j - 1])

    def right(copy, first, last, subs, when=True, flip=False):
        def body(i, _):
            d = first + last - 1 - i if flip else i

            @pl.when((z + d < sp) & when)
            def _():
                for s in subs:
                    copy(z + d, s).start()

            return 0

        lax.fori_loop(first, last, body, 0)

    def left(copy, first, last, subs, when=True, flip=False):
        def body(i, _):
            d = first + last - 1 - i if flip else i

            @pl.when((z - d >= 0) & when)
            def _():
                for s in subs:
                    copy(z - d, s).start()

            return 0

        lax.fori_loop(first, last, body, 0)

    us, ds = range(usubs), range(dsubs)
    far_right, far_left = z + 2 < sp, z - 2 >= 0
    held_right = (zi == 0) & far_right
    held_left = (zi == group - 1) & far_left
    free_right = (zi != 0) | (z + 2 >= sp)
    free_left = (zi != group - 1) | (z - 2 < 0)
    right(up_copy, 1, 2, us[:1], z > 0)
    away_left, away_right = zi != group - 1, zi != 0
    left(up_copy, 1, 2, us)
    left(up_copy, 2, sp, us, zi == group - 1)
    left(down_copy, 1, sp, ds, free_left & jnp.logical_not(away_left))

    def wo_copy(tt):
        return remote(wout_hbm, wo.at[t], wo_send, wo_recv.at[t], there(g, z, tt))

    def wo_pass(j):
        tt = lax.rem(x + j, half) * 2 + core
        return remote(wo.at[tt], wo.at[tt], wo_send, wo_recv.at[tt], there(g, z, partner))

    def wo_arrived(tt):
        await_recv(wo.at[tt], wo_recv.at[tt])

    for j in range(1, half):
        wo_copy(lax.rem(x + j, half) * 2 + core).start()
    wo_copy(partner).start()
    own = [
        pltpu.make_async_copy(wout_hbm, wo.at[t], loc_sem.at[0]),
        pltpu.make_async_copy(up_hbm.at[:, pl.ds(aligned(zi * part, 128), part)], upw.at[z], loc_sem.at[1]),
        pltpu.make_async_copy(down_hbm.at[pl.ds(aligned(zi * part, 16), part), :], dnw.at[z], loc_sem.at[2]),
    ]
    for c in own:
        c.start()

    dh = qkvo.shape[2] // heads
    scale = dh ** (-0.5)
    count = heads * blocks
    pad = -count % 8

    def stacked(value):
        pieces_of = [
            value[h : h + 1, b * BLOCK : (b + 1) * BLOCK] for h in range(heads) for b in range(blocks)
        ]
        if pad:
            pieces_of.append(jnp.zeros((pad, BLOCK), F32))
        return jnp.concatenate(pieces_of, axis=0)

    loaded(gates_in, 0)
    pre = gates_in[0]
    log_forget = jnp.minimum(pre, 0.0) - jnp.log1p(jnp.exp(-jnp.abs(pre))) + gates_in[1]
    cum_row = stacked(log_forget)
    lane = lax.broadcasted_iota(jnp.int32, cum_row.shape, 1)
    step = 1
    while step < BLOCK:
        cum_row = cum_row + jnp.where(lane >= step, pltpu.roll(cum_row, step, 1), 0.0)
        step *= 2
    rest_row = stacked(gates_in[2]) - cum_row
    cum_col = cum_row.T
    rest_col = rest_row.T

    loaded(qkvo.at[pl.ds(0, 2)], 1)
    before, totals = {}, {}
    for h in range(heads):
        cols = pl.ds(h * dh, dh)
        run = None
        for b in range(blocks):
            i = h * blocks + b
            at = pl.ds(b * BLOCK, BLOCK)
            total = cum_row[i : i + 1, BLOCK - 1 : BLOCK]
            tail = total + rest_col[:, i : i + 1]
            tail_max = jnp.max(tail, axis=0, keepdims=True)
            weighted = vb[at, cols].astype(F32) * jnp.exp(tail - tail_max)
            key_t = kb[at, cols].astype(F32).T.astype(BF16)
            keyt[h, b] = key_t
            mem = split_dot(key_t, weighted) * scale
            if run is None:
                run = (total, tail_max, mem)
            else:
                before[h, b] = (run[0], run[1])
                memp[h, b] = run[2]
                new = jnp.maximum(total + run[1], tail_max)
                run = (
                    total + run[0],
                    new,
                    jnp.exp(total + run[1] - new) * run[2] + jnp.exp(tail_max - new) * mem,
                )
        st_loc[h, :dh, :] = run[2]
        st_loc[h, dh : dh + 8, :] = jnp.broadcast_to(run[1], (8, dh))
        st_loc[h, dh + 8 : dh + 16, :] = jnp.broadcast_to(run[0], (8, dh))

    def state_copies():
        return (
            remote(top_out, top_in, st_send.at[0], st_recv.at[0], there(g, z + 1, t)),
            remote(st_out, st_in, st_send.at[1], st_recv.at[1], there(g, z + 1, t)),
        )

    @pl.when(z == 0)
    def _():
        st_in[...] = jnp.zeros_like(st_in)
        top_in[...] = jnp.zeros_like(top_in)

    def state_on():
        for h in range(heads):
            m_in = top_in[h, :1, :]
            m_loc = st_loc[h, dh : dh + 1, :]
            total = st_loc[h, dh + 8 : dh + 9, :]
            new = jnp.maximum(total + m_in, m_loc)
            st_out[h] = (
                jnp.exp(total + m_in - new) * st_in[h].astype(F32)
                + jnp.exp(m_loc - new) * st_loc[h, :dh, :]
            ).astype(BF16)
            top_out[h] = jnp.broadcast_to(new, (8, dh))
        for copy in state_copies():
            copy.start()

    def rest_of_sends():
        right(up_copy, 1, 2, us, z == 0)
        right(up_copy, 2, sp, us)
        right(down_copy, 1, 2, ds[:rsubs], free_right & (z == 0))
        right(down_copy, 1, 2, ds[rsubs:], free_right & (zi == 0))

    right(up_copy, 1, 2, us[1:], z > 0)
    right(down_copy, 1, 2, ds[:rsubs], free_right & (zi == 0) & (z > 0))

    @pl.when((z == 0) & (sp > 1))
    def _():
        state_on()

    @pl.when(z == 0)
    def _():
        rest_of_sends()

    loaded(qkvo.at[pl.ds(2, 2)], 2)
    causal = lax.broadcasted_iota(jnp.int32, (BLOCK, BLOCK), 0) >= lax.broadcasted_iota(
        jnp.int32, (BLOCK, BLOCK), 1
    )
    loaded(hgain_ref, 3)
    gain = hgain_ref[...]

    def take_state(when):
        @pl.when(when)
        def _():
            for copy in state_copies():
                copy.wait_recv()

            @pl.when(z < sp - 1)
            def _():
                state_on()

            rest_of_sends()

    for h in range(heads):
        cols = pl.ds(h * dh, dh)
        if h == heads - 1:
            take_state(z == 1)
        for b in range(blocks):
            i = h * blocks + b
            at = pl.ds(b * BLOCK, BLOCK)
            cum = cum_col[:, i : i + 1]
            query = qb[at, cols]
            log_weight = jnp.where(causal, cum + rest_row[i : i + 1, :], NEG)
            row_max = jnp.max(log_weight, axis=1, keepdims=True)
            base = cum
            if b > 0:
                past, stab = before[h, b]
                base = cum + past
                carry = cum + stab
                row_max = jnp.maximum(row_max, carry)
            scores = (
                jnp.dot(query, keyt[h, b], preferred_element_type=F32)
                * scale
                * jnp.exp(log_weight - row_max)
            )
            hidden = split_dot(vb[at, cols], scores, swap=True)
            if b > 0:
                hidden = hidden + jnp.exp(carry - row_max) * split_dot(query, memp[h, b])
            hloc[at, cols] = hidden
            cols_ref[at, 2 * h : 2 * h + 1] = row_max
            cols_ref[at, 2 * h + 1 : 2 * h + 2] = base
            gates[at, cols] = gain * (1.0 / (1.0 + jnp.exp(-ob[at, cols].astype(F32))))

    if sp > 1:
        @pl.when(z > 1)
        def _():
            relay_up(1)

    take_state(z > 1)
    for h in range(heads):
        cols = pl.ds(h * dh, dh)
        memory = st_in[h]
        stab = top_in[h, 0:1, 0:1]
        for b in range(blocks):
            at = pl.ds(b * BLOCK, BLOCK)
            local_max = cols_ref[at, 2 * h : 2 * h + 1]
            carry = cols_ref[at, 2 * h + 1 : 2 * h + 2] + stab
            row_max = jnp.maximum(local_max, carry)
            past = jnp.dot(qb[at, cols], memory, preferred_element_type=F32)
            hidden = jnp.exp(local_max - row_max) * hloc[at, cols] + jnp.exp(carry - row_max) * past
            mean_sq = jnp.mean(hidden * hidden, axis=1, keepdims=True)
            mixed[at, cols] = (hidden * lax.rsqrt(mean_sq + EPS) * gates[at, cols]).astype(BF16)

    def mixed_copy(j):
        d = lax.rem(t + j, tp)
        return remote(
            mixed.at[pl.ds(aligned(d * rows, 16), rows), :],
            mixin.at[t], mx_send, mx_recv, there(g, z, d),
        )

    for j in range(1, tp):
        mixed_copy(j).start()
    mixin[t] = mixed[pl.ds(aligned(t * rows, 16), rows), :]
    left(up_copy, 2, sp, us, away_left)
    def relays_up(first, last):
        def body(k, _):
            relay_up(k)
            return 0

        lax.fori_loop(first, last, body, 0)

    def relays_down(k):
        for c in range(pieces):
            relay_down(k, c)

    middle = min(sp, 2 + (sp - 2) // 2)
    if sp > 1:
        @pl.when(z <= 1)
        def _():
            relay_up(1)

    for j in range(1, half):
        wo_arrived(lax.rem(x + j, half) * 2 + core)
        wo_pass(j).start()

    own[0].wait()
    loaded(fgain_ref, 4)
    loaded(resb, 5)
    for j in range(1, half):
        wo_arrived(lax.rem(x + j, half) * 2 + 1 - core)
    wo_arrived(partner)
    await_recv(mixin.at[pl.ds(0, tp - 1)], mx_recv)

    chunk = min(512, width)
    sum_sq = jnp.zeros((rows, 1), F32)
    for c in range(width // chunk):
        at = pl.ds(c * chunk, chunk)
        branch = jnp.zeros((rows, chunk), F32)
        for tt in range(tp):
            branch = branch + jnp.dot(mixin[tt], wo[tt, :, at], preferred_element_type=F32).astype(
                BF16
            ).astype(F32)
        value = (resb[:, at].astype(F32) + branch).astype(BF16)
        mid[:, at] = value
        wide = value.astype(F32)
        sum_sq = sum_sq + jnp.sum(wide * wide, axis=1, keepdims=True)
    factor = lax.rsqrt(sum_sq * (1.0 / width) + EPS)
    for c in range(width // chunk):
        at = pl.ds(c * chunk, chunk)
        ntok[mine, :, at] = (mid[:, at].astype(F32) * factor * fgain_ref[:, at]).astype(BF16)

    def slot_of(xx, zz):
        return core * same + zz * half + xx

    def row_part(slot, s):
        return ntok.at[slot, pl.ds(s * trows, trows), :]

    def to_pair(s):
        at = row_part(mine, s)
        return remote(at, at, t_send, tz_recv.at[s], there(g, other, t))

    def to_x(j):
        where = there(g, z, lax.rem(x + j, half) * 2 + core)
        return remote(ntok.at[mine], ntok.at[mine], t_send, t_recv.at[mine], where)

    def pass_x(j, s):
        slot = slot_of(x, 1 - zi)
        at = row_part(slot, s)
        return remote(at, at, t_send, t_recv.at[slot], there(g, z, lax.rem(x + j, half) * 2 + core))

    def give(xx, zz):
        slot = slot_of(xx, zz)
        remote(ntok.at[slot], ntok.at[slot], t_send, t_recv.at[slot], there(g, z, partner)).start()

    def take(slot):
        await_recv(ntok.at[slot], t_recv.at[slot])

    ts = range(tsubs)

    for s in ts:
        if group > 1:
            to_pair(s).start()
    for j in range(1, half):
        to_x(j).start()
    give(x, zi)
    left(down_copy, 1, sp, ds, away_left)
    right(down_copy, 1, sp, ds, away_right)
    left(down_copy, 1, 2, ds, held_left)
    right(down_copy, 1, 2, ds, held_right)
    left(down_copy, 2, sp, ds, held_left, flip=True)
    right(down_copy, 2, sp, ds, held_right, flip=True)

    def relays_up(first, last):
        def body(k, _):
            relay_up(k)
            return 0

        lax.fori_loop(first, last, body, 0)

    @pl.when(edge)
    def _():
        if sp > 1:
            relay_down(1, 0)
        relays_up(2, middle)

    @pl.when(jnp.logical_not(edge))
    def _():
        relays_up(2, sp)

    for j in range(1, half):
        xx = lax.rem(x + j, half)
        take(slot_of(xx, zi))
        give(xx, zi)

    @pl.when(edge)
    def _():
        relays_up(middle, sp)
        if sp > 1:
            for c in range(1, pieces):
                relay_down(1, c)

    if group > 1:
        for s in ts:
            await_recv(row_part(slot_of(x, 1 - zi), s), tz_recv.at[s])
            for j in range(1, half):
                pass_x(j, s).start()
        give(x, 1 - zi)
    own[1].wait()

    others = up_rows - up_rows // grp
    if sp > 1 and grp > 1:
        await_recv(upw.at[pl.ds(0, sp - 1), pl.ds(0, others), :], uy_recv)

    def up_quarter(side, zz):
        at = pl.ds(side * same + zz * half, half)
        value = ntok[at].reshape(half * rows, width)
        y = jnp.dot(value, upw[...].reshape(width, part), preferred_element_type=F32)
        y = jnp.maximum(y, 0.0)
        act[at] = (y * y).astype(BF16).reshape(half, rows, part)

    def up_step(i, _):
        side = core + (1 - 2 * core) * lax.rem(i, 2)
        zz = zi + (1 - 2 * zi) * (i // 2)

        @pl.when(i == 1)
        def _():
            for xx in range(half):
                take((1 - core) * same + zi * half + xx)

        if group > 1:
            @pl.when(i == 2)
            def _():
                for j in range(1, half):
                    xx = lax.rem(x + j, half)
                    take(slot_of(xx, 1 - zi))
                    give(xx, 1 - zi)

            @pl.when(i == 3)
            def _():
                for xx in range(half):
                    take((1 - core) * same + (1 - zi) * half + xx)

        up_quarter(side, zz)
        return 0

    lax.fori_loop(0, 2 * group, up_step, 0)
    early = min(3, sp)

    @pl.when(jnp.logical_not(edge))
    def _():
        for k in range(1, early):
            relays_down(k)

    own[2].wait()

    def pre_copy(unit, h):
        return remote(
            psend.at[unit, h], precv.at[unit, h], p_send, p_recv.at[unit, h], there(g, z, partner)
        )

    def x_copy(unit, h, j, far):
        xx = lax.rem(x + j, half)
        zz = 1 - zi if far else zi
        return remote(
            msend.at[unit, h, zz, xx], xrecv.at[unit, h, x, zz],
            x_send, x_recv.at[unit, h] if far else x_home, there(g, z, xx * 2 + core),
        )

    def x_wait(unit, h):
        await_recv(xrecv.at[unit, h, pl.ds(0, half - 1), 0], x_recv.at[unit, h])

    def z_copy(unit, h):
        return remote(
            zsend.at[unit, h], zrecv.at[unit, h], z_send, z_recv.at[unit, h], there(g, other, t)
        )

    share = part // grp

    def product(side, o, c, which):
        at = pl.ds(aligned(which * share, 128), share)
        value = act[pl.ds(side * same, same), :, at].reshape(same * rows, share)
        return jnp.dot(value, dnw[o, at, c * n : (c + 1) * n], preferred_element_type=F32)

    def begin(o, c):
        for side in range(2):
            acc[side] = product(jnp.where(side == 0, 1 - core, core), o, c, g)

    def multiply(unit, o, c):
        def rest(side, place):
            total = acc[place]
            for j in range(1, grp):
                total = total + product(side, o, c, lax.rem(g + j, grp))
            return total

        total = rest(1 - core, 0).astype(BF16)
        for h in range(parts):
            psend[unit, h] = total[:, h * w : (h + 1) * w].reshape(psend.shape[2:])
            pre_copy(unit, h).start()
        acc[1] = rest(core, 1)

    def unit_of(m):
        return nth(m // pieces) * pieces + lax.rem(m, pieces)

    def spread(unit):
        for h in range(parts):
            pre_copy(unit, h).wait_recv()
            total = acc[1, :, h * w : (h + 1) * w].reshape(precv.shape[2:]) + precv[unit, h].astype(F32)
            msend[unit, h] = total.astype(BF16).reshape(msend.shape[2:])
            if group > 1:
                for j in range(1, half):
                    x_copy(unit, h, j, True).start()
        for h in range(parts):
            for j in range(1, half):
                x_copy(unit, h, j, False).start()
            for zz in range(group):
                xrecv[unit, h, x, zz] = msend[unit, h, zz, x]

    def gathered(unit, h, zz):
        total = xrecv[unit, h, 0, zz].astype(F32)
        for xx in range(1, half):
            total = total + xrecv[unit, h, xx, zz].astype(F32)
        return total

    def hand_over(m):
        unit = unit_of(m)
        if group > 1:
            for h in range(parts):
                x_wait(unit, h)
                zsend[unit, h] = gathered(unit, h, 1 - zi).astype(BF16)
                z_copy(unit, h).start()

    def stage(k, _):
        o = nth(k)
        if early > 2:
            for c in range(pieces):
                @pl.when(edge & (k == c))
                def _():
                    relay_down(2, c)

        @pl.when((k >= early) & edge)
        def _():
            relays_down(k)

        for c in range(pieces):
            m = k * pieces + c

            begin(o, c)
            ahead, piece = (k, c + 1) if c + 1 < pieces else (k + 1, 0)

            @pl.when((ahead >= early) & (ahead < sp) & jnp.logical_not(edge))
            def _():
                relay_down(ahead, piece)

            @pl.when(k > 0)
            def _():
                finish_down(k, c)

            multiply(o * pieces + c, o, c)
            spread(o * pieces + c)

            @pl.when(m >= 2)
            def _():
                hand_over(m - 2)

        return 0

    lax.fori_loop(0, sp, stage, 0)
    units = sp * pieces
    if units > 1:
        hand_over(units - 2)
    hand_over(units - 1)

    if half > 1:
        await_recv(xrecv.at[:, :, pl.ds(0, half - 1), 0], x_home)
    direct = out_cols % 128 == 0 and n % 128 == 0

    def finish(m, _):
        unit = unit_of(m)
        for h in range(parts):
            total = gathered(unit, h, zi)
            if group > 1:
                z_copy(unit, h).wait_recv()
                total = total + zrecv[unit, h].astype(F32)
            if direct:
                at = pl.ds(aligned(unit * n + h * w, 128), w)
                out_ref[:, at] = (mid[:, at].astype(F32) + total).astype(BF16)
            else:
                mlp[unit] = total
        return 0

    lax.fori_loop(0, units, finish, 0)
    if not direct:
        for unit in range(units):
            at = pl.ds(unit * n, n)
            out_ref[:, at] = (mid[:, at].astype(F32) + mlp[unit]).astype(BF16)

    if sp > 1:
        await_send(upw.at[pl.ds(0, sp - 1), pl.ds(0, up_rows // grp), :], wu_send)
        await_send(dnw.at[pl.ds(0, sp - 1), pl.ds(0, part // grp), :], wd_send)
        if grp > 1:
            await_send(upw.at[pl.ds(0, sp - 1), pl.ds(0, others), :], uy_send)
            await_send(dnw.at[pl.ds(0, sp - 1), pl.ds(0, part - share), :], dy_send)
    await_send(wo.at[pl.ds(0, 2 * half - 1)], wo_send)
    await_send(mixin.at[pl.ds(0, tp - 1)], mx_send)
    await_send(ntok.at[pl.ds(0, group * (half - 1) + same + group - 1)], t_send)
    await_send(psend, p_send)
    if half > 1:
        await_send(msend.at[:, :, :, pl.ds(0, half - 1)], x_send)
    if group > 1:
        await_send(zsend, z_send)

    @pl.when(z < sp - 1)
    def _():
        for copy in state_copies():
            copy.wait_send()


def shards(
    mesh_shape,
    queries, memory_keys, memory_values, output_preactivation, input_preactivation,
    forget_preactivation, extra_forget_terms, head_norm_gain, output_projection_matrix, residual,
    feedforward_norm_gain, feedforward_up_matrix, feedforward_down_matrix,
):
    grp, sp, tp = mesh_shape
    tokens, across = queries.shape
    heads = input_preactivation.shape[0]
    blocks = tokens // BLOCK
    dh = across // heads
    rows, width = residual.shape
    up_rows, hidden = feedforward_up_matrix.shape
    out_cols = feedforward_down_matrix.shape[1]
    group = 2 if sp % 2 == 0 else 1
    part = hidden // group
    usubs = 2 if up_rows % (32 * grp) == 0 else 1
    pieces = 2 if out_cols % 256 == 0 else 1
    rsubs = 8 if part % (128 * grp) == 0 else 1
    dsubs = rsubs * pieces
    tsubs = 4 if rows % 64 == 0 else 1
    half = tp // 2
    same = half * group
    layer = tp * group
    units = sp * pieces
    n = out_cols // pieces
    parts = 2 if n % 256 == 0 else 1
    w = n // parts

    vmem = pl.BlockSpec(memory_space=pltpu.VMEM)
    hbm = pl.BlockSpec(memory_space=pl.ANY)
    dma = pltpu.SemaphoreType.DMA
    arrays = (
        queries, memory_keys, memory_values, output_preactivation,
        input_preactivation, forget_preactivation, extra_forget_terms,
        head_norm_gain.reshape(1, dh), output_projection_matrix, residual,
        feedforward_norm_gain.reshape(1, width), feedforward_up_matrix, feedforward_down_matrix,
    )
    return pl.pallas_call(
        functools.partial(
            kernel, (grp, sp, tp, heads, blocks, rows, group, usubs, rsubs, pieces, tsubs, parts)
        ),
        out_shape=jax.ShapeDtypeStruct((rows, width), BF16),
        in_specs=[hbm] * 13,
        out_specs=vmem,
        scratch_shapes=[
            pltpu.VMEM((3, heads, tokens), F32),
            pltpu.VMEM((1, dh), F32),
            pltpu.VMEM((1, width), F32),
            pltpu.VMEM((4, tokens, across), BF16),
            pltpu.VMEM((rows, width), BF16),
            pltpu.VMEM((sp, up_rows, part), BF16),
            pltpu.VMEM((sp, part, out_cols), BF16),
            pltpu.VMEM((tp, across, width), BF16),
            pltpu.VMEM((tokens, across), BF16),
            pltpu.VMEM((tp, rows, across), BF16),
            pltpu.VMEM((rows, width), BF16),
            pltpu.VMEM((layer, rows, width), BF16),
            pltpu.VMEM((layer, rows, part), BF16),
            pltpu.VMEM((units, parts, same, rows, w), BF16),
            pltpu.VMEM((units, parts, same, rows, w), BF16),
            pltpu.VMEM((units, parts, group, half, rows, w), BF16),
            pltpu.VMEM((units, parts, half, group, rows, w), BF16),
            pltpu.VMEM((units, parts, rows, w), BF16),
            pltpu.VMEM((units, parts, rows, w), BF16),
            pltpu.VMEM((2, same * rows, n), F32),
            pltpu.VMEM((units, rows, n) if n % 128 else (1, 8, 128), F32),
            pltpu.VMEM((heads, blocks, dh, BLOCK), BF16),
            pltpu.VMEM((heads, blocks, dh, dh), F32),
            pltpu.VMEM((tokens, across), F32),
            pltpu.VMEM((tokens, across), F32),
            pltpu.VMEM((tokens, 128), F32),
            pltpu.VMEM((heads, dh + 16, dh), F32),
            pltpu.VMEM((heads, dh, dh), BF16),
            pltpu.VMEM((heads, dh, dh), BF16),
            pltpu.VMEM((heads, 8, dh), F32),
            pltpu.VMEM((heads, 8, dh), F32),
            dma((6,)),
            dma((3,)),
            dma,
            dma((sp, usubs)),
            dma,
            dma,
            dma,
            dma((sp * pieces + dsubs,)),
            dma,
            dma((sp, pieces, max(grp - 1, 1))),
            dma,
            dma((tp,)),
            dma((2,)),
            dma((2,)),
            dma,
            dma,
            dma,
            dma((layer,)),
            dma((tsubs,)),
            dma,
            dma((units, parts)),
            dma,
            dma((units, parts)),
            dma,
            dma,
            dma((units, parts)),
        ],
        compiler_params=pltpu.CompilerParams(
            collective_id=0, has_side_effects=True, vmem_limit_bytes=44 * 1024 * 1024
        ),
    )(
        *(pltpu.with_memory_space_constraint(array, pltpu.HBM) for array in arrays)
    )


def solution(mesh):
    in_specs = (
        P(("grp", "sp"), "tp"),
        P(("grp", "sp"), "tp"),
        P(("grp", "sp"), "tp"),
        P(("grp", "sp"), "tp"),
        P("tp", ("grp", "sp")),
        P("tp", ("grp", "sp")),
        P("tp", ("grp", "sp")),
        P(),
        P("tp", None),
        P(("grp", "sp", "tp"), None),
        P(),
        P("sp", "tp"),
        P("tp", "sp"),
    )
    out_specs = P(("grp", "sp", "tp"), None)
    shape = (mesh.shape["grp"], mesh.shape["sp"], mesh.shape["tp"])
    return jax.shard_map(
        functools.partial(shards, shape),
        mesh=mesh,
        in_specs=in_specs,
        out_specs=out_specs,
        check_vma=False,
    )
```
